512 devices in a mesh: sp: 64 (over z, y), tp: 8 (over x, core).
Axes of the slice: x: 4, y: 8, z: 8, core: 2. Of those that a mesh axis runs over, the one named last changes fastest.
Arguments:
- tokens: bfloat16 [12288, 4096], P('sp'), may hold values from -6 to 6
- norm_gain: float32 [4096], replicated, may hold values from 0.1 to 1.9
- conv_value: bfloat16 [4096, 2048], P('sp', 'tp'), may hold values from -0.09375 to 0.09375
- conv_gate: bfloat16 [4096, 2048], P('sp', 'tp'), may hold values from -0.09375 to 0.09375
- state_feed: bfloat16 [4096, 2048], P('sp', 'tp'), may hold values from -0.09375 to 0.09375
- conv_taps: float32 [31, 2048], P(None, 'tp'), may hold values from -1 to 1
- chan_gain: float32 [2048], replicated, may hold values from 0.1 to 1.9
- chan_shift: float32 [2048], replicated, may hold values from -3 to 3
- conv_project: bfloat16 [2048, 4096], P('sp', 'tp'), may hold values from -0.125 to 0.125
- decay_rate: float32 [128, 64], P('tp'), may hold values from 0.1 to 3
- frequency: float32 [128, 64], P('tp'), may hold values from 0.1 to 3
- input_real: float32 [128, 64, 16], P('tp'), may hold values from -0.01953125 to 0.01953125
- input_imag: float32 [128, 64, 16], P('tp'), may hold values from -0.01953125 to 0.01953125
- output_real: float32 [128, 16, 64], P('tp'), may hold values from -0.5 to 0.5
- output_imag: float32 [128, 16, 64], P('tp'), may hold values from -0.5 to 0.5
- skip_gain: float32 [2048], P('tp'), may hold values from -3 to 3
- state_value: bfloat16 [2048, 4096], P('sp', 'tp'), may hold values from -0.125 to 0.125
- state_gate: bfloat16 [2048, 4096], P('sp', 'tp'), may hold values from -0.125 to 0.125
- initial_state: float32 [2, 128, 64], P(None, 'tp'), may hold values from -5 to 5
Outputs:
- mixer_out: bfloat16 [12288, 4096], P('sp', 'tp')
- final_state: float32 [2, 128, 64], P(None, 'tp')
The draws below stay inside these ranges and needn't reach their ends.
All inputs are finite; a program needn't handle non-finite values.
Results may differ from the reference program's by a relative error of at most 0.0085.
Values may be sent and summed in bfloat16 or wider, within the bound.
No kernel may reach another device: no remote copies, remote signals or barrier semaphores. Data moves between devices by JAX's collectives and lax.ppermute only.
A program may use at most 64 MiB of HBM per device.

```python
import math
import jax
import jax.numpy as jnp
from jax import lax

D = 4096
CH = 2048
GROUP = 16
STATE = 64
KERNEL = 31
TOKENS = 12288
GROUPS = 128


def steps_of(rng, extent, split, low, largest):
    def one(dim, shards_of):
        steps = jax.random.uniform(jax.random.fold_in(jax.random.fold_in(rng, 6), dim), (shards_of,), jnp.float32, low / len(split), largest / len(split))
        return jnp.repeat(jnp.exp(steps), extent[dim] // shards_of).reshape((-1,) + (1,) * (len(extent) - dim - 1))

    factor_of = one(*split[0])
    for cut in split[1:]:
        factor_of = factor_of * one(*cut)
    return factor_of


def bell_draw(rng, extent, scale, bound, split=(), held_as=jnp.bfloat16):
    result = jax.random.normal(rng, extent, jnp.float32) * scale
    if len(split) > 0:
        result = steps_of(rng, extent, split, -0.22, 0.18) * result
    return jnp.clip(result, min=-bound, max=bound).astype(held_as)


def setup_inputs(seed: int = 0) -> dict:
    key_of = jax.random.split(jax.random.key(seed), 20)
    tokens = bell_draw(key_of[0], (TOKENS, D), 1.0, 6.0, ((0, 64),))
    norm_gain = jnp.clip(1.0 + 0.18 * jax.random.normal(key_of[1], (D,), jnp.float32), 0.1, 1.9)
    conv_value = bell_draw(key_of[2], (D, CH), D ** -0.5, 0.09375, ((0, 64), (1, 8)))
    conv_gate = bell_draw(key_of[3], (D, CH), D ** -0.5, 0.09375, ((0, 64), (1, 8)))
    state_feed = bell_draw(key_of[4], (D, CH), D ** -0.5, 0.09375, ((0, 64), (1, 8)))
    conv_taps = bell_draw(key_of[5], (KERNEL, CH), KERNEL ** -0.5, 1.0, ((1, 8),), jnp.float32)
    chan_gain = jnp.clip(1.0 + 0.18 * jax.random.normal(key_of[6], (CH,), jnp.float32), 0.1, 1.9)
    chan_shift = bell_draw(key_of[7], (CH,), 0.5, 3.0, (), jnp.float32)
    conv_project = bell_draw(key_of[8], (CH, D), CH ** -0.5, 0.125, ((0, 64), (1, 8)))
    decay_rate = jnp.clip(jnp.exp(math.log(3.0) - 3.4011974 * jax.random.uniform(key_of[9], (GROUPS, STATE), jnp.float32) ** steps_of(key_of[9], (GROUPS, STATE), ((0, 8),), -0.2, 0.2)), 0.1, 3.0)
    frequency = jnp.clip(0.1 + 2.9 * jax.random.uniform(key_of[10], (GROUPS, STATE), jnp.float32) ** steps_of(key_of[10], (GROUPS, STATE), ((0, 8),), -0.2, 0.2), 0.1, 3.0)
    input_real = bell_draw(key_of[11], (GROUPS, STATE, GROUP), (8 * TOKENS) ** -0.5, 0.01953125, ((0, 8),), jnp.float32)
    input_imag = bell_draw(key_of[12], (GROUPS, STATE, GROUP), (8 * TOKENS) ** -0.5, 0.01953125, ((0, 8),), jnp.float32)
    output_real = bell_draw(key_of[13], (GROUPS, GROUP, STATE), (2 * STATE) ** -0.5, 0.5, ((0, 8),), jnp.float32)
    output_imag = bell_draw(key_of[14], (GROUPS, GROUP, STATE), (2 * STATE) ** -0.5, 0.5, ((0, 8),), jnp.float32)
    skip_gain = bell_draw(key_of[15], (CH,), 0.5, 3.0, ((0, 8),), jnp.float32)
    state_value = bell_draw(key_of[16], (CH, D), CH ** -0.5, 0.125, ((0, 64), (1, 8)))
    state_gate = bell_draw(key_of[17], (CH, D), CH ** -0.5, 0.125, ((0, 64), (1, 8)))
    initial_state = bell_draw(key_of[18], (2, GROUPS, STATE), 1.0, 5.0, ((1, 8),), jnp.float32)
    return dict(tokens=tokens, norm_gain=norm_gain, conv_value=conv_value, conv_gate=conv_gate, state_feed=state_feed, conv_taps=conv_taps, chan_gain=chan_gain, chan_shift=chan_shift, conv_project=conv_project, decay_rate=decay_rate, frequency=frequency, input_real=input_real, input_imag=input_imag, output_real=output_real, output_imag=output_imag, skip_gain=skip_gain, state_value=state_value, state_gate=state_gate, initial_state=initial_state)


def reference(tokens, norm_gain, conv_value, conv_gate, state_feed, conv_taps, chan_gain, chan_shift, conv_project, decay_rate, frequency, input_real, input_imag, output_real, output_imag, skip_gain, state_value, state_gate, initial_state):
    highest = lax.Precision.HIGHEST
    floats = tokens.astype(jnp.float32)
    normed = (floats * lax.rsqrt(lax.optimization_barrier(jnp.mean(floats * floats, axis=1, keepdims=True)) + 1e-06) * norm_gain).astype(jnp.bfloat16)
    value_in = jnp.dot(normed, conv_value, preferred_element_type=jnp.float32)
    gate_in = jnp.dot(normed, conv_gate, preferred_element_type=jnp.float32)
    gated_linear = (value_in * jax.nn.sigmoid(gate_in)).astype(jnp.bfloat16)
    kernel = conv_taps.shape[0]
    length = tokens.shape[0]
    padded = jnp.pad(gated_linear.astype(jnp.float32), ((kernel - 1, 0), (0, 0)))
    conv_sum = jnp.zeros(gated_linear.shape, jnp.float32)
    for offset in range(kernel):
        conv_sum = conv_sum + conv_taps[offset] * padded[offset:offset + length]
    conv_out = conv_sum.astype(jnp.bfloat16)
    conv_full = conv_out.astype(jnp.float32)
    row_mean = lax.optimization_barrier(jnp.mean(conv_full, axis=1, keepdims=True))
    centred = conv_full - row_mean
    variance = lax.optimization_barrier(jnp.mean(centred * centred, axis=1, keepdims=True))
    conv_act = jax.nn.silu(centred * lax.rsqrt(variance + 1e-05) * chan_gain + chan_shift).astype(jnp.bfloat16)
    conv_branch = jnp.dot(conv_act, conv_project, preferred_element_type=jnp.float32)
    state_drive = jnp.dot(normed, state_feed, preferred_element_type=jnp.float32).astype(jnp.bfloat16)
    groups, state_size, group_size = input_real.shape
    rate_real = -decay_rate / TOKENS
    magnitude = jnp.exp(rate_real)
    step_real = magnitude * jnp.cos(frequency)
    step_imag = magnitude * jnp.sin(frequency)
    modulus = rate_real * rate_real + frequency * frequency
    lift_real = step_real - 1.0
    factor_real = (lift_real * rate_real + step_imag * frequency) / modulus
    factor_imag = (step_imag * rate_real - lift_real * frequency) / modulus
    drive_real = factor_real[..., None] * input_real - factor_imag[..., None] * input_imag
    drive_imag = factor_real[..., None] * input_imag + factor_imag[..., None] * input_real
    grouped = state_drive.astype(jnp.float32).reshape(length, groups, group_size)

    def advance(carried, token_in):
        prior_real, prior_imag = carried
        pushed_real = jnp.einsum('gph,gh->gp', drive_real, token_in, precision=highest)
        pushed_imag = jnp.einsum('gph,gh->gp', drive_imag, token_in, precision=highest)
        next_real = step_real * prior_real - step_imag * prior_imag + pushed_real
        next_imag = step_real * prior_imag + step_imag * prior_real + pushed_imag
        emitted = jnp.einsum('ghp,gp->gh', output_real, next_real, precision=highest) - jnp.einsum('ghp,gp->gh', output_imag, next_imag, precision=highest)
        return ((next_real, next_imag), emitted)
    (last_real, last_imag), responses = lax.scan(advance, (initial_state[0], initial_state[1]), grouped)
    response = responses.reshape(length, groups * group_size) + skip_gain * state_drive.astype(jnp.float32)
    activated = jax.nn.gelu(response).astype(jnp.bfloat16)
    state_values = jnp.dot(activated, state_value, preferred_element_type=jnp.float32)
    state_gates = jnp.dot(activated, state_gate, preferred_element_type=jnp.float32)
    mixer_out = (conv_branch + state_values * jax.nn.sigmoid(state_gates)).astype(jnp.bfloat16)
    final_state = jnp.stack([last_real, last_imag])
    return (mixer_out, final_state)
```

```python
import functools

import jax
import jax.numpy as jnp
from jax import lax
from jax.experimental import pallas as pl
from jax.experimental.pallas import tpu as pltpu
from jax.sharding import Mesh, PartitionSpec as P

BF = jnp.bfloat16
F32 = jnp.float32
LANES = 128


def rotate(first_real, first_imag, second_real, second_imag):
    return (
        first_real * second_real - first_imag * second_imag,
        first_real * second_imag + first_imag * second_real,
    )


def power_table(base_real, base_imag, exponent, largest):
    result_real = jnp.ones((exponent.shape[0], base_real.shape[0]), F32)
    result_imag = jnp.zeros((exponent.shape[0], base_real.shape[0]), F32)
    square_real, square_imag = (base_real, base_imag)
    for place in range(max(largest, 1).bit_length()):
        chosen = (exponent >> place & 1 == 1)[:, None]
        next_real, next_imag = rotate(result_real, result_imag, square_real, square_imag)
        result_real = jnp.where(chosen, next_real, result_real)
        result_imag = jnp.where(chosen, next_imag, result_imag)
        square_real, square_imag = rotate(square_real, square_imag, square_real, square_imag)
    return (result_real, result_imag)


def first_kernel(
    normed_ref, weights_ref, drive_ref, undo_ref, gated_ref, feed_ref, sums_ref, total_ref, acc_ref, last_ref
):
    step = pl.program_id(0)
    devices, _, width = weights_ref.shape
    rows = 64

    @pl.when(step == 0)
    def _():
        acc_ref[...] = jnp.zeros_like(acc_ref)

    for kind in range(3):
        block = weights_ref[:, kind * rows : (kind + 1) * rows, :].reshape(devices * rows, width)
        acc_ref[:, kind * width : (kind + 1) * width] += jnp.dot(
            normed_ref[...], block, preferred_element_type=F32
        )

    @pl.when(step == pl.num_programs(0) - 1)
    def _():
        length = acc_ref.shape[0]
        gated_ref[...] = (acc_ref[:, :width] * jax.nn.sigmoid(acc_ref[:, width : 2 * width])).astype(BF)
        feed = acc_ref[:, 2 * width :].astype(BF)
        feed_ref[...] = feed
        lower = (
            lax.broadcasted_iota(jnp.int32, (length, length), 0)
            >= lax.broadcasted_iota(jnp.int32, (length, length), 1)
        ).astype(BF)
        chunks = sums_ref.shape[1] // (2 * LANES)
        for at in range(chunks):
            real = slice(2 * at * LANES, (2 * at + 1) * LANES)
            imag = slice((2 * at + 1) * LANES, (2 * at + 2) * LANES)
            both = slice(2 * at * LANES, (2 * at + 2) * LANES)
            pushed = jnp.dot(feed, drive_ref[:, both], preferred_element_type=F32)
            scaled_real, scaled_imag = rotate(
                undo_ref[:, real], undo_ref[:, imag], pushed[:, :LANES], pushed[:, LANES:]
            )
            scaled = jnp.concatenate([scaled_real, scaled_imag], axis=1).astype(BF)
            sums = jnp.dot(lower, scaled, preferred_element_type=F32)
            sums_ref[:, both] = sums
            last_ref[at : at + 1, :] = sums[length - 1 :, :LANES]
            last_ref[chunks + at : chunks + at + 1, :] = sums[length - 1 :, LANES:]
        total_ref[...] = jnp.broadcast_to(last_ref[...][None], total_ref.shape)


def conv_kernel(before_ref, gated_ref, taps_ref, out_ref, pad_ref):
    length, width = gated_ref.shape
    lead = before_ref.shape[0]
    taps = taps_ref.shape[0]
    pad_ref[:lead] = before_ref[...].astype(F32)
    pad_ref[lead:] = gated_ref[...].astype(F32)
    for col in range(width // LANES):
        cols = slice(col * LANES, (col + 1) * LANES)
        acc = jnp.zeros((length, LANES), F32)
        for tap in range(taps):
            start = lead - (taps - 1) + tap
            acc = acc + taps_ref[tap : tap + 1, cols] * pad_ref[start : start + length, cols]
        rounded = acc.astype(BF)
        for copy in range(out_ref.shape[0]):
            out_ref[copy, :, cols] = rounded


def second_kernel(
    totals_ref, lead_ref, tail_ref, ends_ref, power_ref, sums_ref, mix_ref, feed_ref, skip_ref, out_ref, final_ref
):
    chunks = final_ref.shape[0] // 2
    total_real, total_imag = (totals_ref[:, :chunks, :], totals_ref[:, chunks:, :])
    lead_real, lead_imag = rotate(lead_ref[:, :chunks, :], lead_ref[:, chunks:, :], total_real, total_imag)
    entry_real = ends_ref[0, :chunks] + jnp.sum(lead_real, axis=0)
    entry_imag = ends_ref[0, chunks:] + jnp.sum(lead_imag, axis=0)
    tail_real, tail_imag = rotate(tail_ref[:, :chunks, :], tail_ref[:, chunks:, :], total_real, total_imag)
    final_ref[:chunks] = ends_ref[1, :chunks] + jnp.sum(tail_real, axis=0)
    final_ref[chunks:] = ends_ref[1, chunks:] + jnp.sum(tail_imag, axis=0)
    feed = feed_ref[...].astype(F32)
    response = skip_ref[...] * feed
    for at in range(chunks):
        real = slice(2 * at * LANES, (2 * at + 1) * LANES)
        imag = slice((2 * at + 1) * LANES, (2 * at + 2) * LANES)
        both = slice(2 * at * LANES, (2 * at + 2) * LANES)
        state_real, state_imag = rotate(
            power_ref[:, real],
            power_ref[:, imag],
            sums_ref[:, real] + entry_real[at : at + 1],
            sums_ref[:, imag] + entry_imag[at : at + 1],
        )
        states = jnp.concatenate([state_real, state_imag], axis=1).astype(BF)
        response = response + jnp.dot(states, mix_ref[both, :], preferred_element_type=F32)
    activated = jax.nn.gelu(response).astype(BF)
    for copy in range(out_ref.shape[0]):
        out_ref[copy] = activated


def last_kernel(conv_ref, act_ref, weights_ref, gain_ref, shift_ref, out_ref, acc_ref, mean_ref, scale_ref):
    step = pl.program_id(0)
    blocks, length, width = conv_ref.shape
    devices = weights_ref.shape[0]
    rows = 32

    @pl.when(step == 0)
    def _():
        acc_ref[...] = jnp.zeros_like(acc_ref)
        channels = blocks * width
        total = jnp.zeros((length, width), F32)
        for at in range(blocks):
            total = total + conv_ref[at].astype(F32)
        mean = jnp.sum(total, axis=1, keepdims=True) / channels
        spread = jnp.zeros((length, width), F32)
        for at in range(blocks):
            centred = conv_ref[at].astype(F32) - mean
            spread = spread + centred * centred
        variance = jnp.sum(spread, axis=1, keepdims=True) / channels
        mean_ref[...] = jnp.broadcast_to(mean, mean_ref.shape)
        scale_ref[...] = jnp.broadcast_to(lax.rsqrt(variance + 1e-05), scale_ref.shape)

    centred = conv_ref[step].astype(F32) - mean_ref[...]
    conv_act = jax.nn.silu(centred * scale_ref[...] * gain_ref[0] + shift_ref[0]).astype(BF)
    activated = act_ref[0]
    for part in range(6):
        block = weights_ref[:, part * rows : (part + 1) * rows, :].reshape(devices * rows, width)
        acc_ref[:, part * width : (part + 1) * width] += jnp.dot(
            conv_act if part < 2 else activated, block, preferred_element_type=F32
        )

    @pl.when(step == pl.num_programs(0) - 1)
    def _():
        columns = 2 * width
        out_ref[...] = (
            acc_ref[:, :columns]
            + acc_ref[:, columns : 2 * columns] * jax.nn.sigmoid(acc_ref[:, 2 * columns :])
        ).astype(BF)


def whole(shape):
    return pl.BlockSpec(shape, lambda *_: (0,) * len(shape))


def packed(real, imag):
    n, s = real.shape
    both = jnp.stack([real.reshape(n, s // LANES, LANES), imag.reshape(n, s // LANES, LANES)], axis=2)
    return both.reshape(n, 2 * s)


def rows_of(real, imag):
    n, s = real.shape
    return jnp.concatenate([real.reshape(n, s // LANES, LANES), imag.reshape(n, s // LANES, LANES)], axis=1)


def local(
    tokens,
    norm_gain,
    conv_value,
    conv_gate,
    state_feed,
    conv_taps,
    chan_gain,
    chan_shift,
    conv_project,
    decay_rate,
    frequency,
    input_real,
    input_imag,
    output_real,
    output_imag,
    skip_gain,
    state_value,
    state_gate,
    initial_state,
):
    seq_devices = lax.axis_size("sp")
    tp_devices = lax.axis_size("tp")
    position = lax.axis_index("sp")
    length, model = tokens.shape
    rows_in, width = conv_value.shape
    rows_out, columns = conv_project.shape
    shard = jnp.concatenate(
        [conv_value, conv_gate, state_feed]
        + [w[:, at : at + width] for w in (conv_project, state_value, state_gate) for at in (0, width)],
        axis=0,
    )
    gathered = lax.all_gather(shard, "sp", axis=0, tiled=False)

    floats = tokens.astype(F32)
    normed = (
        floats * lax.rsqrt(jnp.mean(floats * floats, axis=1, keepdims=True) + 1e-06) * norm_gain
    ).astype(BF)

    groups, state_size, group_size = input_real.shape
    flat = groups * state_size
    total_tokens = length * seq_devices
    rate_real = -decay_rate / total_tokens
    magnitude = jnp.exp(rate_real)
    step_real = magnitude * jnp.cos(frequency)
    step_imag = magnitude * jnp.sin(frequency)
    modulus = rate_real * rate_real + frequency * frequency
    lift_real = step_real - 1.0
    factor_real = (lift_real * rate_real + step_imag * frequency) / modulus
    factor_imag = (step_imag * rate_real - lift_real * frequency) / modulus
    drive_real = factor_real[..., None] * input_real - factor_imag[..., None] * input_imag
    drive_imag = factor_real[..., None] * input_imag + factor_imag[..., None] * input_real

    def spread(blocks):
        g, a, b = blocks.shape
        row = lax.broadcasted_iota(jnp.int32, (g * a, g * b), 0) // a
        col = lax.broadcasted_iota(jnp.int32, (g * a, g * b), 1) // b
        return jnp.where(row == col, jnp.tile(blocks.reshape(g * a, b), (1, g)), 0.0)

    drive = packed(
        spread(jnp.swapaxes(drive_real, 1, 2)), spread(jnp.swapaxes(drive_imag, 1, 2))
    ).astype(BF)
    mix = jnp.swapaxes(packed(
        spread(output_real), -spread(output_imag)
    ), 0, 1).astype(BF)

    base_real = step_real.reshape(flat)
    base_imag = step_imag.reshape(flat)
    square_size = base_real * base_real + base_imag * base_imag
    counted = lax.iota(jnp.int32, length) + 1
    power_real, power_imag = power_table(base_real, base_imag, counted, length)
    undo_real, undo_imag = power_table(base_real / square_size, -base_imag / square_size, counted, length)
    span_real, span_imag = (power_real[-1], power_imag[-1])
    device_ids = lax.iota(jnp.int32, seq_devices)
    lag = position - device_ids
    lead_real, lead_imag = power_table(span_real, span_imag, jnp.maximum(lag, 0), seq_devices)
    earlier = (lag > 0).astype(F32)[:, None]
    lead = rows_of(lead_real * earlier, lead_imag * earlier)
    tail = rows_of(*power_table(span_real, span_imag, seq_devices - device_ids, seq_devices))
    ends = rows_of(
        *rotate(
            *power_table(span_real, span_imag, jnp.stack([position, jnp.int32(seq_devices)]), seq_devices),
            initial_state[0].reshape(1, flat),
            initial_state[1].reshape(1, flat),
        )
    )
    power = packed(power_real, power_imag)
    undo = packed(undo_real, undo_imag)
    chunks = flat // LANES

    steps = 8
    per_step = seq_devices // steps
    gated, feed, sums, total = pl.pallas_call(
        first_kernel,
        grid=(steps,),
        in_specs=[
            pl.BlockSpec((length, model // steps), lambda k: (0, k)),
            pl.BlockSpec((per_step, 3 * rows_in, width), lambda k: (k, 0, 0)),
            whole(drive.shape),
            whole(undo.shape),
        ],
        out_specs=[
            whole((length, width)),
            whole((length, width)),
            whole((length, 2 * flat)),
            whole((seq_devices, 2 * chunks, LANES)),
        ],
        out_shape=[
            jax.ShapeDtypeStruct((length, width), BF),
            jax.ShapeDtypeStruct((length, width), BF),
            jax.ShapeDtypeStruct((length, 2 * flat), F32),
            jax.ShapeDtypeStruct((seq_devices, 2 * chunks, LANES), F32),
        ],
        scratch_shapes=[pltpu.VMEM((length, 3 * width), F32), pltpu.VMEM((2 * chunks, LANES), F32)],
        name="first",
    )(normed, gathered, drive, undo)

    taps = conv_taps.shape[0]
    halo = (taps - 1 + 15) // 16 * 16
    before = lax.ppermute(
        gated[length - halo :], "sp", [(source, source + 1) for source in range(seq_devices - 1)]
    )
    totals = lax.all_to_all(total, "sp", 0, 0, tiled=True)
    conv_copies = pl.pallas_call(
        conv_kernel,
        out_shape=jax.ShapeDtypeStruct((tp_devices, length, width), BF),
        scratch_shapes=[pltpu.VMEM((halo + length, width), F32)],
        name="conv",
    )(before, gated, conv_taps)
    conv_rows = lax.all_to_all(conv_copies, "tp", 0, 0, tiled=True)

    act_copies, final = pl.pallas_call(
        second_kernel,
        out_shape=[
            jax.ShapeDtypeStruct((tp_devices, length, width), BF),
            jax.ShapeDtypeStruct((2 * chunks, LANES), F32),
        ],
        name="second",
    )(totals, lead, tail, ends, power, sums, mix, feed, skip_gain.reshape(1, width))
    final_state = final.reshape(2, groups, state_size)
    act_rows = lax.all_to_all(act_copies, "tp", 0, 0, tiled=True)

    mixer_out = pl.pallas_call(
        last_kernel,
        grid=(tp_devices,),
        in_specs=[
            whole((tp_devices, length, width)),
            pl.BlockSpec((1, length, width), lambda k: (k, 0, 0)),
            pl.BlockSpec((seq_devices // tp_devices, 3 * rows_in, width), lambda k: (k, 1, 0)),
            pl.BlockSpec((1, 1, width), lambda k: (k, 0, 0)),
            pl.BlockSpec((1, 1, width), lambda k: (k, 0, 0)),
        ],
        out_specs=whole((length, columns)),
        out_shape=jax.ShapeDtypeStruct((length, columns), BF),
        scratch_shapes=[
            pltpu.VMEM((length, 6 * width), F32),
            pltpu.VMEM((length, width), F32),
            pltpu.VMEM((length, width), F32),
        ],
        name="last",
    )(
        conv_rows,
        act_rows,
        gathered,
        chan_gain.reshape(tp_devices, 1, width),
        chan_shift.reshape(tp_devices, 1, width),
    )
    return (mixer_out, final_state)


def solution(mesh):
    in_specs = (
        P("sp", None),
        P(),
        P("sp", "tp"),
        P("sp", "tp"),
        P("sp", "tp"),
        P(None, "tp"),
        P(),
        P(),
        P("sp", "tp"),
        P("tp", None),
        P("tp", None),
        P("tp", None, None),
        P("tp", None, None),
        P("tp", None, None),
        P("tp", None, None),
        P("tp"),
        P("sp", "tp"),
        P("sp", "tp"),
        P(None, "tp", None),
    )
    out_specs = (P("sp", "tp"), P(None, "tp", None))
    return jax.shard_map(local, mesh=mesh, in_specs=in_specs, out_specs=out_specs, check_vma=False)
```

```python
import functools

import jax
import jax.numpy as jnp
from jax import lax
from jax.experimental import pallas as pl
from jax.experimental.pallas import tpu as pltpu
from jax.sharding import Mesh, PartitionSpec as P

BF = jnp.bfloat16
F32 = jnp.float32
LANES = 128
CHUNK = 256


def rotate(first_real, first_imag, second_real, second_imag):
    return (
        first_real * second_real - first_imag * second_imag,
        first_real * second_imag + first_imag * second_real,
    )


def power_table(base_real, base_imag, exponent, largest):
    result_real = jnp.ones((exponent.shape[0], base_real.shape[0]), F32)
    result_imag = jnp.zeros((exponent.shape[0], base_real.shape[0]), F32)
    square_real, square_imag = (base_real, base_imag)
    for place in range(max(largest, 1).bit_length()):
        chosen = (exponent >> place & 1 == 1)[:, None]
        next_real, next_imag = rotate(result_real, result_imag, square_real, square_imag)
        result_real = jnp.where(chosen, next_real, result_real)
        result_imag = jnp.where(chosen, next_imag, result_imag)
        square_real, square_imag = rotate(square_real, square_imag, square_real, square_imag)
    return (result_real, result_imag)


def pack_kernel(*refs):
    out_ref = refs[-1]
    width = out_ref.shape[1]
    at = 0
    for ref in refs[:-1]:
        for col in range(0, ref.shape[1], width):
            out_ref[at : at + ref.shape[0]] = ref[:, col : col + width]
            at += ref.shape[0]


def first_kernel(
    normed_ref,
    weights_ref,
    drive_real_ref,
    drive_imag_ref,
    undo_real_ref,
    undo_imag_ref,
    gated_ref,
    feed_ref,
    sums_real_ref,
    sums_imag_ref,
    total_ref,
    acc_ref,
    last_ref,
):
    step = pl.program_id(0)
    devices, _, width = weights_ref.shape
    rows = weights_ref.shape[1] // 3

    @pl.when(step == 0)
    def _():
        acc_ref[...] = jnp.zeros_like(acc_ref)

    for kind in range(3):
        block = weights_ref[:, kind * rows : (kind + 1) * rows, :].reshape(devices * rows, width)
        acc_ref[:, kind * width : (kind + 1) * width] += jnp.dot(
            normed_ref[...], block, preferred_element_type=F32
        )

    @pl.when(step == pl.num_programs(0) - 1)
    def _():
        length = acc_ref.shape[0]
        gated_ref[...] = (acc_ref[:, :width] * jax.nn.sigmoid(acc_ref[:, width : 2 * width])).astype(BF)
        feed = acc_ref[:, 2 * width :].astype(BF)
        feed_ref[...] = feed
        lower = (
            lax.broadcasted_iota(jnp.int32, (length, length), 0)
            >= lax.broadcasted_iota(jnp.int32, (length, length), 1)
        ).astype(BF)
        flat = sums_real_ref.shape[1]
        half = last_ref.shape[0] // 2
        for at in range(0, flat, CHUNK):
            cols = slice(at, at + CHUNK)
            pushed_real = jnp.dot(feed, drive_real_ref[:, cols], preferred_element_type=F32)
            pushed_imag = jnp.dot(feed, drive_imag_ref[:, cols], preferred_element_type=F32)
            scaled = rotate(undo_real_ref[:, cols], undo_imag_ref[:, cols], pushed_real, pushed_imag)
            for part, ref in enumerate((sums_real_ref, sums_imag_ref)):
                sums = jnp.dot(lower, scaled[part].astype(BF), preferred_element_type=F32)
                ref[:, cols] = sums
                for lane in range(0, CHUNK, LANES):
                    row = part * half + (at + lane) // LANES
                    last_ref[row : row + 1, :] = sums[length - 1 :, lane : lane + LANES]
        total_ref[...] = jnp.broadcast_to(last_ref[...][None], total_ref.shape)


def conv_kernel(before_ref, gated_ref, taps_ref, out_ref, pad_ref):
    length, width = gated_ref.shape
    lead = before_ref.shape[0]
    taps = taps_ref.shape[0]
    pad_ref[:lead] = before_ref[...].astype(F32)
    pad_ref[lead:] = gated_ref[...].astype(F32)
    for col in range(width // LANES):
        cols = slice(col * LANES, (col + 1) * LANES)
        acc = jnp.zeros((length, LANES), F32)
        for tap in range(taps):
            start = lead - (taps - 1) + tap
            acc = acc + taps_ref[tap : tap + 1, cols] * pad_ref[start : start + length, cols]
        rounded = acc.astype(BF)
        for copy in range(out_ref.shape[0]):
            out_ref[copy, :, cols] = rounded


def second_kernel(
    totals_ref,
    lead_ref,
    tail_ref,
    ends_ref,
    power_real_ref,
    power_imag_ref,
    sums_real_ref,
    sums_imag_ref,
    mix_real_ref,
    mix_imag_ref,
    feed_ref,
    skip_ref,
    out_ref,
    final_ref,
    entry_ref,
):
    half = final_ref.shape[0] // 2
    total_real, total_imag = (totals_ref[:, :half, :], totals_ref[:, half:, :])
    lead_real, lead_imag = rotate(lead_ref[:, :half, :], lead_ref[:, half:, :], total_real, total_imag)
    entry_ref[:half] = ends_ref[0, :half] + jnp.sum(lead_real, axis=0)
    entry_ref[half:] = ends_ref[0, half:] + jnp.sum(lead_imag, axis=0)
    tail_real, tail_imag = rotate(tail_ref[:, :half, :], tail_ref[:, half:, :], total_real, total_imag)
    final_ref[:half] = ends_ref[1, :half] + jnp.sum(tail_real, axis=0)
    final_ref[half:] = ends_ref[1, half:] + jnp.sum(tail_imag, axis=0)
    response = skip_ref[...] * feed_ref[...].astype(F32)
    for at in range(0, sums_real_ref.shape[1], CHUNK):
        cols = slice(at, at + CHUNK)
        rows = range(at // LANES, (at + CHUNK) // LANES)
        entry_real = jnp.concatenate([entry_ref[row : row + 1] for row in rows], axis=1)
        entry_imag = jnp.concatenate([entry_ref[half + row : half + row + 1] for row in rows], axis=1)
        state_real, state_imag = rotate(
            power_real_ref[:, cols],
            power_imag_ref[:, cols],
            sums_real_ref[:, cols] + entry_real,
            sums_imag_ref[:, cols] + entry_imag,
        )
        response = response + jnp.dot(state_real.astype(BF), mix_real_ref[cols, :], preferred_element_type=F32)
        response = response + jnp.dot(state_imag.astype(BF), mix_imag_ref[cols, :], preferred_element_type=F32)
    activated = jax.nn.gelu(response).astype(BF)
    for copy in range(out_ref.shape[0]):
        out_ref[copy] = activated


def branch_kernel(conv_ref, weights_ref, gain_ref, shift_ref, out_ref, mean_ref, scale_ref):
    step = pl.program_id(0)
    blocks, length, width = conv_ref.shape
    devices = weights_ref.shape[0]
    rows = weights_ref.shape[1] // 2

    @pl.when(step == 0)
    def _():
        out_ref[...] = jnp.zeros_like(out_ref)
        channels = blocks * width
        total = jnp.zeros((length, width), F32)
        for at in range(blocks):
            total = total + conv_ref[at].astype(F32)
        mean = jnp.sum(total, axis=1, keepdims=True) / channels
        spread = jnp.zeros((length, width), F32)
        for at in range(blocks):
            centred = conv_ref[at].astype(F32) - mean
            spread = spread + centred * centred
        variance = jnp.sum(spread, axis=1, keepdims=True) / channels
        mean_ref[...] = jnp.broadcast_to(mean, mean_ref.shape)
        scale_ref[...] = jnp.broadcast_to(lax.rsqrt(variance + 1e-05), scale_ref.shape)

    centred = conv_ref[step].astype(F32) - mean_ref[...]
    conv_act = jax.nn.silu(centred * scale_ref[...] * gain_ref[0] + shift_ref[0]).astype(BF)
    for part in range(2):
        block = weights_ref[:, part * rows : (part + 1) * rows, :].reshape(devices * rows, width)
        out_ref[:, part * width : (part + 1) * width] += jnp.dot(conv_act, block, preferred_element_type=F32)


def last_kernel(act_ref, value_ref, gate_ref, branch_ref, out_ref, acc_ref):
    step = pl.program_id(0)
    width = act_ref.shape[2]
    devices = value_ref.shape[0]
    rows = value_ref.shape[1] // 2

    @pl.when(step == 0)
    def _():
        acc_ref[...] = jnp.zeros_like(acc_ref)

    activated = act_ref[0]
    for part in range(4):
        ref = (value_ref, value_ref, gate_ref, gate_ref)[part]
        at = part % 2 * rows
        block = ref[:, at : at + rows, :].reshape(devices * rows, width)
        acc_ref[:, part * width : (part + 1) * width] += jnp.dot(
            activated, block, preferred_element_type=F32
        )

    @pl.when(step == pl.num_programs(0) - 1)
    def _():
        columns = 2 * width
        out_ref[...] = (
            branch_ref[...] + acc_ref[:, :columns] * jax.nn.sigmoid(acc_ref[:, columns:])
        ).astype(BF)


def whole(shape):
    return pl.BlockSpec(shape, lambda *_: (0,) * len(shape))


def spread(blocks, size):
    total, b = blocks.shape
    wide = total // size * b
    pick = lax.broadcasted_iota(jnp.int32, (b, wide), 1) % b == lax.broadcasted_iota(jnp.int32, (b, wide), 0)
    tiled = jnp.dot(blocks.astype(BF), pick.astype(BF), preferred_element_type=F32)
    row = lax.broadcasted_iota(jnp.int32, tiled.shape, 0) // size
    col = lax.broadcasted_iota(jnp.int32, tiled.shape, 1) // b
    return jnp.where(row == col, tiled, 0.0).astype(BF)


def rows_of(real, imag):
    n, s = real.shape
    return jnp.concatenate([real.reshape(n, s // LANES, LANES), imag.reshape(n, s // LANES, LANES)], axis=1)


def local(
    tokens,
    norm_gain,
    conv_value,
    conv_gate,
    state_feed,
    conv_taps,
    chan_gain,
    chan_shift,
    conv_project,
    decay_rate,
    frequency,
    input_real,
    input_imag,
    output_real,
    output_imag,
    skip_gain,
    state_value,
    state_gate,
    initial_state,
):
    seq_devices = lax.axis_size("sp")
    tp_devices = lax.axis_size("tp")
    position = lax.axis_index("sp")
    length, model = tokens.shape
    rows_in, width = conv_value.shape
    rows_out, columns = conv_project.shape
    shard = pl.pallas_call(
        pack_kernel,
        out_shape=jax.ShapeDtypeStruct((3 * rows_in + 3 * rows_out * (columns // width), width), BF),
        name="pack",
    )(conv_value, conv_gate, state_feed, conv_project, state_value, state_gate)
    gathered = lax.all_gather(shard, "sp", axis=0, tiled=False)

    floats = tokens.astype(F32)
    normed = (
        floats * lax.rsqrt(jnp.mean(floats * floats, axis=1, keepdims=True) + 1e-06) * norm_gain
    ).astype(BF)

    groups, state_size, group_size = input_real.shape
    flat = groups * state_size
    total_tokens = length * seq_devices
    rate_real = -decay_rate / total_tokens
    magnitude = jnp.exp(rate_real)
    step_real = magnitude * jnp.cos(frequency)
    step_imag = magnitude * jnp.sin(frequency)
    modulus = rate_real * rate_real + frequency * frequency
    lift_real = step_real - 1.0
    factor_real = (lift_real * rate_real + step_imag * frequency) / modulus
    factor_imag = (step_imag * rate_real - lift_real * frequency) / modulus
    drive_real = factor_real[..., None] * input_real - factor_imag[..., None] * input_imag
    drive_imag = factor_real[..., None] * input_imag + factor_imag[..., None] * input_real

    drive_real = spread(jnp.swapaxes(drive_real, 1, 2).reshape(groups * group_size, state_size), group_size)
    drive_imag = spread(jnp.swapaxes(drive_imag, 1, 2).reshape(groups * group_size, state_size), group_size)
    mix_real = spread(jnp.swapaxes(output_real, 1, 2).reshape(flat, group_size), state_size)
    mix_imag = spread(jnp.swapaxes(-output_imag, 1, 2).reshape(flat, group_size), state_size)

    base_real = step_real.reshape(flat)
    base_imag = step_imag.reshape(flat)
    square_size = base_real * base_real + base_imag * base_imag

    def powers(real, imag):
        low = power_table(real, imag, lax.iota(jnp.int32, 8) + 1, 8)
        high = power_table(real, imag, lax.iota(jnp.int32, length // 8) * 8, length)
        table = rotate(high[0][:, None], high[1][:, None], low[0][None], low[1][None])
        return tuple(part.reshape(length, flat) for part in table)

    power_real, power_imag = powers(base_real, base_imag)
    undo_real, undo_imag = powers(base_real / square_size, -base_imag / square_size)
    span_real, span_imag = (power_real[-1], power_imag[-1])
    device_ids = lax.iota(jnp.int32, seq_devices)
    lag = position - device_ids
    lead_real, lead_imag = power_table(span_real, span_imag, jnp.maximum(lag, 0), seq_devices)
    earlier = (lag > 0).astype(F32)[:, None]
    lead = rows_of(lead_real * earlier, lead_imag * earlier)
    tail = rows_of(*power_table(span_real, span_imag, seq_devices - device_ids, seq_devices))
    ends = rows_of(
        *rotate(
            *power_table(span_real, span_imag, jnp.stack([position, jnp.int32(seq_devices)]), seq_devices),
            initial_state[0].reshape(1, flat),
            initial_state[1].reshape(1, flat),
        )
    )
    (
        normed, drive_real, drive_imag, mix_real, mix_imag, power_real, power_imag, undo_real, undo_imag, lead, tail, ends
    ) = lax.optimization_barrier((
        normed, drive_real, drive_imag, mix_real, mix_imag, power_real, power_imag, undo_real, undo_imag, lead, tail, ends
    ))
    chunks = flat // LANES

    steps = 8
    per_step = seq_devices // steps
    gated, feed, sums_real, sums_imag, total = pl.pallas_call(
        first_kernel,
        grid=(steps,),
        in_specs=[
            pl.BlockSpec((length, model // steps), lambda k: (0, k)),
            pl.BlockSpec((per_step, 3 * rows_in, width), lambda k: (k, 0, 0)),
            whole(drive_real.shape),
            whole(drive_imag.shape),
            whole(undo_real.shape),
            whole(undo_imag.shape),
        ],
        out_specs=[
            whole((length, width)),
            whole((length, width)),
            whole((length, flat)),
            whole((length, flat)),
            whole((seq_devices, 2 * chunks, LANES)),
        ],
        out_shape=[
            jax.ShapeDtypeStruct((length, width), BF),
            jax.ShapeDtypeStruct((length, width), BF),
            jax.ShapeDtypeStruct((length, flat), F32),
            jax.ShapeDtypeStruct((length, flat), F32),
            jax.ShapeDtypeStruct((seq_devices, 2 * chunks, LANES), F32),
        ],
        scratch_shapes=[pltpu.VMEM((length, 3 * width), F32), pltpu.VMEM((2 * chunks, LANES), F32)],
        name="first",
    )(normed, gathered, drive_real, drive_imag, undo_real, undo_imag)

    taps = conv_taps.shape[0]
    halo = (taps - 1 + 15) // 16 * 16
    before = lax.ppermute(
        gated[length - halo :], "sp", [(source, source + 1) for source in range(seq_devices - 1)]
    )
    totals = lax.all_to_all(total, "sp", 0, 0, tiled=True)
    conv_copies = pl.pallas_call(
        conv_kernel,
        out_shape=jax.ShapeDtypeStruct((tp_devices, length, width), BF),
        scratch_shapes=[pltpu.VMEM((halo + length, width), F32)],
        name="conv",
    )(before, gated, conv_taps)
    conv_rows = lax.all_to_all(conv_copies, "tp", 0, 0, tiled=True)

    act_copies, final = pl.pallas_call(
        second_kernel,
        out_shape=[
            jax.ShapeDtypeStruct((tp_devices, length, width), BF),
            jax.ShapeDtypeStruct((2 * chunks, LANES), F32),
        ],
        scratch_shapes=[pltpu.VMEM((2 * chunks, LANES), F32)],
        name="second",
    )(
        totals, lead, tail, ends, power_real, power_imag, sums_real, sums_imag, mix_real, mix_imag, feed,
        skip_gain.reshape(1, width),
    )
    final_state = final.reshape(2, groups, state_size)
    act_rows = lax.all_to_all(act_copies, "tp", 0, 0, tiled=True)

    per_block = seq_devices // tp_devices
    first_out = 3 * rows_in // (2 * rows_out)
    branch = pl.pallas_call(
        branch_kernel,
        grid=(tp_devices,),
        in_specs=[
            whole((tp_devices, length, width)),
            pl.BlockSpec((per_block, 2 * rows_out, width), lambda k: (k, first_out, 0)),
            pl.BlockSpec((1, 1, width), lambda k: (k, 0, 0)),
            pl.BlockSpec((1, 1, width), lambda k: (k, 0, 0)),
        ],
        out_specs=whole((length, columns)),
        out_shape=jax.ShapeDtypeStruct((length, columns), F32),
        scratch_shapes=[pltpu.VMEM((length, width), F32), pltpu.VMEM((length, width), F32)],
        name="branch",
    )(
        conv_rows,
        gathered,
        chan_gain.reshape(tp_devices, 1, width),
        chan_shift.reshape(tp_devices, 1, width),
    )
    mixer_out = pl.pallas_call(
        last_kernel,
        grid=(tp_devices,),
        in_specs=[
            pl.BlockSpec((1, length, width), lambda k: (k, 0, 0)),
            pl.BlockSpec((per_block, 2 * rows_out, width), lambda k: (k, first_out + 1, 0)),
            pl.BlockSpec((per_block, 2 * rows_out, width), lambda k: (k, first_out + 2, 0)),
            whole((length, columns)),
        ],
        out_specs=whole((length, columns)),
        out_shape=jax.ShapeDtypeStruct((length, columns), BF),
        scratch_shapes=[pltpu.VMEM((length, 4 * width), F32)],
        name="last",
    )(act_rows, gathered, gathered, branch)
    return (mixer_out, final_state)


def solution(mesh):
    in_specs = (
        P("sp", None),
        P(),
        P("sp", "tp"),
        P("sp", "tp"),
        P("sp", "tp"),
        P(None, "tp"),
        P(),
        P(),
        P("sp", "tp"),
        P("tp", None),
        P("tp", None),
        P("tp", None, None),
        P("tp", None, None),
        P("tp", None, None),
        P("tp", None, None),
        P("tp"),
        P("sp", "tp"),
        P("sp", "tp"),
        P(None, "tp", None),
    )
    out_specs = (P("sp", "tp"), P(None, "tp", None))
    return jax.shard_map(local, mesh=mesh, in_specs=in_specs, out_specs=out_specs, check_vma=False)
```

```python
import jax
import jax.numpy as jnp
from jax import lax
from jax.experimental import pallas as pl
from jax.experimental.pallas import tpu as pltpu
from jax.sharding import PartitionSpec as P

BF = jnp.bfloat16
F32 = jnp.float32
LANES = 128
CHUNK = 256


def rotate(first_real, first_imag, second_real, second_imag):
    return (
        first_real * second_real - first_imag * second_imag,
        first_real * second_imag + first_imag * second_real,
    )


def power_table(base_real, base_imag, exponent, largest):
    result_real = jnp.ones((exponent.shape[0], base_real.shape[0]), F32)
    result_imag = jnp.zeros((exponent.shape[0], base_real.shape[0]), F32)
    square_real, square_imag = (base_real, base_imag)
    for place in range(max(largest, 1).bit_length()):
        chosen = (exponent >> place & 1 == 1)[:, None]
        next_real, next_imag = rotate(result_real, result_imag, square_real, square_imag)
        result_real = jnp.where(chosen, next_real, result_real)
        result_imag = jnp.where(chosen, next_imag, result_imag)
        square_real, square_imag = rotate(square_real, square_imag, square_real, square_imag)
    return (result_real, result_imag)


def pack_kernel(*refs):
    out_ref = refs[-1]
    width = out_ref.shape[1]
    at = 0
    for ref in refs[:-1]:
        for col in range(0, ref.shape[1], width):
            out_ref[at : at + ref.shape[0]] = ref[:, col : col + width]
            at += ref.shape[0]


def first_kernel(
    normed_ref,
    weights_ref,
    drive_real_ref,
    drive_imag_ref,
    undo_real_ref,
    undo_imag_ref,
    gated_ref,
    feed_ref,
    sums_real_ref,
    sums_imag_ref,
    total_ref,
    buffer_ref,
    acc_ref,
    last_ref,
    sems,
):
    devices, rows, width = buffer_ref.shape
    rows //= 3
    parts = sems.shape[0]
    per_part = devices // parts

    def fetch(part):
        at = pl.ds(part * per_part, per_part)
        return pltpu.make_async_copy(weights_ref.at[at, pl.ds(0, 3 * rows)], buffer_ref.at[at], sems.at[part])

    for part in range(parts):
        fetch(part).start()
    span = per_part * rows
    for part in range(parts):
        fetch(part).wait()
        for kind in range(3):
            block = buffer_ref[
                part * per_part : (part + 1) * per_part, kind * rows : (kind + 1) * rows, :
            ].reshape(span, width)
            product = jnp.dot(
                normed_ref[:, part * span : (part + 1) * span], block, preferred_element_type=F32
            )
            cols = slice(kind * width, (kind + 1) * width)
            acc_ref[:, cols] = product if part == 0 else acc_ref[:, cols] + product

    length = acc_ref.shape[0]
    feed = acc_ref[:, 2 * width :].astype(BF)
    feed_ref[...] = feed
    lower = (
        lax.broadcasted_iota(jnp.int32, (length, length), 0)
        >= lax.broadcasted_iota(jnp.int32, (length, length), 1)
    ).astype(BF)
    flat = sums_real_ref.shape[1]
    half = last_ref.shape[0] // 2
    for at in range(0, flat, CHUNK):
        cols = slice(at, at + CHUNK)
        pushed_real = jnp.dot(feed, drive_real_ref[:, cols], preferred_element_type=F32)
        pushed_imag = jnp.dot(feed, drive_imag_ref[:, cols], preferred_element_type=F32)
        scaled = rotate(undo_real_ref[:, cols], undo_imag_ref[:, cols], pushed_real, pushed_imag)
        for part, ref in enumerate((sums_real_ref, sums_imag_ref)):
            sums = jnp.dot(lower, scaled[part].astype(BF), preferred_element_type=F32)
            ref[:, cols] = sums
            for lane in range(0, CHUNK, LANES):
                row = part * half + (at + lane) // LANES
                last_ref[row : row + 1, :] = sums[length - 1 :, lane : lane + LANES]
    total_ref[...] = jnp.broadcast_to(last_ref[...][None], total_ref.shape)
    gated_ref[...] = (acc_ref[:, :width] * jax.nn.sigmoid(acc_ref[:, width : 2 * width])).astype(BF)


def conv_kernel(before_ref, gated_ref, taps_ref, out_ref, pad_ref):
    length, width = gated_ref.shape
    lead = before_ref.shape[0]
    taps = taps_ref.shape[0]
    pad_ref[:lead] = before_ref[...].astype(F32)
    pad_ref[lead:] = gated_ref[...].astype(F32)
    for col in range(width // LANES):
        cols = slice(col * LANES, (col + 1) * LANES)
        acc = jnp.zeros((length, LANES), F32)
        for tap in range(taps):
            start = lead - (taps - 1) + tap
            acc = acc + taps_ref[tap : tap + 1, cols] * pad_ref[start : start + length, cols]
        out_ref[:, cols] = acc.astype(BF)


def second_kernel(
    totals_ref,
    lead_ref,
    tail_ref,
    ends_ref,
    power_real_ref,
    power_imag_ref,
    sums_real_ref,
    sums_imag_ref,
    mix_real_ref,
    mix_imag_ref,
    feed_ref,
    skip_ref,
    conv_ref,
    out_ref,
    final_ref,
    entry_ref,
):
    half = final_ref.shape[0] // 2
    total_real, total_imag = (totals_ref[:, :half, :], totals_ref[:, half:, :])
    lead_real, lead_imag = rotate(lead_ref[:, :half, :], lead_ref[:, half:, :], total_real, total_imag)
    entry_ref[:half] = ends_ref[0, :half] + jnp.sum(lead_real, axis=0)
    entry_ref[half:] = ends_ref[0, half:] + jnp.sum(lead_imag, axis=0)
    tail_real, tail_imag = rotate(tail_ref[:, :half, :], tail_ref[:, half:, :], total_real, total_imag)
    final_ref[:half] = ends_ref[1, :half] + jnp.sum(tail_real, axis=0)
    final_ref[half:] = ends_ref[1, half:] + jnp.sum(tail_imag, axis=0)
    response = skip_ref[...] * feed_ref[...].astype(F32)
    for at in range(0, sums_real_ref.shape[1], CHUNK):
        cols = slice(at, at + CHUNK)
        rows = range(at // LANES, (at + CHUNK) // LANES)
        entry_real = jnp.concatenate([entry_ref[row : row + 1] for row in rows], axis=1)
        entry_imag = jnp.concatenate([entry_ref[half + row : half + row + 1] for row in rows], axis=1)
        state_real, state_imag = rotate(
            power_real_ref[:, cols],
            power_imag_ref[:, cols],
            sums_real_ref[:, cols] + entry_real,
            sums_imag_ref[:, cols] + entry_imag,
        )
        response = response + jnp.dot(state_real.astype(BF), mix_real_ref[cols, :], preferred_element_type=F32)
        response = response + jnp.dot(state_imag.astype(BF), mix_imag_ref[cols, :], preferred_element_type=F32)
    activated = jax.nn.gelu(response).astype(BF)
    length = activated.shape[0]
    conv = conv_ref[...]
    for copy in range(out_ref.shape[0]):
        out_ref[copy, :length] = conv
        out_ref[copy, length:] = activated


def last_kernel(rows_ref, weights_ref, gain_ref, shift_ref, out_ref, buffer_ref, act_ref, acc_ref, sems):
    blocks, length, width = rows_ref.shape
    length //= 2
    devices, rows, _ = buffer_ref.shape
    rows //= 6
    parts = sems.shape[0]
    per_part = devices // parts
    per_block = blocks // parts

    def fetch(part):
        at = pl.ds(part * per_part, per_part)
        return pltpu.make_async_copy(
            weights_ref.at[at, pl.ds(6 * rows, 6 * rows)], buffer_ref.at[at], sems.at[part]
        )

    for part in range(parts):
        fetch(part).start()
    channels = blocks * width
    total = jnp.zeros((length, width), F32)
    squares = jnp.zeros((length, width), F32)
    for at in range(blocks):
        total = total + rows_ref[at, :length, :].astype(F32)
    mean = jnp.sum(total, axis=1, keepdims=True) / channels
    for at in range(blocks):
        centred = rows_ref[at, :length, :].astype(F32) - mean
        squares = squares + centred * centred
    scale = lax.rsqrt(jnp.sum(squares, axis=1, keepdims=True) / channels + 1e-05)
    for at in range(blocks):
        centred = rows_ref[at, :length, :].astype(F32) - mean
        cols = slice(at * width, (at + 1) * width)
        act_ref[:, cols] = jax.nn.silu(centred * scale * gain_ref[:, cols] + shift_ref[:, cols]).astype(BF)
    span = per_part * rows
    for part in range(parts):
        fetch(part).wait()
        conv_act = act_ref[:, part * span : (part + 1) * span]
        activated = jnp.concatenate(
            [rows_ref[part * per_block + at, length:, :] for at in range(per_block)], axis=1
        )
        for kind in range(6):
            block = buffer_ref[
                part * per_part : (part + 1) * per_part, kind * rows : (kind + 1) * rows, :
            ].reshape(span, width)
            product = jnp.dot(conv_act if kind < 2 else activated, block, preferred_element_type=F32)
            cols = slice(kind * width, (kind + 1) * width)
            acc_ref[:, cols] = product if part == 0 else acc_ref[:, cols] + product
    columns = 2 * width
    out_ref[...] = (
        acc_ref[:, :columns]
        + acc_ref[:, columns : 2 * columns] * jax.nn.sigmoid(acc_ref[:, 2 * columns :])
    ).astype(BF)


def grant(mib):
    return pltpu.CompilerParams(vmem_limit_bytes=mib << 20)


def whole(shape):
    return pl.BlockSpec(shape, lambda *_: (0,) * len(shape))


def spread(blocks, size):
    total, b = blocks.shape
    wide = total // size * b
    pick = lax.broadcasted_iota(jnp.int32, (b, wide), 1) % b == lax.broadcasted_iota(jnp.int32, (b, wide), 0)
    tiled = jnp.dot(blocks.astype(BF), pick.astype(BF), preferred_element_type=F32)
    row = lax.broadcasted_iota(jnp.int32, tiled.shape, 0) // size
    col = lax.broadcasted_iota(jnp.int32, tiled.shape, 1) // b
    return jnp.where(row == col, tiled, 0.0).astype(BF)


def rows_of(real, imag):
    n, s = real.shape
    return jnp.concatenate([real.reshape(n, s // LANES, LANES), imag.reshape(n, s // LANES, LANES)], axis=1)


def local(
    tokens,
    norm_gain,
    conv_value,
    conv_gate,
    state_feed,
    conv_taps,
    chan_gain,
    chan_shift,
    conv_project,
    decay_rate,
    frequency,
    input_real,
    input_imag,
    output_real,
    output_imag,
    skip_gain,
    state_value,
    state_gate,
    initial_state,
):
    seq_devices = lax.axis_size("sp")
    tp_devices = lax.axis_size("tp")
    position = lax.axis_index("sp")
    length, model = tokens.shape
    rows_in, width = conv_value.shape
    rows_out, columns = conv_project.shape
    shard = pl.pallas_call(
        pack_kernel,
        out_shape=jax.ShapeDtypeStruct((3 * rows_in + 3 * rows_out * (columns // width), width), BF),
        name="pack",
    )(conv_value, conv_gate, state_feed, conv_project, state_value, state_gate)
    gathered = lax.all_gather(shard, "sp", axis=0, tiled=False)

    floats = tokens.astype(F32)
    normed = (
        floats * lax.rsqrt(jnp.mean(floats * floats, axis=1, keepdims=True) + 1e-06) * norm_gain
    ).astype(BF)

    groups, state_size, group_size = input_real.shape
    flat = groups * state_size
    total_tokens = length * seq_devices
    rate_real = -decay_rate / total_tokens
    magnitude = jnp.exp(rate_real)
    step_real = magnitude * jnp.cos(frequency)
    step_imag = magnitude * jnp.sin(frequency)
    modulus = rate_real * rate_real + frequency * frequency
    lift_real = step_real - 1.0
    factor_real = (lift_real * rate_real + step_imag * frequency) / modulus
    factor_imag = (step_imag * rate_real - lift_real * frequency) / modulus
    drive_real = factor_real[..., None] * input_real - factor_imag[..., None] * input_imag
    drive_imag = factor_real[..., None] * input_imag + factor_imag[..., None] * input_real

    drive_real = spread(jnp.swapaxes(drive_real, 1, 2).reshape(groups * group_size, state_size), group_size)
    drive_imag = spread(jnp.swapaxes(drive_imag, 1, 2).reshape(groups * group_size, state_size), group_size)
    mix_real = spread(jnp.swapaxes(output_real, 1, 2).reshape(flat, group_size), state_size)
    mix_imag = spread(jnp.swapaxes(-output_imag, 1, 2).reshape(flat, group_size), state_size)

    base_real = step_real.reshape(flat)
    base_imag = step_imag.reshape(flat)
    square_size = base_real * base_real + base_imag * base_imag

    def powers(real, imag):
        low = power_table(real, imag, lax.iota(jnp.int32, 8) + 1, 8)
        high = power_table(real, imag, lax.iota(jnp.int32, length // 8) * 8, length)
        table = rotate(high[0][:, None], high[1][:, None], low[0][None], low[1][None])
        return tuple(part.reshape(length, flat) for part in table)

    power_real, power_imag = powers(base_real, base_imag)
    undo_real, undo_imag = powers(base_real / square_size, -base_imag / square_size)
    span_real, span_imag = (power_real[-1], power_imag[-1])
    device_ids = lax.iota(jnp.int32, seq_devices)
    lag = position - device_ids
    lead_real, lead_imag = power_table(span_real, span_imag, jnp.maximum(lag, 0), seq_devices)
    earlier = (lag > 0).astype(F32)[:, None]
    lead = rows_of(lead_real * earlier, lead_imag * earlier)
    tail = rows_of(*power_table(span_real, span_imag, seq_devices - device_ids, seq_devices))
    ends = rows_of(
        *rotate(
            *power_table(span_real, span_imag, jnp.stack([position, jnp.int32(seq_devices)]), seq_devices),
            initial_state[0].reshape(1, flat),
            initial_state[1].reshape(1, flat),
        )
    )
    (
        normed, drive_real, drive_imag, mix_real, mix_imag, power_real, power_imag, undo_real, undo_imag, lead, tail, ends
    ) = lax.optimization_barrier((
        normed, drive_real, drive_imag, mix_real, mix_imag, power_real, power_imag, undo_real, undo_imag, lead, tail, ends
    ))
    chunks = flat // LANES

    parts = 4
    hbm = pl.BlockSpec(memory_space=pltpu.HBM)
    gated, feed, sums_real, sums_imag, total = pl.pallas_call(
        first_kernel,
        in_specs=[
            whole(normed.shape),
            hbm,
            whole(drive_real.shape),
            whole(drive_imag.shape),
            whole(undo_real.shape),
            whole(undo_imag.shape),
        ],
        out_shape=[
            jax.ShapeDtypeStruct((length, width), BF),
            jax.ShapeDtypeStruct((length, width), BF),
            jax.ShapeDtypeStruct((length, flat), F32),
            jax.ShapeDtypeStruct((length, flat), F32),
            jax.ShapeDtypeStruct((seq_devices, 2 * chunks, LANES), F32),
        ],
        scratch_shapes=[
            pltpu.VMEM((seq_devices, 3 * rows_in, width), BF),
            pltpu.VMEM((length, 3 * width), F32),
            pltpu.VMEM((2 * chunks, LANES), F32),
            pltpu.SemaphoreType.DMA((parts,)),
        ],
        compiler_params=grant(24),
        name="first",
    )(normed, gathered, drive_real, drive_imag, undo_real, undo_imag)

    taps = conv_taps.shape[0]
    halo = (taps - 1 + 15) // 16 * 16
    before = lax.ppermute(
        gated[length - halo :], "sp", [(source, source + 1) for source in range(seq_devices - 1)]
    )
    totals = lax.all_to_all(total, "sp", 0, 0, tiled=True)
    conv_out = pl.pallas_call(
        conv_kernel,
        out_shape=jax.ShapeDtypeStruct((length, width), BF),
        scratch_shapes=[pltpu.VMEM((halo + length, width), F32)],
        compiler_params=grant(4),
        name="conv",
    )(before, gated, conv_taps)

    copies, final = pl.pallas_call(
        second_kernel,
        out_shape=[
            jax.ShapeDtypeStruct((tp_devices, 2 * length, width), BF),
            jax.ShapeDtypeStruct((2 * chunks, LANES), F32),
        ],
        scratch_shapes=[pltpu.VMEM((2 * chunks, LANES), F32)],
        compiler_params=grant(16),
        name="second",
    )(
        totals, lead, tail, ends, power_real, power_imag, sums_real, sums_imag, mix_real, mix_imag, feed,
        skip_gain.reshape(1, width), conv_out,
    )
    final_state = final.reshape(2, groups, state_size)
    exchanged = lax.all_to_all(copies, "tp", 0, 0, tiled=True)

    mixer_out = pl.pallas_call(
        last_kernel,
        in_specs=[
            whole(exchanged.shape),
            hbm,
            whole((1, chan_gain.shape[0])),
            whole((1, chan_gain.shape[0])),
        ],
        out_shape=jax.ShapeDtypeStruct((length, columns), BF),
        scratch_shapes=[
            pltpu.VMEM((seq_devices, 6 * rows_out, width), BF),
            pltpu.VMEM((length, tp_devices * width), BF),
            pltpu.VMEM((length, 6 * width), F32),
            pltpu.SemaphoreType.DMA((parts,)),
        ],
        compiler_params=grant(24),
        name="last",
    )(exchanged, gathered, chan_gain.reshape(1, -1), chan_shift.reshape(1, -1))
    return (mixer_out, final_state)


def solution(mesh):
    in_specs = (
        P("sp", None),
        P(),
        P("sp", "tp"),
        P("sp", "tp"),
        P("sp", "tp"),
        P(None, "tp"),
        P(),
        P(),
        P("sp", "tp"),
        P("tp", None),
        P("tp", None),
        P("tp", None, None),
        P("tp", None, None),
        P("tp", None, None),
        P("tp", None, None),
        P("tp"),
        P("sp", "tp"),
        P("sp", "tp"),
        P(None, "tp", None),
    )
    out_specs = (P("sp", "tp"), P(None, "tp", None))
    return jax.shard_map(local, mesh=mesh, in_specs=in_specs, out_specs=out_specs, check_vma=False)
```

```python
import jax
import jax.numpy as jnp
from jax import lax
from jax.experimental import pallas as pl
from jax.experimental.pallas import tpu as pltpu
from jax.sharding import Mesh, PartitionSpec as P

BF = jnp.bfloat16
F32 = jnp.float32
LANES = 128
CHUNK = 256
SP = ("z", "yh", "yl")
TP = ("x", "c")
SEQUENCE = ("z", "yh", "c")


def rotate(first_real, first_imag, second_real, second_imag):
    return (
        first_real * second_real - first_imag * second_imag,
        first_real * second_imag + first_imag * second_real,
    )


def power_table(base_real, base_imag, exponent, largest):
    result_real = jnp.ones((exponent.shape[0], base_real.shape[0]), F32)
    result_imag = jnp.zeros((exponent.shape[0], base_real.shape[0]), F32)
    square_real, square_imag = (base_real, base_imag)
    for place in range(max(largest, 1).bit_length()):
        chosen = (exponent >> place & 1 == 1)[:, None]
        next_real, next_imag = rotate(result_real, result_imag, square_real, square_imag)
        result_real = jnp.where(chosen, next_real, result_real)
        result_imag = jnp.where(chosen, next_imag, result_imag)
        square_real, square_imag = rotate(square_real, square_imag, square_real, square_imag)
    return (result_real, result_imag)


def pack_kernel(*refs):
    out_ref = refs[-1]
    width = out_ref.shape[1]
    at = 0
    for ref in refs[:-1]:
        for col in range(0, ref.shape[1], width):
            out_ref[at : at + ref.shape[0]] = ref[:, col : col + width]
            at += ref.shape[0]


def norm_kernel(core_ref, tokens_ref, gain_ref, out_ref):
    floats = tokens_ref[...].astype(F32)
    model = floats.shape[1]
    scale = lax.rsqrt(jnp.sum(floats * floats, axis=1, keepdims=True) / model + 1e-06)
    first_core = core_ref[0] == 0
    low = lax.broadcasted_iota(jnp.int32, (floats.shape[0], LANES), 1) < LANES // 2
    for at in range(0, model, 2 * LANES):
        left = tokens_ref[:, at : at + LANES].astype(F32) * scale * gain_ref[:, at : at + LANES]
        right = (
            tokens_ref[:, at + LANES : at + 2 * LANES].astype(F32)
            * scale
            * gain_ref[:, at + LANES : at + 2 * LANES]
        )
        taken = jnp.where(
            low,
            jnp.where(first_core, left, pltpu.roll(left, LANES // 2, 1)),
            jnp.where(first_core, pltpu.roll(right, LANES // 2, 1), right),
        )
        out_ref[:, at // 2 : at // 2 + LANES] = taken.astype(BF)


def project_kernel(keep_ref, send_ref, weights_ref, keep_out_ref, send_out_ref, buffer_ref, sems):
    outer, inner, rows, width = buffer_ref.shape
    rows //= 3
    parts = sems.shape[0]
    per_part = outer // parts

    def fetch(part):
        at = pl.ds(part * per_part, per_part)
        return pltpu.make_async_copy(weights_ref.at[at], buffer_ref.at[at], sems.at[part])

    for part in range(parts):
        fetch(part).start()
    span = per_part * inner * rows
    for part in range(parts):
        fetch(part).wait()
        for kind in range(3):
            block = buffer_ref[
                part * per_part : (part + 1) * per_part, :, kind * rows : (kind + 1) * rows, :
            ].reshape(span, width)
            cols = slice(kind * width, (kind + 1) * width)
            for lhs_ref, out_ref in ((send_ref, send_out_ref), (keep_ref, keep_out_ref)):
                product = jnp.dot(
                    lhs_ref[:, part * span : (part + 1) * span], block, preferred_element_type=F32
                )
                out_ref[:, cols] = product if part == 0 else out_ref[:, cols] + product


def first_kernel(
    kept_ref,
    received_ref,
    drive_real_ref,
    drive_imag_ref,
    undo_real_ref,
    undo_imag_ref,
    gated_ref,
    feed_ref,
    sums_real_ref,
    sums_imag_ref,
    total_ref,
    last_ref,
):
    length, width = gated_ref.shape
    feed = (kept_ref[:, 2 * width :] + received_ref[:, 2 * width :]).astype(BF)
    feed_ref[...] = feed
    lower = (
        lax.broadcasted_iota(jnp.int32, (length, length), 0)
        >= lax.broadcasted_iota(jnp.int32, (length, length), 1)
    ).astype(BF)
    flat = sums_real_ref.shape[1]
    half = last_ref.shape[0] // 2
    for at in range(0, flat, CHUNK):
        cols = slice(at, at + CHUNK)
        pushed_real = jnp.dot(feed, drive_real_ref[:, cols], preferred_element_type=F32)
        pushed_imag = jnp.dot(feed, drive_imag_ref[:, cols], preferred_element_type=F32)
        scaled = rotate(undo_real_ref[:, cols], undo_imag_ref[:, cols], pushed_real, pushed_imag)
        for part, ref in enumerate((sums_real_ref, sums_imag_ref)):
            sums = jnp.dot(lower, scaled[part].astype(BF), preferred_element_type=F32)
            ref[:, cols] = sums
            for lane in range(0, CHUNK, LANES):
                row = part * half + (at + lane) // LANES
                last_ref[row : row + 1, :] = sums[length - 1 :, lane : lane + LANES]
    total_ref[...] = jnp.broadcast_to(last_ref[...][None], total_ref.shape)
    value = kept_ref[:, :width] + received_ref[:, :width]
    gate = kept_ref[:, width : 2 * width] + received_ref[:, width : 2 * width]
    gated_ref[...] = (value * jax.nn.sigmoid(gate)).astype(BF)


def conv_kernel(before_ref, gated_ref, taps_ref, out_ref, pad_ref):
    length, width = gated_ref.shape
    lead = before_ref.shape[0]
    taps = taps_ref.shape[0]
    pad_ref[:lead] = before_ref[...].astype(F32)
    pad_ref[lead:] = gated_ref[...].astype(F32)
    for col in range(width // LANES):
        cols = slice(col * LANES, (col + 1) * LANES)
        acc = jnp.zeros((length, LANES), F32)
        for tap in range(taps):
            start = lead - (taps - 1) + tap
            acc = acc + taps_ref[tap : tap + 1, cols] * pad_ref[start : start + length, cols]
        out_ref[:, cols] = acc.astype(BF)


def second_kernel(
    totals_ref,
    lead_ref,
    tail_ref,
    ends_ref,
    power_real_ref,
    power_imag_ref,
    sums_real_ref,
    sums_imag_ref,
    mix_real_ref,
    mix_imag_ref,
    feed_ref,
    skip_ref,
    conv_ref,
    out_ref,
    final_ref,
    entry_ref,
):
    half = final_ref.shape[0] // 2
    total_real, total_imag = (totals_ref[:, :half, :], totals_ref[:, half:, :])
    lead_real, lead_imag = rotate(lead_ref[:, :half, :], lead_ref[:, half:, :], total_real, total_imag)
    entry_ref[:half] = ends_ref[0, :half] + jnp.sum(lead_real, axis=0)
    entry_ref[half:] = ends_ref[0, half:] + jnp.sum(lead_imag, axis=0)
    tail_real, tail_imag = rotate(tail_ref[:, :half, :], tail_ref[:, half:, :], total_real, total_imag)
    final_ref[:half] = ends_ref[1, :half] + jnp.sum(tail_real, axis=0)
    final_ref[half:] = ends_ref[1, half:] + jnp.sum(tail_imag, axis=0)
    response = skip_ref[...] * feed_ref[...].astype(F32)
    for at in range(0, sums_real_ref.shape[1], CHUNK):
        cols = slice(at, at + CHUNK)
        rows = range(at // LANES, (at + CHUNK) // LANES)
        entry_real = jnp.concatenate([entry_ref[row : row + 1] for row in rows], axis=1)
        entry_imag = jnp.concatenate([entry_ref[half + row : half + row + 1] for row in rows], axis=1)
        state_real, state_imag = rotate(
            power_real_ref[:, cols],
            power_imag_ref[:, cols],
            sums_real_ref[:, cols] + entry_real,
            sums_imag_ref[:, cols] + entry_imag,
        )
        response = response + jnp.dot(state_real.astype(BF), mix_real_ref[cols, :], preferred_element_type=F32)
        response = response + jnp.dot(state_imag.astype(BF), mix_imag_ref[cols, :], preferred_element_type=F32)
    activated = jax.nn.gelu(response).astype(BF)
    length = activated.shape[0]
    conv = conv_ref[...]
    for copy in range(out_ref.shape[0]):
        out_ref[copy, :length] = conv
        out_ref[copy, length:] = activated


def last_kernel(
    core_ref, rows_ref, own_ref, other_ref, gain_ref, shift_ref, out_ref, buffer_ref, act_ref, acc_ref, sems
):
    blocks, length, width = rows_ref.shape
    length //= 2
    outer, inner, cores, rows, _ = buffer_ref.shape
    rows //= 6
    parts = sems.shape[0]
    per_part = outer // parts
    per_block = blocks // parts
    core = core_ref[0]

    def fetch(part, half):
        at = pl.ds(part * per_part, per_part)
        slot, ref = ((core, own_ref), (1 - core, other_ref))[half]
        return pltpu.make_async_copy(ref.at[at], buffer_ref.at[at, :, slot], sems.at[part, half])

    for part in range(parts):
        fetch(part, 0).start()
        fetch(part, 1).start()
    channels = blocks * width
    total = jnp.zeros((length, width), F32)
    squares = jnp.zeros((length, width), F32)
    for at in range(blocks):
        total = total + rows_ref[at, :length, :].astype(F32)
    mean = jnp.sum(total, axis=1, keepdims=True) / channels
    for at in range(blocks):
        centred = rows_ref[at, :length, :].astype(F32) - mean
        squares = squares + centred * centred
    scale = lax.rsqrt(jnp.sum(squares, axis=1, keepdims=True) / channels + 1e-05)
    for at in range(blocks):
        centred = rows_ref[at, :length, :].astype(F32) - mean
        cols = slice(at * width, (at + 1) * width)
        act_ref[:, cols] = jax.nn.silu(centred * scale * gain_ref[:, cols] + shift_ref[:, cols]).astype(BF)
    span = per_part * inner * cores * rows
    for part in range(parts):
        fetch(part, 0).wait()
        fetch(part, 1).wait()
        conv_act = act_ref[:, part * span : (part + 1) * span]
        activated = jnp.concatenate(
            [rows_ref[part * per_block + at, length:, :] for at in range(per_block)], axis=1
        )
        for kind in range(6):
            block = buffer_ref[
                part * per_part : (part + 1) * per_part, :, :, kind * rows : (kind + 1) * rows, :
            ].reshape(span, width)
            product = jnp.dot(conv_act if kind < 2 else activated, block, preferred_element_type=F32)
            cols = slice(kind * width, (kind + 1) * width)
            acc_ref[:, cols] = product if part == 0 else acc_ref[:, cols] + product
    columns = 2 * width
    out_ref[...] = (
        acc_ref[:, :columns]
        + acc_ref[:, columns : 2 * columns] * jax.nn.sigmoid(acc_ref[:, 2 * columns :])
    ).astype(BF)


def grant(mib):
    return pltpu.CompilerParams(vmem_limit_bytes=mib << 20)


def whole(shape):
    return pl.BlockSpec(shape, lambda *_: (0,) * len(shape))


def spread(blocks, size):
    total, b = blocks.shape
    wide = total // size * b
    pick = lax.broadcasted_iota(jnp.int32, (b, wide), 1) % b == lax.broadcasted_iota(jnp.int32, (b, wide), 0)
    tiled = jnp.dot(blocks.astype(BF), pick.astype(BF), preferred_element_type=F32)
    row = lax.broadcasted_iota(jnp.int32, tiled.shape, 0) // size
    col = lax.broadcasted_iota(jnp.int32, tiled.shape, 1) // b
    return jnp.where(row == col, tiled, 0.0).astype(BF)


def rows_of(real, imag):
    n, s = real.shape
    return jnp.concatenate([real.reshape(n, s // LANES, LANES), imag.reshape(n, s // LANES, LANES)], axis=1)


def local(
    tokens,
    norm_gain,
    conv_value,
    conv_gate,
    state_feed,
    conv_taps,
    chan_gain,
    chan_shift,
    conv_project,
    decay_rate,
    frequency,
    input_real,
    input_imag,
    output_real,
    output_imag,
    skip_gain,
    state_value,
    state_gate,
    initial_state,
):
    seq_devices = lax.axis_size("z") * lax.axis_size("yh") * lax.axis_size("c")
    tp_devices = lax.axis_size("x") * lax.axis_size("yl")
    core = lax.axis_index("c")
    same = lax.axis_index("yl") == core
    position = (lax.axis_index("z") * lax.axis_size("yh") + lax.axis_index("yh")) * 2 + core
    length, model = tokens.shape
    rows_in, width = conv_value.shape
    rows_out, columns = conv_project.shape
    inner = lax.axis_size("yh")

    def swapped(value):
        return lax.ppermute(value, ("yl", "c"), [(a * 2 + b, b * 2 + a) for a in range(2) for b in range(2)])

    def packed(rows, *arrays):
        return pl.pallas_call(
            pack_kernel,
            out_shape=jax.ShapeDtypeStruct((rows, width), BF),
            compiler_params=grant(4),
            name="pack",
        )(*arrays)

    def spread_y(shard):
        return lax.all_to_all(
            jnp.broadcast_to(shard[None], (inner, *shard.shape)), "yh", 0, 0, tiled=True
        )

    shard_first = swapped(packed(3 * rows_in, conv_value, conv_gate, state_feed))
    rows_first = spread_y(shard_first)
    weights_first = lax.all_gather(rows_first, "z", axis=0, tiled=False)
    shard_last = packed(6 * rows_out, conv_project, state_value, state_gate)
    shard_last, _ = lax.optimization_barrier((shard_last, rows_first))
    rows_last = spread_y(swapped(shard_last))
    weights_last = lax.all_gather(rows_last, "z", axis=0, tiled=False)

    core_scalar = core.astype(jnp.int32).reshape(1)
    smem = pl.BlockSpec(memory_space=pltpu.SMEM)
    tokens, decay_rate, skip_gain, conv_taps, _ = lax.optimization_barrier(
        (tokens, decay_rate, skip_gain, conv_taps, shard_first)
    )
    own_half = pl.pallas_call(
        norm_kernel,
        in_specs=[smem, whole(tokens.shape), whole((1, model))],
        out_shape=jax.ShapeDtypeStruct((length, model // 2), BF),
        name="norm",
    )(core_scalar, tokens, norm_gain.reshape(1, model))
    across = [(0, 1), (1, 0)]
    other_half = lax.ppermute(own_half, "yl", across)
    keep = jnp.where(same, own_half, other_half)
    send = jnp.where(same, other_half, own_half)

    groups, state_size, group_size = input_real.shape
    small = groups * group_size
    parameters = [
        jnp.concatenate([jnp.swapaxes(p, 1, 2).reshape(small, state_size) for p in (input_real, input_imag)], axis=1),
        jnp.concatenate([p.reshape(small, state_size) for p in (output_real, output_imag)], axis=1),
        jnp.concatenate([decay_rate, frequency], axis=1),
        jnp.concatenate([initial_state[0], initial_state[1]], axis=1),
        conv_taps[:, :LANES],
        conv_taps[:, LANES:],
        skip_gain.reshape(width // LANES, LANES),
    ]
    ends_at = []
    for p in parameters:
        ends_at.append((ends_at[-1] if ends_at else 0) + p.shape[0])
    flat_parameters = jnp.concatenate(parameters, axis=0)
    flat_parameters = jnp.where(same, flat_parameters, lax.ppermute(flat_parameters, "c", across))
    inputs, outputs, rates, initial, taps_left, taps_right, skip = jnp.split(flat_parameters, ends_at[:-1], axis=0)
    conv_taps = jnp.concatenate([taps_left, taps_right], axis=1)
    input_real, input_imag = (
        part.reshape(groups, group_size, state_size) for part in jnp.split(inputs, 2, axis=1)
    )
    output_real, output_imag = (
        part.reshape(groups, group_size, state_size) for part in jnp.split(outputs, 2, axis=1)
    )
    decay_rate, frequency = jnp.split(rates, 2, axis=1)
    initial_state = jnp.split(initial, 2, axis=1)

    flat = groups * state_size
    total_tokens = length * seq_devices
    rate_real = -decay_rate / total_tokens
    magnitude = jnp.exp(rate_real)
    step_real = magnitude * jnp.cos(frequency)
    step_imag = magnitude * jnp.sin(frequency)
    modulus = rate_real * rate_real + frequency * frequency
    lift_real = step_real - 1.0
    factor_real = (lift_real * rate_real + step_imag * frequency) / modulus
    factor_imag = (step_imag * rate_real - lift_real * frequency) / modulus
    drive_real = factor_real[:, None] * input_real - factor_imag[:, None] * input_imag
    drive_imag = factor_real[:, None] * input_imag + factor_imag[:, None] * input_real

    drive_real = spread(drive_real.reshape(small, state_size), group_size)
    drive_imag = spread(drive_imag.reshape(small, state_size), group_size)
    mix_real = spread(jnp.swapaxes(output_real, 1, 2).reshape(flat, group_size), state_size)
    mix_imag = spread(jnp.swapaxes(-output_imag, 1, 2).reshape(flat, group_size), state_size)

    base_real = step_real.reshape(flat)
    base_imag = step_imag.reshape(flat)
    square_size = base_real * base_real + base_imag * base_imag

    def powers(real, imag):
        low = power_table(real, imag, lax.iota(jnp.int32, 8) + 1, 8)
        high = power_table(real, imag, lax.iota(jnp.int32, length // 8) * 8, length)
        table = rotate(high[0][:, None], high[1][:, None], low[0][None], low[1][None])
        return tuple(part.reshape(length, flat) for part in table)

    power_real, power_imag = powers(base_real, base_imag)
    undo_real, undo_imag = powers(base_real / square_size, -base_imag / square_size)
    span_real, span_imag = (power_real[-1], power_imag[-1])
    device_ids = lax.iota(jnp.int32, seq_devices)
    lag = position - device_ids
    lead_real, lead_imag = power_table(span_real, span_imag, jnp.maximum(lag, 0), seq_devices)
    earlier = (lag > 0).astype(F32)[:, None]
    lead = rows_of(lead_real * earlier, lead_imag * earlier)
    tail = rows_of(*power_table(span_real, span_imag, seq_devices - device_ids, seq_devices))
    ends = rows_of(
        *rotate(
            *power_table(span_real, span_imag, jnp.stack([position, jnp.int32(seq_devices)]), seq_devices),
            initial_state[0].reshape(1, flat),
            initial_state[1].reshape(1, flat),
        )
    )
    (
        keep, drive_real, drive_imag, mix_real, mix_imag, power_real, power_imag, undo_real, undo_imag, lead, tail, ends
    ) = lax.optimization_barrier((
        keep, drive_real, drive_imag, mix_real, mix_imag, power_real, power_imag, undo_real, undo_imag, lead, tail, ends
    ))
    chunks = flat // LANES

    parts = 4
    hbm = pl.BlockSpec(memory_space=pl.ANY)
    kept, sent = pl.pallas_call(
        project_kernel,
        in_specs=[whole(keep.shape), whole(send.shape), hbm],
        out_shape=[jax.ShapeDtypeStruct((length, 3 * width), F32)] * 2,
        scratch_shapes=[pltpu.VMEM(weights_first.shape, BF), pltpu.SemaphoreType.DMA((parts,))],
        name="project",
    )(keep, send, weights_first)
    received = lax.ppermute(sent, "c", across)
    gated, feed, sums_real, sums_imag, total = pl.pallas_call(
        first_kernel,
        out_shape=[
            jax.ShapeDtypeStruct((length, width), BF),
            jax.ShapeDtypeStruct((length, width), BF),
            jax.ShapeDtypeStruct((length, flat), F32),
            jax.ShapeDtypeStruct((length, flat), F32),
            jax.ShapeDtypeStruct((seq_devices, 2 * chunks, LANES), F32),
        ],
        scratch_shapes=[pltpu.VMEM((2 * chunks, LANES), F32)],
        name="first",
    )(kept, received, drive_real, drive_imag, undo_real, undo_imag)

    taps = conv_taps.shape[0]
    halo = (taps - 1 + 15) // 16 * 16
    before = lax.ppermute(
        gated[length - halo :], SEQUENCE, [(source, source + 1) for source in range(seq_devices - 1)]
    )
    totals = lax.all_to_all(total, SEQUENCE, 0, 0, tiled=True)
    conv_out = pl.pallas_call(
        conv_kernel,
        out_shape=jax.ShapeDtypeStruct((length, width), BF),
        scratch_shapes=[pltpu.VMEM((halo + length, width), F32)],
        compiler_params=grant(4),
        name="conv",
    )(before, gated, conv_taps)

    copies, final = pl.pallas_call(
        second_kernel,
        out_shape=[
            jax.ShapeDtypeStruct((tp_devices, 2 * length, width), BF),
            jax.ShapeDtypeStruct((2 * chunks, LANES), F32),
        ],
        scratch_shapes=[pltpu.VMEM((2 * chunks, LANES), F32)],
        name="second",
    )(
        totals, lead, tail, ends, power_real, power_imag, sums_real, sums_imag, mix_real, mix_imag, feed,
        skip.reshape(1, width), conv_out,
    )
    final = swapped(final)
    final_state = final.reshape(2, groups, state_size)
    exchanged = lax.all_to_all(copies, ("x", "yl"), 0, 0, tiled=True)

    weights_sent, exchanged = lax.optimization_barrier((weights_last, exchanged))
    weights_other = lax.ppermute(weights_sent, "c", across)
    mixed = pl.pallas_call(
        last_kernel,
        in_specs=[
            smem,
            whole(exchanged.shape),
            hbm,
            hbm,
            whole((1, chan_gain.shape[0])),
            whole((1, chan_gain.shape[0])),
        ],
        out_shape=jax.ShapeDtypeStruct((length, columns), BF),
        scratch_shapes=[
            pltpu.VMEM((*weights_last.shape[:2], 2, *weights_last.shape[2:]), BF),
            pltpu.VMEM((length, tp_devices * width), BF),
            pltpu.VMEM((length, 6 * width), F32),
            pltpu.SemaphoreType.DMA((parts, 2)),
        ],
        name="last",
    )(core_scalar, exchanged, weights_last, weights_other, chan_gain.reshape(1, -1), chan_shift.reshape(1, -1))
    mixer_out = swapped(mixed)
    return (mixer_out, final_state)


def solution(mesh):
    mesh = Mesh(mesh.devices.reshape(8, 4, 2, 4, 2), ("z", "yh", "yl", "x", "c"))
    in_specs = (
        P(SP, None),
        P(),
        P(SP, TP),
        P(SP, TP),
        P(SP, TP),
        P(None, TP),
        P(),
        P(),
        P(SP, TP),
        P(TP, None),
        P(TP, None),
        P(TP, None, None),
        P(TP, None, None),
        P(TP, None, None),
        P(TP, None, None),
        P(TP),
        P(SP, TP),
        P(SP, TP),
        P(None, TP, None),
    )
    out_specs = (P(SP, TP), P(None, TP, None))
    return jax.shard_map(local, mesh=mesh, in_specs=in_specs, out_specs=out_specs, check_vma=False)
```

```python
import jax
import jax.numpy as jnp
from jax import lax
from jax.experimental import pallas as pl
from jax.experimental.pallas import tpu as pltpu
from jax.sharding import Mesh, PartitionSpec as P

BF = jnp.bfloat16
F32 = jnp.float32
LANES = 128
CHUNK = 256
SP = ("z", "yh", "yl")
TP = ("x", "c")
SEQUENCE = ("z", "yh", "c")


def rotate(first_real, first_imag, second_real, second_imag):
    return (
        first_real * second_real - first_imag * second_imag,
        first_real * second_imag + first_imag * second_real,
    )


def power_table(base_real, base_imag, exponent, largest):
    result_real = jnp.ones((exponent.shape[0], base_real.shape[0]), F32)
    result_imag = jnp.zeros((exponent.shape[0], base_real.shape[0]), F32)
    square_real, square_imag = (base_real, base_imag)
    for place in range(max(largest, 1).bit_length()):
        chosen = (exponent >> place & 1 == 1)[:, None]
        next_real, next_imag = rotate(result_real, result_imag, square_real, square_imag)
        result_real = jnp.where(chosen, next_real, result_real)
        result_imag = jnp.where(chosen, next_imag, result_imag)
        square_real, square_imag = rotate(square_real, square_imag, square_real, square_imag)
    return (result_real, result_imag)


def pack_kernel(*refs):
    out_ref = refs[-1]
    width = out_ref.shape[1]
    at = 0
    for ref in refs[:-1]:
        for col in range(0, ref.shape[1], width):
            out_ref[at : at + ref.shape[0]] = ref[:, col : col + width]
            at += ref.shape[0]


def norm_kernel(core_ref, tokens_ref, gain_ref, out_ref):
    floats = tokens_ref[...].astype(F32)
    model = floats.shape[1]
    scale = lax.rsqrt(jnp.sum(floats * floats, axis=1, keepdims=True) / model + 1e-06)
    first_core = core_ref[0] == 0
    low = lax.broadcasted_iota(jnp.int32, (floats.shape[0], LANES), 1) < LANES // 2
    for at in range(0, model, 2 * LANES):
        left = tokens_ref[:, at : at + LANES].astype(F32) * scale * gain_ref[:, at : at + LANES]
        right = (
            tokens_ref[:, at + LANES : at + 2 * LANES].astype(F32)
            * scale
            * gain_ref[:, at + LANES : at + 2 * LANES]
        )
        taken = jnp.where(
            low,
            jnp.where(first_core, left, pltpu.roll(left, LANES // 2, 1)),
            jnp.where(first_core, pltpu.roll(right, LANES // 2, 1), right),
        )
        out_ref[:, at // 2 : at // 2 + LANES] = taken.astype(BF)


def project_kernel(keep_ref, send_ref, weights_ref, keep_out_ref, send_out_ref, buffer_ref, sems):
    outer, inner, rows, width = buffer_ref.shape
    rows //= 3
    parts = sems.shape[0]
    per_part = outer // parts

    def fetch(part):
        at = pl.ds(part * per_part, per_part)
        return pltpu.make_async_copy(weights_ref.at[at], buffer_ref.at[at], sems.at[part])

    for part in range(parts):
        fetch(part).start()
    span = per_part * inner * rows
    length = keep_ref.shape[0]
    for part in range(parts):
        fetch(part).wait()
        lhs = jnp.concatenate([ref[:, part * span : (part + 1) * span] for ref in (send_ref, keep_ref)], axis=0)
        for kind in range(3):
            block = buffer_ref[
                part * per_part : (part + 1) * per_part, :, kind * rows : (kind + 1) * rows, :
            ].reshape(span, width)
            cols = slice(kind * width, (kind + 1) * width)
            product = jnp.dot(lhs, block, preferred_element_type=F32)
            for at, out_ref in ((0, send_out_ref), (length, keep_out_ref)):
                rows_of_it = product[at : at + length]
                out_ref[:, cols] = rows_of_it if part == 0 else out_ref[:, cols] + rows_of_it


def first_kernel(
    kept_ref,
    received_ref,
    drive_real_ref,
    drive_imag_ref,
    undo_real_ref,
    undo_imag_ref,
    gated_ref,
    feed_ref,
    sums_real_ref,
    sums_imag_ref,
    total_ref,
    last_ref,
):
    length, width = gated_ref.shape
    feed = (kept_ref[:, 2 * width :] + received_ref[:, 2 * width :]).astype(BF)
    feed_ref[...] = feed
    lower = (
        lax.broadcasted_iota(jnp.int32, (length, length), 0)
        >= lax.broadcasted_iota(jnp.int32, (length, length), 1)
    ).astype(BF)
    flat = sums_real_ref.shape[1]
    half = last_ref.shape[0] // 2
    for at in range(0, flat, CHUNK):
        cols = slice(at, at + CHUNK)
        pushed_real = jnp.dot(feed, drive_real_ref[:, cols], preferred_element_type=F32)
        pushed_imag = jnp.dot(feed, drive_imag_ref[:, cols], preferred_element_type=F32)
        scaled = rotate(undo_real_ref[:, cols], undo_imag_ref[:, cols], pushed_real, pushed_imag)
        for part, ref in enumerate((sums_real_ref, sums_imag_ref)):
            sums = jnp.dot(lower, scaled[part].astype(BF), preferred_element_type=F32)
            ref[:, cols] = sums
            for lane in range(0, CHUNK, LANES):
                row = part * half + (at + lane) // LANES
                last_ref[row : row + 1, :] = sums[length - 1 :, lane : lane + LANES]
    total_ref[...] = jnp.broadcast_to(last_ref[...][None], total_ref.shape)
    value = kept_ref[:, :width] + received_ref[:, :width]
    gate = kept_ref[:, width : 2 * width] + received_ref[:, width : 2 * width]
    gated_ref[...] = (value * jax.nn.sigmoid(gate)).astype(BF)


def conv_kernel(before_ref, gated_ref, taps_ref, out_ref, pad_ref):
    length, width = gated_ref.shape
    lead = before_ref.shape[0]
    taps = taps_ref.shape[0]
    pad_ref[:lead] = before_ref[...].astype(F32)
    pad_ref[lead:] = gated_ref[...].astype(F32)
    for col in range(width // LANES):
        cols = slice(col * LANES, (col + 1) * LANES)
        acc = jnp.zeros((length, LANES), F32)
        for tap in range(taps):
            start = lead - (taps - 1) + tap
            acc = acc + taps_ref[tap : tap + 1, cols] * pad_ref[start : start + length, cols]
        out_ref[:, cols] = acc.astype(BF)


def weighted(weights_ref, values_ref):
    half = values_ref.shape[1] // 2
    real, imag = rotate(
        weights_ref[:, :half, :], weights_ref[:, half:, :], values_ref[:, :half, :], values_ref[:, half:, :]
    )
    return jnp.sum(real, axis=0), jnp.sum(imag, axis=0)


def row_kernel(totals_ref, tail_ref, out_ref):
    half = totals_ref.shape[1] // 2
    real, imag = weighted(tail_ref, totals_ref)
    for copy in range(out_ref.shape[0]):
        out_ref[copy, :half] = real
        out_ref[copy, half:] = imag


def second_kernel(
    totals_ref,
    lead_ref,
    ends_of_rows_ref,
    lead_rows_ref,
    tail_rows_ref,
    ends_ref,
    power_real_ref,
    power_imag_ref,
    sums_real_ref,
    sums_imag_ref,
    mix_real_ref,
    mix_imag_ref,
    feed_ref,
    skip_ref,
    conv_ref,
    out_ref,
    final_ref,
    entry_ref,
):
    half = final_ref.shape[0] // 2
    lead = weighted(lead_ref, totals_ref)
    lead_rows = weighted(lead_rows_ref, ends_of_rows_ref)
    tail_rows = weighted(tail_rows_ref, ends_of_rows_ref)
    for part in range(2):
        rows = slice(part * half, (part + 1) * half)
        entry_ref[rows] = ends_ref[0, rows] + lead[part] + lead_rows[part]
        final_ref[rows] = ends_ref[1, rows] + tail_rows[part]
    response = skip_ref[...] * feed_ref[...].astype(F32)
    for at in range(0, sums_real_ref.shape[1], CHUNK):
        cols = slice(at, at + CHUNK)
        rows = range(at // LANES, (at + CHUNK) // LANES)
        entry_real = jnp.concatenate([entry_ref[row : row + 1] for row in rows], axis=1)
        entry_imag = jnp.concatenate([entry_ref[half + row : half + row + 1] for row in rows], axis=1)
        state_real, state_imag = rotate(
            power_real_ref[:, cols],
            power_imag_ref[:, cols],
            sums_real_ref[:, cols] + entry_real,
            sums_imag_ref[:, cols] + entry_imag,
        )
        response = response + jnp.dot(state_real.astype(BF), mix_real_ref[cols, :], preferred_element_type=F32)
        response = response + jnp.dot(state_imag.astype(BF), mix_imag_ref[cols, :], preferred_element_type=F32)
    activated = jax.nn.gelu(response).astype(BF)
    length = activated.shape[0]
    conv = conv_ref[...]
    for copy in range(out_ref.shape[0]):
        out_ref[copy, :length] = conv
        out_ref[copy, length:] = activated


def last_kernel(
    core_ref, rows_ref, own_ref, other_ref, gain_ref, shift_ref, out_ref, buffer_ref, act_ref, acc_ref, sems
):
    blocks, length, width = rows_ref.shape
    length //= 2
    outer, inner, cores, rows, _ = buffer_ref.shape
    rows //= 6
    parts = sems.shape[0]
    per_part = outer // parts
    per_block = blocks // parts
    core = core_ref[0]

    def fetch(part, half):
        at = pl.ds(part * per_part, per_part)
        slot, ref = ((core, own_ref), (1 - core, other_ref))[half]
        return pltpu.make_async_copy(ref.at[at], buffer_ref.at[at, :, slot], sems.at[part, half])

    for part in range(parts):
        fetch(part, 0).start()
        fetch(part, 1).start()
    channels = blocks * width
    total = jnp.zeros((length, width), F32)
    squares = jnp.zeros((length, width), F32)
    for at in range(blocks):
        total = total + rows_ref[at, :length, :].astype(F32)
    mean = jnp.sum(total, axis=1, keepdims=True) / channels
    for at in range(blocks):
        centred = rows_ref[at, :length, :].astype(F32) - mean
        squares = squares + centred * centred
    scale = lax.rsqrt(jnp.sum(squares, axis=1, keepdims=True) / channels + 1e-05)
    for at in range(blocks):
        centred = rows_ref[at, :length, :].astype(F32) - mean
        cols = slice(at * width, (at + 1) * width)
        act_ref[:, cols] = jax.nn.silu(centred * scale * gain_ref[:, cols] + shift_ref[:, cols]).astype(BF)
    span = per_part * inner * cores * rows
    for part in range(parts):
        fetch(part, 0).wait()
        fetch(part, 1).wait()
        conv_act = act_ref[:, part * span : (part + 1) * span]
        activated = jnp.concatenate(
            [rows_ref[part * per_block + at, length:, :] for at in range(per_block)], axis=1
        )
        for kind in range(6):
            block = buffer_ref[
                part * per_part : (part + 1) * per_part, :, :, kind * rows : (kind + 1) * rows, :
            ].reshape(span, width)
            product = jnp.dot(conv_act if kind < 2 else activated, block, preferred_element_type=F32)
            cols = slice(kind * width, (kind + 1) * width)
            acc_ref[:, cols] = product if part == 0 else acc_ref[:, cols] + product
    columns = 2 * width
    out_ref[...] = (
        acc_ref[:, :columns]
        + acc_ref[:, columns : 2 * columns] * jax.nn.sigmoid(acc_ref[:, 2 * columns :])
    ).astype(BF)


def grant(mib):
    return pltpu.CompilerParams(vmem_limit_bytes=mib << 20)


def whole(shape):
    return pl.BlockSpec(shape, lambda *_: (0,) * len(shape))


def spread(blocks, size):
    total, b = blocks.shape
    wide = total // size * b
    pick = lax.broadcasted_iota(jnp.int32, (b, wide), 1) % b == lax.broadcasted_iota(jnp.int32, (b, wide), 0)
    tiled = jnp.dot(blocks.astype(BF), pick.astype(BF), preferred_element_type=F32)
    row = lax.broadcasted_iota(jnp.int32, tiled.shape, 0) // size
    col = lax.broadcasted_iota(jnp.int32, tiled.shape, 1) // b
    return jnp.where(row == col, tiled, 0.0).astype(BF)


def rows_of(real, imag):
    n, s = real.shape
    return jnp.concatenate([real.reshape(n, s // LANES, LANES), imag.reshape(n, s // LANES, LANES)], axis=1)


def local(
    tokens,
    norm_gain,
    conv_value,
    conv_gate,
    state_feed,
    conv_taps,
    chan_gain,
    chan_shift,
    conv_project,
    decay_rate,
    frequency,
    input_real,
    input_imag,
    output_real,
    output_imag,
    skip_gain,
    state_value,
    state_gate,
    initial_state,
):
    seq_devices = lax.axis_size("z") * lax.axis_size("yh") * lax.axis_size("c")
    tp_devices = lax.axis_size("x") * lax.axis_size("yl")
    core = lax.axis_index("c")
    same = lax.axis_index("yl") == core
    position = (lax.axis_index("z") * lax.axis_size("yh") + lax.axis_index("yh")) * 2 + core
    length, model = tokens.shape
    rows_in, width = conv_value.shape
    rows_out, columns = conv_project.shape
    inner = lax.axis_size("yh")

    def swapped(value):
        return lax.ppermute(value, ("yl", "c"), [(a * 2 + b, b * 2 + a) for a in range(2) for b in range(2)])

    def packed(rows, *arrays):
        return pl.pallas_call(
            pack_kernel,
            out_shape=jax.ShapeDtypeStruct((rows, width), BF),
            name="pack",
        )(*arrays)

    def copies_of(shard):
        return jnp.broadcast_to(shard[None], (inner, *shard.shape))

    shard_first = swapped(packed(3 * rows_in, conv_value, conv_gate, state_feed))
    wide_first = copies_of(shard_first)
    wide_first, decay_rate, skip_gain, conv_taps, input_real, input_imag, output_real, output_imag = (
        lax.optimization_barrier(
            (wide_first, decay_rate, skip_gain, conv_taps, input_real, input_imag, output_real, output_imag)
        )
    )
    rows_first = lax.all_to_all(wide_first, "yh", 0, 0, tiled=True)
    weights_first = lax.all_gather(rows_first, "z", axis=0, tiled=False)
    shard_last = packed(6 * rows_out, conv_project, state_value, state_gate)
    tokens, _ = lax.optimization_barrier((tokens, rows_first))

    core_scalar = core.astype(jnp.int32).reshape(1)
    smem = pl.BlockSpec(memory_space=pltpu.SMEM)
    own_half = pl.pallas_call(
        norm_kernel,
        in_specs=[smem, whole(tokens.shape), whole((1, model))],
        out_shape=jax.ShapeDtypeStruct((length, model // 2), BF),
        name="norm",
    )(core_scalar, tokens, norm_gain.reshape(1, model))
    across = [(0, 1), (1, 0)]
    other_half = lax.ppermute(own_half, "yl", across)
    shard_last, _ = lax.optimization_barrier((shard_last, own_half))
    rows_last = lax.all_to_all(copies_of(swapped(shard_last)), "yh", 0, 0, tiled=True)
    weights_last = lax.all_gather(rows_last, "z", axis=0, tiled=False)
    keep = jnp.where(same, own_half, other_half)
    send = jnp.where(same, other_half, own_half)

    groups, state_size, group_size = input_real.shape
    small = groups * group_size
    parameters = [
        jnp.concatenate([jnp.swapaxes(p, 1, 2).reshape(small, state_size) for p in (input_real, input_imag)], axis=1),
        jnp.concatenate([p.reshape(small, state_size) for p in (output_real, output_imag)], axis=1),
        jnp.concatenate([decay_rate, frequency], axis=1),
        jnp.concatenate([initial_state[0], initial_state[1]], axis=1),
        conv_taps[:, :LANES],
        conv_taps[:, LANES:],
        skip_gain.reshape(width // LANES, LANES),
    ]
    ends_at = []
    for p in parameters:
        ends_at.append((ends_at[-1] if ends_at else 0) + p.shape[0])
    flat_parameters = jnp.concatenate(parameters, axis=0)
    flat_parameters = jnp.where(same, flat_parameters, lax.ppermute(flat_parameters, "c", across))
    flat_parameters, _ = lax.optimization_barrier((flat_parameters, own_half))
    inputs, outputs, rates, initial, taps_left, taps_right, skip = jnp.split(flat_parameters, ends_at[:-1], axis=0)
    conv_taps = jnp.concatenate([taps_left, taps_right], axis=1)
    input_real, input_imag = (
        part.reshape(groups, group_size, state_size) for part in jnp.split(inputs, 2, axis=1)
    )
    output_real, output_imag = (
        part.reshape(groups, group_size, state_size) for part in jnp.split(outputs, 2, axis=1)
    )
    decay_rate, frequency = jnp.split(rates, 2, axis=1)
    initial_state = jnp.split(initial, 2, axis=1)

    flat = groups * state_size
    total_tokens = length * seq_devices
    rate_real = -decay_rate / total_tokens
    magnitude = jnp.exp(rate_real)
    step_real = magnitude * jnp.cos(frequency)
    step_imag = magnitude * jnp.sin(frequency)
    modulus = rate_real * rate_real + frequency * frequency
    lift_real = step_real - 1.0
    factor_real = (lift_real * rate_real + step_imag * frequency) / modulus
    factor_imag = (step_imag * rate_real - lift_real * frequency) / modulus
    drive_real = factor_real[:, None] * input_real - factor_imag[:, None] * input_imag
    drive_imag = factor_real[:, None] * input_imag + factor_imag[:, None] * input_real

    drive_real = spread(drive_real.reshape(small, state_size), group_size)
    drive_imag = spread(drive_imag.reshape(small, state_size), group_size)
    mix_real = spread(jnp.swapaxes(output_real, 1, 2).reshape(flat, group_size), state_size)
    mix_imag = spread(jnp.swapaxes(-output_imag, 1, 2).reshape(flat, group_size), state_size)

    base_real = step_real.reshape(flat)
    base_imag = step_imag.reshape(flat)
    square_size = base_real * base_real + base_imag * base_imag

    def powers(real, imag):
        low = power_table(real, imag, lax.iota(jnp.int32, 8) + 1, 8)
        high = power_table(real, imag, lax.iota(jnp.int32, length // 8) * 8, length)
        table = rotate(high[0][:, None], high[1][:, None], low[0][None], low[1][None])
        return tuple(part.reshape(length, flat) for part in table)

    power_real, power_imag = powers(base_real, base_imag)
    undo_real, undo_imag = powers(base_real / square_size, -base_imag / square_size)
    span_real, span_imag = (power_real[-1], power_imag[-1])
    row_devices = inner * 2
    outer = seq_devices // row_devices
    in_row = position % row_devices
    row = position // row_devices
    lag = in_row - lax.iota(jnp.int32, row_devices)
    lag_rows = row - lax.iota(jnp.int32, outer)

    def spans(exponent, chosen=None):
        real, imag = power_table(span_real, span_imag, jnp.maximum(exponent, 0), seq_devices)
        if chosen is not None:
            real, imag = (part * chosen.astype(F32)[:, None] for part in (real, imag))
        return rows_of(real, imag)

    lead = spans(lag, lag > 0)
    tail = spans(row_devices - lax.iota(jnp.int32, row_devices))
    lead_rows = spans((lag_rows - 1) * row_devices + in_row, lag_rows > 0)
    tail_rows = spans((outer - 1 - lax.iota(jnp.int32, outer)) * row_devices)
    ends = rows_of(
        *rotate(
            *power_table(span_real, span_imag, jnp.stack([position, jnp.int32(seq_devices)]), seq_devices),
            initial_state[0].reshape(1, flat),
            initial_state[1].reshape(1, flat),
        )
    )
    (
        keep, drive_real, drive_imag, mix_real, mix_imag, power_real, power_imag, undo_real, undo_imag, lead, tail, lead_rows,
        tail_rows, ends
    ) = lax.optimization_barrier((
        keep, drive_real, drive_imag, mix_real, mix_imag, power_real, power_imag, undo_real, undo_imag, lead, tail, lead_rows,
        tail_rows, ends
    ))
    chunks = flat // LANES

    parts = 4
    hbm = pl.BlockSpec(memory_space=pl.ANY)
    kept, sent = pl.pallas_call(
        project_kernel,
        in_specs=[whole(keep.shape), whole(send.shape), hbm],
        out_shape=[jax.ShapeDtypeStruct((length, 3 * width), F32)] * 2,
        scratch_shapes=[pltpu.VMEM(weights_first.shape, BF), pltpu.SemaphoreType.DMA((parts,))],
        name="project",
    )(keep, send, weights_first)
    received = lax.ppermute(sent, "c", across)
    gated, feed, sums_real, sums_imag, total = pl.pallas_call(
        first_kernel,
        out_shape=[
            jax.ShapeDtypeStruct((length, width), BF),
            jax.ShapeDtypeStruct((length, width), BF),
            jax.ShapeDtypeStruct((length, flat), F32),
            jax.ShapeDtypeStruct((length, flat), F32),
            jax.ShapeDtypeStruct((row_devices, 2 * chunks, LANES), F32),
        ],
        scratch_shapes=[pltpu.VMEM((2 * chunks, LANES), F32)],
        name="first",
    )(kept, received, drive_real, drive_imag, undo_real, undo_imag)

    taps = conv_taps.shape[0]
    halo = (taps - 1 + 15) // 16 * 16
    before = lax.ppermute(
        gated[length - halo :], SEQUENCE, [(source, source + 1) for source in range(seq_devices - 1)]
    )
    totals = lax.all_to_all(total, SEQUENCE[1:], 0, 0, tiled=True)
    end_of_row = pl.pallas_call(
        row_kernel,
        out_shape=jax.ShapeDtypeStruct((outer, 2 * chunks, LANES), F32),
        name="row",
    )(totals, tail)
    ends_of_rows = lax.all_to_all(end_of_row, SEQUENCE[0], 0, 0, tiled=True)
    conv_out = pl.pallas_call(
        conv_kernel,
        out_shape=jax.ShapeDtypeStruct((length, width), BF),
        scratch_shapes=[pltpu.VMEM((halo + length, width), F32)],
        compiler_params=grant(4),
        name="conv",
    )(before, gated, conv_taps)

    copies, final = pl.pallas_call(
        second_kernel,
        out_shape=[
            jax.ShapeDtypeStruct((tp_devices, 2 * length, width), BF),
            jax.ShapeDtypeStruct((2 * chunks, LANES), F32),
        ],
        scratch_shapes=[pltpu.VMEM((2 * chunks, LANES), F32)],
        name="second",
    )(
        totals, lead, ends_of_rows, lead_rows, tail_rows, ends, power_real, power_imag, sums_real, sums_imag,
        mix_real, mix_imag, feed,
        skip.reshape(1, width), conv_out,
    )
    final = swapped(final)
    final_state = final.reshape(2, groups, state_size)
    exchanged = lax.all_to_all(copies, ("x", "yl"), 0, 0, tiled=True)

    weights_sent, exchanged = lax.optimization_barrier((weights_last, exchanged))
    weights_other = lax.ppermute(weights_sent, "c", across)
    mixed = pl.pallas_call(
        last_kernel,
        in_specs=[
            smem,
            whole(exchanged.shape),
            hbm,
            hbm,
            whole((1, chan_gain.shape[0])),
            whole((1, chan_gain.shape[0])),
        ],
        out_shape=jax.ShapeDtypeStruct((length, columns), BF),
        scratch_shapes=[
            pltpu.VMEM((*weights_last.shape[:2], 2, *weights_last.shape[2:]), BF),
            pltpu.VMEM((length, tp_devices * width), BF),
            pltpu.VMEM((length, 6 * width), F32),
            pltpu.SemaphoreType.DMA((parts, 2)),
        ],
        name="last",
    )(core_scalar, exchanged, weights_last, weights_other, chan_gain.reshape(1, -1), chan_shift.reshape(1, -1))
    mixer_out = swapped(mixed)
    return (mixer_out, final_state)


def solution(mesh):
    mesh = Mesh(mesh.devices.reshape(8, 4, 2, 4, 2), ("z", "yh", "yl", "x", "c"))
    in_specs = (
        P(SP, None),
        P(),
        P(SP, TP),
        P(SP, TP),
        P(SP, TP),
        P(None, TP),
        P(),
        P(),
        P(SP, TP),
        P(TP, None),
        P(TP, None),
        P(TP, None, None),
        P(TP, None, None),
        P(TP, None, None),
        P(TP, None, None),
        P(TP),
        P(SP, TP),
        P(SP, TP),
        P(None, TP, None),
    )
    out_specs = (P(SP, TP), P(None, TP, None))
    return jax.shard_map(local, mesh=mesh, in_specs=in_specs, out_specs=out_specs, check_vma=False)
```

```python
import jax
import jax.numpy as jnp
from jax import lax
from jax.experimental import pallas as pl
from jax.experimental.pallas import tpu as pltpu
from jax.sharding import Mesh, PartitionSpec as P

BF = jnp.bfloat16
F32 = jnp.float32
LANES = 128
CHUNK = 256
SP = ("z", "yh", "yl")
TP = ("x", "c")
SEQUENCE = ("z", "yh", "c")


def rotate(first_real, first_imag, second_real, second_imag):
    return (
        first_real * second_real - first_imag * second_imag,
        first_real * second_imag + first_imag * second_real,
    )


def power_table(base_real, base_imag, exponent, largest):
    result_real = jnp.ones((exponent.shape[0], base_real.shape[0]), F32)
    result_imag = jnp.zeros((exponent.shape[0], base_real.shape[0]), F32)
    square_real, square_imag = (base_real, base_imag)
    for place in range(max(largest, 1).bit_length()):
        chosen = (exponent >> place & 1 == 1)[:, None]
        next_real, next_imag = rotate(result_real, result_imag, square_real, square_imag)
        result_real = jnp.where(chosen, next_real, result_real)
        result_imag = jnp.where(chosen, next_imag, result_imag)
        square_real, square_imag = rotate(square_real, square_imag, square_real, square_imag)
    return (result_real, result_imag)


def pack_kernel(*refs):
    out_ref = refs[-1]
    width = out_ref.shape[1]
    at = 0
    for ref in refs[:-1]:
        for col in range(0, ref.shape[1], width):
            out_ref[at : at + ref.shape[0]] = ref[:, col : col + width]
            at += ref.shape[0]


def arrange_kernel(places_ref, *refs):
    out_ref = refs[-1]
    for at, ref in enumerate(refs[:-1]):
        out_ref[places_ref[at]] = ref[...]


def norm_kernel(core_ref, tokens_ref, gain_ref, out_ref):
    floats = tokens_ref[...].astype(F32)
    model = floats.shape[1]
    scale = lax.rsqrt(jnp.sum(floats * floats, axis=1, keepdims=True) / model + 1e-06)
    first_core = core_ref[0] == 0
    low = lax.broadcasted_iota(jnp.int32, (floats.shape[0], LANES), 1) < LANES // 2
    for at in range(0, model, 2 * LANES):
        left = tokens_ref[:, at : at + LANES].astype(F32) * scale * gain_ref[:, at : at + LANES]
        right = (
            tokens_ref[:, at + LANES : at + 2 * LANES].astype(F32)
            * scale
            * gain_ref[:, at + LANES : at + 2 * LANES]
        )
        taken = jnp.where(
            low,
            jnp.where(first_core, left, pltpu.roll(left, LANES // 2, 1)),
            jnp.where(first_core, pltpu.roll(right, LANES // 2, 1), right),
        )
        out_ref[:, at // 2 : at // 2 + LANES] = taken.astype(BF)


def project_kernel(
    keep_ref, send_ref, weights_ref, keep_out_ref, send_out_ref, buffer_ref, tokens_ref, sems, token_sems
):
    outer, inner, rows, width = buffer_ref.shape
    rows //= 3
    parts = sems.shape[0]
    per_part = outer // parts
    length = keep_out_ref.shape[0]
    span = per_part * inner * rows

    def fetch(part):
        at = pl.ds(part * per_part, per_part)
        return pltpu.make_async_copy(weights_ref.at[at], buffer_ref.at[at], sems.at[part])

    def fetch_tokens(part, half):
        ref = (send_ref, keep_ref)[half]
        return pltpu.make_async_copy(
            ref.at[:, pl.ds(part * span, span)],
            tokens_ref.at[part, pl.ds(half * length, length)],
            token_sems.at[part, half],
        )

    for part in range(parts):
        fetch_tokens(part, 0).start()
        fetch_tokens(part, 1).start()
        fetch(part).start()
    for part in range(parts):
        fetch_tokens(part, 0).wait()
        fetch_tokens(part, 1).wait()
        fetch(part).wait()
        for kind in range(3):
            block = buffer_ref[
                part * per_part : (part + 1) * per_part, :, kind * rows : (kind + 1) * rows, :
            ].reshape(span, width)
            cols = slice(kind * width, (kind + 1) * width)
            product = jnp.dot(tokens_ref[part], block, preferred_element_type=F32)
            for at, out_ref in ((0, send_out_ref), (length, keep_out_ref)):
                its_rows = product[at : at + length]
                out_ref[:, cols] = its_rows if part == 0 else out_ref[:, cols] + its_rows


def first_kernel(
    kept_ref,
    received_ref,
    drive_real_ref,
    drive_imag_ref,
    undo_real_ref,
    undo_imag_ref,
    gated_ref,
    feed_ref,
    sums_real_ref,
    sums_imag_ref,
    total_ref,
    last_ref,
):
    length, width = gated_ref.shape
    feed = (kept_ref[:, 2 * width :] + received_ref[:, 2 * width :]).astype(BF)
    feed_ref[...] = feed
    lower = (
        lax.broadcasted_iota(jnp.int32, (length, length), 0)
        >= lax.broadcasted_iota(jnp.int32, (length, length), 1)
    ).astype(BF)
    flat = sums_real_ref.shape[1]
    half = last_ref.shape[0] // 2
    for at in range(0, flat, CHUNK):
        cols = slice(at, at + CHUNK)
        pushed_real = jnp.dot(feed, drive_real_ref[:, cols], preferred_element_type=F32)
        pushed_imag = jnp.dot(feed, drive_imag_ref[:, cols], preferred_element_type=F32)
        scaled = rotate(undo_real_ref[:, cols], undo_imag_ref[:, cols], pushed_real, pushed_imag)
        for part, ref in enumerate((sums_real_ref, sums_imag_ref)):
            sums = jnp.dot(lower, scaled[part].astype(BF), preferred_element_type=F32)
            ref[:, cols] = sums
            for lane in range(0, CHUNK, LANES):
                row = part * half + (at + lane) // LANES
                last_ref[row : row + 1, :] = sums[length - 1 :, lane : lane + LANES]
    total_ref[...] = jnp.broadcast_to(last_ref[...][None], total_ref.shape)
    value = kept_ref[:, :width] + received_ref[:, :width]
    gate = kept_ref[:, width : 2 * width] + received_ref[:, width : 2 * width]
    gated_ref[...] = (value * jax.nn.sigmoid(gate)).astype(BF)


def conv_kernel(before_ref, gated_ref, taps_ref, out_ref, pad_ref):
    length, width = gated_ref.shape
    lead = before_ref.shape[0]
    taps = taps_ref.shape[0]
    pad_ref[:lead] = before_ref[...].astype(F32)
    pad_ref[lead:] = gated_ref[...].astype(F32)
    for col in range(width // LANES):
        cols = slice(col * LANES, (col + 1) * LANES)
        acc = jnp.zeros((length, LANES), F32)
        for tap in range(taps):
            start = lead - (taps - 1) + tap
            acc = acc + taps_ref[tap : tap + 1, cols] * pad_ref[start : start + length, cols]
        out_ref[:, cols] = acc.astype(BF)


def weighted(weights_ref, values_ref):
    half = values_ref.shape[1] // 2
    real, imag = rotate(
        weights_ref[:, :half, :], weights_ref[:, half:, :], values_ref[:, :half, :], values_ref[:, half:, :]
    )
    return jnp.sum(real, axis=0), jnp.sum(imag, axis=0)


def row_kernel(totals_ref, tail_ref, out_ref):
    half = totals_ref.shape[1] // 2
    real, imag = weighted(tail_ref, totals_ref)
    for copy in range(out_ref.shape[0]):
        out_ref[copy, :half] = real
        out_ref[copy, half:] = imag


def second_kernel(
    totals_ref,
    lead_ref,
    ends_of_rows_ref,
    lead_rows_ref,
    tail_rows_ref,
    ends_ref,
    power_real_ref,
    power_imag_ref,
    sums_real_ref,
    sums_imag_ref,
    mix_real_ref,
    mix_imag_ref,
    feed_ref,
    skip_ref,
    conv_ref,
    out_ref,
    final_ref,
    entry_ref,
):
    half = final_ref.shape[0] // 2
    lead = weighted(lead_ref, totals_ref)
    lead_rows = weighted(lead_rows_ref, ends_of_rows_ref)
    tail_rows = weighted(tail_rows_ref, ends_of_rows_ref)
    for part in range(2):
        rows = slice(part * half, (part + 1) * half)
        entry_ref[rows] = ends_ref[0, rows] + lead[part] + lead_rows[part]
        final_ref[rows] = ends_ref[1, rows] + tail_rows[part]
    response = skip_ref[...] * feed_ref[...].astype(F32)
    for at in range(0, sums_real_ref.shape[1], CHUNK):
        cols = slice(at, at + CHUNK)
        rows = range(at // LANES, (at + CHUNK) // LANES)
        entry_real = jnp.concatenate([entry_ref[row : row + 1] for row in rows], axis=1)
        entry_imag = jnp.concatenate([entry_ref[half + row : half + row + 1] for row in rows], axis=1)
        state_real, state_imag = rotate(
            power_real_ref[:, cols],
            power_imag_ref[:, cols],
            sums_real_ref[:, cols] + entry_real,
            sums_imag_ref[:, cols] + entry_imag,
        )
        response = response + jnp.dot(state_real.astype(BF), mix_real_ref[cols, :], preferred_element_type=F32)
        response = response + jnp.dot(state_imag.astype(BF), mix_imag_ref[cols, :], preferred_element_type=F32)
    activated = jax.nn.gelu(response).astype(BF)
    length = activated.shape[0]
    conv = conv_ref[...]
    for copy in range(out_ref.shape[0]):
        out_ref[copy, :length] = conv
        out_ref[copy, length:] = activated


def last_kernel(
    core_ref, rows_ref, own_ref, other_ref, gain_ref, shift_ref, out_ref, buffer_ref, act_ref, acc_ref, sems
):
    blocks, length, width = rows_ref.shape
    length //= 2
    outer, inner, cores, rows, _ = buffer_ref.shape
    rows //= 6
    parts = sems.shape[0]
    per_part = outer // parts
    per_block = blocks // parts
    core = core_ref[0]

    def fetch(part, half):
        at = pl.ds(part * per_part, per_part)
        slot, ref = ((core, own_ref), (1 - core, other_ref))[half]
        return pltpu.make_async_copy(ref.at[at], buffer_ref.at[at, :, slot], sems.at[part, half])

    for part in range(parts):
        fetch(part, 0).start()
        fetch(part, 1).start()
    channels = blocks * width
    total = jnp.zeros((length, width), F32)
    squares = jnp.zeros((length, width), F32)
    for at in range(blocks):
        total = total + rows_ref[at, :length, :].astype(F32)
    mean = jnp.sum(total, axis=1, keepdims=True) / channels
    for at in range(blocks):
        centred = rows_ref[at, :length, :].astype(F32) - mean
        squares = squares + centred * centred
    scale = lax.rsqrt(jnp.sum(squares, axis=1, keepdims=True) / channels + 1e-05)
    for at in range(blocks):
        centred = rows_ref[at, :length, :].astype(F32) - mean
        cols = slice(at * width, (at + 1) * width)
        act_ref[:, cols] = jax.nn.silu(centred * scale * gain_ref[:, cols] + shift_ref[:, cols]).astype(BF)
    span = per_part * inner * cores * rows
    for part in range(parts):
        fetch(part, 0).wait()
        fetch(part, 1).wait()
        conv_act = act_ref[:, part * span : (part + 1) * span]
        activated = jnp.concatenate(
            [rows_ref[part * per_block + at, length:, :] for at in range(per_block)], axis=1
        )
        for kind in range(6):
            block = buffer_ref[
                part * per_part : (part + 1) * per_part, :, :, kind * rows : (kind + 1) * rows, :
            ].reshape(span, width)
            product = jnp.dot(conv_act if kind < 2 else activated, block, preferred_element_type=F32)
            cols = slice(kind * width, (kind + 1) * width)
            acc_ref[:, cols] = product if part == 0 else acc_ref[:, cols] + product
    columns = 2 * width
    out_ref[...] = (
        acc_ref[:, :columns]
        + acc_ref[:, columns : 2 * columns] * jax.nn.sigmoid(acc_ref[:, 2 * columns :])
    ).astype(BF)


def grant(mib):
    return pltpu.CompilerParams(vmem_limit_bytes=mib << 20)


def whole(shape):
    return pl.BlockSpec(shape, lambda *_: (0,) * len(shape))


def spread(blocks, size):
    total, b = blocks.shape
    wide = total // size * b
    pick = lax.broadcasted_iota(jnp.int32, (b, wide), 1) % b == lax.broadcasted_iota(jnp.int32, (b, wide), 0)
    tiled = jnp.dot(blocks.astype(BF), pick.astype(BF), preferred_element_type=F32)
    row = lax.broadcasted_iota(jnp.int32, tiled.shape, 0) // size
    col = lax.broadcasted_iota(jnp.int32, tiled.shape, 1) // b
    return jnp.where(row == col, tiled, 0.0).astype(BF)


def rows_of(real, imag):
    n, s = real.shape
    return jnp.concatenate([real.reshape(n, s // LANES, LANES), imag.reshape(n, s // LANES, LANES)], axis=1)


def local(
    tokens,
    norm_gain,
    conv_value,
    conv_gate,
    state_feed,
    conv_taps,
    chan_gain,
    chan_shift,
    conv_project,
    decay_rate,
    frequency,
    input_real,
    input_imag,
    output_real,
    output_imag,
    skip_gain,
    state_value,
    state_gate,
    initial_state,
):
    seq_devices = lax.axis_size("z") * lax.axis_size("yh") * lax.axis_size("c")
    tp_devices = lax.axis_size("x") * lax.axis_size("yl")
    core = lax.axis_index("c")
    same = lax.axis_index("yl") == core
    position = (lax.axis_index("z") * lax.axis_size("yh") + lax.axis_index("yh")) * 2 + core
    length, model = tokens.shape
    rows_in, width = conv_value.shape
    rows_out, columns = conv_project.shape
    inner = lax.axis_size("yh")

    def swapped(value):
        return lax.ppermute(value, ("yl", "c"), [(a * 2 + b, b * 2 + a) for a in range(2) for b in range(2)])

    def packed(rows, *arrays):
        return pl.pallas_call(
            pack_kernel,
            out_shape=jax.ShapeDtypeStruct((rows, width), BF),
            name="pack",
        )(*arrays)

    def copies_of(shard):
        return jnp.broadcast_to(shard[None], (inner, *shard.shape))

    smem = pl.BlockSpec(memory_space=pltpu.SMEM)
    shard_first = packed(3 * rows_in, conv_value, conv_gate, state_feed)
    tokens, decay_rate, skip_gain, conv_taps, input_real, input_imag, output_real, output_imag, shard_first = (
        lax.optimization_barrier(
            (tokens, decay_rate, skip_gain, conv_taps, input_real, input_imag, output_real, output_imag, shard_first)
        )
    )
    blocks = []
    for shift in range(inner):
        pairs = [
            (h * 4 + a * 2 + b, (h + shift) % inner * 4 + b * 2 + a)
            for h in range(inner)
            for a in range(2)
            for b in range(2)
        ]
        blocks.append(lax.ppermute(shard_first, ("yh", "yl", "c"), pairs))
    places = (lax.axis_index("yh") - lax.iota(jnp.int32, inner)) % inner
    rows_first = pl.pallas_call(
        arrange_kernel,
        in_specs=[smem] + [whole(shard_first.shape)] * inner,
        out_shape=jax.ShapeDtypeStruct((inner, *shard_first.shape), BF),
        name="arrange",
    )(places, *blocks)
    weights_first = lax.all_gather(rows_first, "z", axis=0, tiled=False)
    shard_last = packed(6 * rows_out, conv_project, state_value, state_gate)
    core_scalar = core.astype(jnp.int32).reshape(1)
    own_half = pl.pallas_call(
        norm_kernel,
        in_specs=[smem, whole(tokens.shape), whole((1, model))],
        out_shape=jax.ShapeDtypeStruct((length, model // 2), BF),
        name="norm",
    )(core_scalar, tokens, norm_gain.reshape(1, model))
    across = [(0, 1), (1, 0)]
    half_sent, _ = lax.optimization_barrier((own_half, rows_first))
    other_half = lax.ppermute(half_sent, "yl", across)
    shard_last, _ = lax.optimization_barrier((shard_last, rows_first))
    rows_last = lax.all_to_all(copies_of(swapped(shard_last)), "yh", 0, 0, tiled=True)
    weights_last = lax.all_gather(rows_last, "z", axis=0, tiled=False)
    keep = jnp.where(same, own_half, other_half)
    send = jnp.where(same, other_half, own_half)

    groups, state_size, group_size = input_real.shape
    small = groups * group_size
    parameters = [
        jnp.concatenate([jnp.swapaxes(p, 1, 2).reshape(small, state_size) for p in (input_real, input_imag)], axis=1),
        jnp.concatenate([p.reshape(small, state_size) for p in (output_real, output_imag)], axis=1),
        jnp.concatenate([decay_rate, frequency], axis=1),
        jnp.concatenate([initial_state[0], initial_state[1]], axis=1),
        conv_taps[:, :LANES],
        conv_taps[:, LANES:],
        skip_gain.reshape(width // LANES, LANES),
    ]
    ends_at = []
    for p in parameters:
        ends_at.append((ends_at[-1] if ends_at else 0) + p.shape[0])
    flat_parameters = jnp.concatenate(parameters, axis=0)
    flat_parameters = jnp.where(same, flat_parameters, lax.ppermute(flat_parameters, "c", across))
    flat_parameters, _ = lax.optimization_barrier((flat_parameters, own_half))
    inputs, outputs, rates, initial, taps_left, taps_right, skip = jnp.split(flat_parameters, ends_at[:-1], axis=0)
    conv_taps = jnp.concatenate([taps_left, taps_right], axis=1)
    input_real, input_imag = (
        part.reshape(groups, group_size, state_size) for part in jnp.split(inputs, 2, axis=1)
    )
    output_real, output_imag = (
        part.reshape(groups, group_size, state_size) for part in jnp.split(outputs, 2, axis=1)
    )
    decay_rate, frequency = jnp.split(rates, 2, axis=1)
    initial_state = jnp.split(initial, 2, axis=1)

    flat = groups * state_size
    total_tokens = length * seq_devices
    rate_real = -decay_rate / total_tokens
    magnitude = jnp.exp(rate_real)
    step_real = magnitude * jnp.cos(frequency)
    step_imag = magnitude * jnp.sin(frequency)
    modulus = rate_real * rate_real + frequency * frequency
    lift_real = step_real - 1.0
    factor_real = (lift_real * rate_real + step_imag * frequency) / modulus
    factor_imag = (step_imag * rate_real - lift_real * frequency) / modulus
    drive_real = factor_real[:, None] * input_real - factor_imag[:, None] * input_imag
    drive_imag = factor_real[:, None] * input_imag + factor_imag[:, None] * input_real

    drive_real = spread(drive_real.reshape(small, state_size), group_size)
    drive_imag = spread(drive_imag.reshape(small, state_size), group_size)
    mix_real = spread(jnp.swapaxes(output_real, 1, 2).reshape(flat, group_size), state_size)
    mix_imag = spread(jnp.swapaxes(-output_imag, 1, 2).reshape(flat, group_size), state_size)

    base_real = step_real.reshape(flat)
    base_imag = step_imag.reshape(flat)
    square_size = base_real * base_real + base_imag * base_imag

    def powers(real, imag):
        low = power_table(real, imag, lax.iota(jnp.int32, 8) + 1, 8)
        high = power_table(real, imag, lax.iota(jnp.int32, length // 8) * 8, length)
        table = rotate(high[0][:, None], high[1][:, None], low[0][None], low[1][None])
        return tuple(part.reshape(length, flat) for part in table)

    power_real, power_imag = powers(base_real, base_imag)
    undo_real, undo_imag = powers(base_real / square_size, -base_imag / square_size)
    span_real, span_imag = (power_real[-1], power_imag[-1])
    row_devices = inner * 2
    outer = seq_devices // row_devices
    in_row = position % row_devices
    row = position // row_devices
    lag = in_row - lax.iota(jnp.int32, row_devices)
    lag_rows = row - lax.iota(jnp.int32, outer)

    def spans(exponent, chosen=None):
        real, imag = power_table(span_real, span_imag, jnp.maximum(exponent, 0), seq_devices)
        if chosen is not None:
            real, imag = (part * chosen.astype(F32)[:, None] for part in (real, imag))
        return rows_of(real, imag)

    lead = spans(lag, lag > 0)
    tail = spans(row_devices - lax.iota(jnp.int32, row_devices))
    lead_rows = spans((lag_rows - 1) * row_devices + in_row, lag_rows > 0)
    tail_rows = spans((outer - 1 - lax.iota(jnp.int32, outer)) * row_devices)
    ends = rows_of(
        *rotate(
            *power_table(span_real, span_imag, jnp.stack([position, jnp.int32(seq_devices)]), seq_devices),
            initial_state[0].reshape(1, flat),
            initial_state[1].reshape(1, flat),
        )
    )
    (
        keep, drive_real, drive_imag, mix_real, mix_imag, power_real, power_imag, undo_real, undo_imag, lead, tail, lead_rows,
        tail_rows, ends
    ) = lax.optimization_barrier((
        keep, drive_real, drive_imag, mix_real, mix_imag, power_real, power_imag, undo_real, undo_imag, lead, tail, lead_rows,
        tail_rows, ends
    ))
    chunks = flat // LANES

    parts = 4
    hbm = pl.BlockSpec(memory_space=pl.ANY)
    kept, sent = pl.pallas_call(
        project_kernel,
        in_specs=[hbm, hbm, hbm],
        out_shape=[jax.ShapeDtypeStruct((length, 3 * width), F32)] * 2,
        scratch_shapes=[
            pltpu.VMEM(weights_first.shape, BF),
            pltpu.VMEM((parts, 2 * length, model // 2 // parts), BF),
            pltpu.SemaphoreType.DMA((parts,)),
            pltpu.SemaphoreType.DMA((parts, 2)),
        ],
        name="project",
    )(keep, send, weights_first)
    received = lax.ppermute(sent, "c", across)
    gated, feed, sums_real, sums_imag, total = pl.pallas_call(
        first_kernel,
        out_shape=[
            jax.ShapeDtypeStruct((length, width), BF),
            jax.ShapeDtypeStruct((length, width), BF),
            jax.ShapeDtypeStruct((length, flat), F32),
            jax.ShapeDtypeStruct((length, flat), F32),
            jax.ShapeDtypeStruct((row_devices, 2 * chunks, LANES), F32),
        ],
        scratch_shapes=[pltpu.VMEM((2 * chunks, LANES), F32)],
        name="first",
    )(kept, received, drive_real, drive_imag, undo_real, undo_imag)

    taps = conv_taps.shape[0]
    halo = (taps - 1 + 15) // 16 * 16
    before = lax.ppermute(
        gated[length - halo :], SEQUENCE, [(source, source + 1) for source in range(seq_devices - 1)]
    )
    totals = lax.all_to_all(total, SEQUENCE[1:], 0, 0, tiled=True)
    end_of_row = pl.pallas_call(
        row_kernel,
        out_shape=jax.ShapeDtypeStruct((outer, 2 * chunks, LANES), F32),
        name="row",
    )(totals, tail)
    ends_of_rows = lax.all_to_all(end_of_row, SEQUENCE[0], 0, 0, tiled=True)
    conv_out = pl.pallas_call(
        conv_kernel,
        out_shape=jax.ShapeDtypeStruct((length, width), BF),
        scratch_shapes=[pltpu.VMEM((halo + length, width), F32)],
        compiler_params=grant(4),
        name="conv",
    )(before, gated, conv_taps)

    copies, final = pl.pallas_call(
        second_kernel,
        out_shape=[
            jax.ShapeDtypeStruct((tp_devices, 2 * length, width), BF),
            jax.ShapeDtypeStruct((2 * chunks, LANES), F32),
        ],
        scratch_shapes=[pltpu.VMEM((2 * chunks, LANES), F32)],
        name="second",
    )(
        totals, lead, ends_of_rows, lead_rows, tail_rows, ends, power_real, power_imag, sums_real, sums_imag,
        mix_real, mix_imag, feed,
        skip.reshape(1, width), conv_out,
    )
    final = swapped(final)
    exchanged = lax.all_to_all(copies, ("x", "yl"), 0, 0, tiled=True)

    exchanged, final = lax.optimization_barrier((exchanged, final))
    weights_sent, _ = lax.optimization_barrier((weights_last, copies))
    weights_other = lax.ppermute(weights_sent, "c", across)
    mixed = pl.pallas_call(
        last_kernel,
        in_specs=[
            smem,
            whole(exchanged.shape),
            hbm,
            hbm,
            whole((1, chan_gain.shape[0])),
            whole((1, chan_gain.shape[0])),
        ],
        out_shape=jax.ShapeDtypeStruct((length, columns), BF),
        scratch_shapes=[
            pltpu.VMEM((*weights_last.shape[:2], 2, *weights_last.shape[2:]), BF),
            pltpu.VMEM((length, tp_devices * width), BF),
            pltpu.VMEM((length, 6 * width), F32),
            pltpu.SemaphoreType.DMA((parts, 2)),
        ],
        name="last",
    )(core_scalar, exchanged, weights_last, weights_other, chan_gain.reshape(1, -1), chan_shift.reshape(1, -1))
    mixer_out = swapped(mixed)
    return (mixer_out, final.reshape(2, groups, state_size))


def solution(mesh):
    mesh = Mesh(mesh.devices.reshape(8, 4, 2, 4, 2), ("z", "yh", "yl", "x", "c"))
    in_specs = (
        P(SP, None),
        P(),
        P(SP, TP),
        P(SP, TP),
        P(SP, TP),
        P(None, TP),
        P(),
        P(),
        P(SP, TP),
        P(TP, None),
        P(TP, None),
        P(TP, None, None),
        P(TP, None, None),
        P(TP, None, None),
        P(TP, None, None),
        P(TP),
        P(SP, TP),
        P(SP, TP),
        P(None, TP, None),
    )
    out_specs = (P(SP, TP), P(None, TP, None))
    return jax.shard_map(local, mesh=mesh, in_specs=in_specs, out_specs=out_specs, check_vma=False)
```

```python
import jax
import jax.numpy as jnp
from jax import lax
from jax.experimental import pallas as pl
from jax.experimental.pallas import tpu as pltpu
from jax.sharding import Mesh, PartitionSpec as P

BF = jnp.bfloat16
F32 = jnp.float32
LANES = 128
CHUNK = 256
SP = ("z", "yh", "yl")
TP = ("x", "c")
SEQUENCE = ("z", "yh", "c")


def rotate(first_real, first_imag, second_real, second_imag):
    return (
        first_real * second_real - first_imag * second_imag,
        first_real * second_imag + first_imag * second_real,
    )


def power_table(base_real, base_imag, exponent, largest):
    result_real = jnp.ones((exponent.shape[0], base_real.shape[0]), F32)
    result_imag = jnp.zeros((exponent.shape[0], base_real.shape[0]), F32)
    square_real, square_imag = (base_real, base_imag)
    for place in range(max(largest, 1).bit_length()):
        chosen = (exponent >> place & 1 == 1)[:, None]
        next_real, next_imag = rotate(result_real, result_imag, square_real, square_imag)
        result_real = jnp.where(chosen, next_real, result_real)
        result_imag = jnp.where(chosen, next_imag, result_imag)
        square_real, square_imag = rotate(square_real, square_imag, square_real, square_imag)
    return (result_real, result_imag)


def pack_kernel(*refs):
    out_ref = refs[-1]
    width = out_ref.shape[1]
    at = 0
    for ref in refs[:-1]:
        for col in range(0, ref.shape[1], width):
            out_ref[at : at + ref.shape[0]] = ref[:, col : col + width]
            at += ref.shape[0]


def arrange_kernel(places_ref, *refs):
    out_ref = refs[-1]
    for at, ref in enumerate(refs[:-1]):
        out_ref[places_ref[at]] = ref[...]


def norm_kernel(core_ref, tokens_ref, gain_ref, out_ref):
    floats = tokens_ref[...].astype(F32)
    model = floats.shape[1]
    scale = lax.rsqrt(jnp.sum(floats * floats, axis=1, keepdims=True) / model + 1e-06)
    first_core = core_ref[0] == 0
    low = lax.broadcasted_iota(jnp.int32, (floats.shape[0], LANES), 1) < LANES // 2
    for at in range(0, model, 2 * LANES):
        left = tokens_ref[:, at : at + LANES].astype(F32) * scale * gain_ref[:, at : at + LANES]
        right = (
            tokens_ref[:, at + LANES : at + 2 * LANES].astype(F32)
            * scale
            * gain_ref[:, at + LANES : at + 2 * LANES]
        )
        taken = jnp.where(
            low,
            jnp.where(first_core, left, pltpu.roll(left, LANES // 2, 1)),
            jnp.where(first_core, pltpu.roll(right, LANES // 2, 1), right),
        )
        out_ref[:, at // 2 : at // 2 + LANES] = taken.astype(BF)


def project_kernel(
    keep_ref, send_ref, weights_ref, keep_out_ref, send_out_ref, buffer_ref, tokens_ref, sems, token_sems
):
    outer, inner, rows, width = buffer_ref.shape
    rows //= 3
    parts = sems.shape[0]
    per_part = outer // parts
    length = keep_out_ref.shape[0]
    span = per_part * inner * rows

    def fetch(part):
        at = pl.ds(part * per_part, per_part)
        return pltpu.make_async_copy(weights_ref.at[at], buffer_ref.at[at], sems.at[part])

    def fetch_tokens(part, half):
        ref = (send_ref, keep_ref)[half]
        return pltpu.make_async_copy(
            ref.at[:, pl.ds(part * span, span)],
            tokens_ref.at[part, pl.ds(half * length, length)],
            token_sems.at[part, half],
        )

    for part in range(parts):
        fetch_tokens(part, 0).start()
        fetch_tokens(part, 1).start()
        fetch(part).start()
    for part in range(parts):
        fetch_tokens(part, 0).wait()
        fetch_tokens(part, 1).wait()
        fetch(part).wait()
        for kind in range(3):
            block = buffer_ref[
                part * per_part : (part + 1) * per_part, :, kind * rows : (kind + 1) * rows, :
            ].reshape(span, width)
            cols = slice(kind * width, (kind + 1) * width)
            product = jnp.dot(tokens_ref[part], block, preferred_element_type=F32)
            for at, out_ref in ((0, send_out_ref), (length, keep_out_ref)):
                its_rows = product[at : at + length]
                out_ref[:, cols] = its_rows if part == 0 else out_ref[:, cols] + its_rows


def first_kernel(
    kept_ref,
    received_ref,
    drive_real_ref,
    drive_imag_ref,
    undo_real_ref,
    undo_imag_ref,
    gated_ref,
    feed_ref,
    sums_real_ref,
    sums_imag_ref,
    total_ref,
    last_ref,
):
    length, width = gated_ref.shape
    feed = (kept_ref[:, 2 * width :] + received_ref[:, 2 * width :]).astype(BF)
    feed_ref[...] = feed
    lower = (
        lax.broadcasted_iota(jnp.int32, (length, length), 0)
        >= lax.broadcasted_iota(jnp.int32, (length, length), 1)
    ).astype(BF)
    flat = sums_real_ref.shape[1]
    half = last_ref.shape[0] // 2
    for at in range(0, flat, CHUNK):
        cols = slice(at, at + CHUNK)
        pushed_real = jnp.dot(feed, drive_real_ref[:, cols], preferred_element_type=F32)
        pushed_imag = jnp.dot(feed, drive_imag_ref[:, cols], preferred_element_type=F32)
        scaled = rotate(undo_real_ref[:, cols], undo_imag_ref[:, cols], pushed_real, pushed_imag)
        for part, ref in enumerate((sums_real_ref, sums_imag_ref)):
            sums = jnp.dot(lower, scaled[part].astype(BF), preferred_element_type=F32)
            ref[:, cols] = sums
            for lane in range(0, CHUNK, LANES):
                row = part * half + (at + lane) // LANES
                last_ref[row : row + 1, :] = sums[length - 1 :, lane : lane + LANES]
    total_ref[...] = jnp.broadcast_to(last_ref[...][None], total_ref.shape)
    value = kept_ref[:, :width] + received_ref[:, :width]
    gate = kept_ref[:, width : 2 * width] + received_ref[:, width : 2 * width]
    gated_ref[...] = (value * jax.nn.sigmoid(gate)).astype(BF)


def conv_kernel(before_ref, gated_ref, taps_ref, out_ref, pad_ref):
    length, width = gated_ref.shape
    lead = before_ref.shape[0]
    taps = taps_ref.shape[0]
    pad_ref[:lead] = before_ref[...].astype(F32)
    pad_ref[lead:] = gated_ref[...].astype(F32)
    for col in range(width // LANES):
        cols = slice(col * LANES, (col + 1) * LANES)
        acc = jnp.zeros((length, LANES), F32)
        for tap in range(taps):
            start = lead - (taps - 1) + tap
            acc = acc + taps_ref[tap : tap + 1, cols] * pad_ref[start : start + length, cols]
        out_ref[:, cols] = acc.astype(BF)


def weighted(weights_ref, values_ref):
    half = values_ref.shape[1] // 2
    real, imag = rotate(
        weights_ref[:, :half, :], weights_ref[:, half:, :], values_ref[:, :half, :], values_ref[:, half:, :]
    )
    return jnp.sum(real, axis=0), jnp.sum(imag, axis=0)


def row_kernel(totals_ref, tail_ref, out_ref):
    half = totals_ref.shape[1] // 2
    real, imag = weighted(tail_ref, totals_ref)
    for copy in range(out_ref.shape[0]):
        out_ref[copy, :half] = real
        out_ref[copy, half:] = imag


def second_kernel(
    totals_ref,
    lead_ref,
    ends_of_rows_ref,
    lead_rows_ref,
    tail_rows_ref,
    ends_ref,
    power_real_ref,
    power_imag_ref,
    sums_real_ref,
    sums_imag_ref,
    mix_real_ref,
    mix_imag_ref,
    feed_ref,
    skip_ref,
    conv_ref,
    out_ref,
    final_ref,
    entry_ref,
):
    half = final_ref.shape[0] // 2
    lead = weighted(lead_ref, totals_ref)
    lead_rows = weighted(lead_rows_ref, ends_of_rows_ref)
    tail_rows = weighted(tail_rows_ref, ends_of_rows_ref)
    for part in range(2):
        rows = slice(part * half, (part + 1) * half)
        entry_ref[rows] = ends_ref[0, rows] + lead[part] + lead_rows[part]
        final_ref[rows] = ends_ref[1, rows] + tail_rows[part]
    response = skip_ref[...] * feed_ref[...].astype(F32)
    for at in range(0, sums_real_ref.shape[1], CHUNK):
        cols = slice(at, at + CHUNK)
        rows = range(at // LANES, (at + CHUNK) // LANES)
        entry_real = jnp.concatenate([entry_ref[row : row + 1] for row in rows], axis=1)
        entry_imag = jnp.concatenate([entry_ref[half + row : half + row + 1] for row in rows], axis=1)
        state_real, state_imag = rotate(
            power_real_ref[:, cols],
            power_imag_ref[:, cols],
            sums_real_ref[:, cols] + entry_real,
            sums_imag_ref[:, cols] + entry_imag,
        )
        response = response + jnp.dot(state_real.astype(BF), mix_real_ref[cols, :], preferred_element_type=F32)
        response = response + jnp.dot(state_imag.astype(BF), mix_imag_ref[cols, :], preferred_element_type=F32)
    activated = jax.nn.gelu(response).astype(BF)
    length = activated.shape[0]
    conv = conv_ref[...]
    for copy in range(out_ref.shape[0]):
        out_ref[copy, :length] = conv
        out_ref[copy, length:] = activated


def last_kernel(
    core_ref, rows_ref, own_ref, other_ref, gain_ref, shift_ref, out_ref, buffer_ref, act_ref, acc_ref, sems
):
    blocks, length, width = rows_ref.shape
    length //= 2
    outer, inner, cores, rows, _ = buffer_ref.shape
    rows //= 6
    parts = sems.shape[0]
    per_part = outer // parts
    per_block = blocks // parts
    core = core_ref[0]

    def fetch(part, half):
        at = pl.ds(part * per_part, per_part)
        slot, ref = ((core, own_ref), (1 - core, other_ref))[half]
        return pltpu.make_async_copy(ref.at[at], buffer_ref.at[at, :, slot], sems.at[part, half])

    for part in range(parts):
        fetch(part, 0).start()
        fetch(part, 1).start()
    channels = blocks * width
    total = jnp.zeros((length, width), F32)
    squares = jnp.zeros((length, width), F32)
    for at in range(blocks):
        total = total + rows_ref[at, :length, :].astype(F32)
    mean = jnp.sum(total, axis=1, keepdims=True) / channels
    for at in range(blocks):
        centred = rows_ref[at, :length, :].astype(F32) - mean
        squares = squares + centred * centred
    scale = lax.rsqrt(jnp.sum(squares, axis=1, keepdims=True) / channels + 1e-05)
    for at in range(blocks):
        centred = rows_ref[at, :length, :].astype(F32) - mean
        cols = slice(at * width, (at + 1) * width)
        act_ref[:, cols] = jax.nn.silu(centred * scale * gain_ref[:, cols] + shift_ref[:, cols]).astype(BF)
    span = per_part * inner * cores * rows
    for part in range(parts):
        fetch(part, 0).wait()
        fetch(part, 1).wait()
        conv_act = act_ref[:, part * span : (part + 1) * span]
        activated = jnp.concatenate(
            [rows_ref[part * per_block + at, length:, :] for at in range(per_block)], axis=1
        )
        for kind in range(6):
            block = buffer_ref[
                part * per_part : (part + 1) * per_part, :, :, kind * rows : (kind + 1) * rows, :
            ].reshape(span, width)
            product = jnp.dot(conv_act if kind < 2 else activated, block, preferred_element_type=F32)
            cols = slice(kind * width, (kind + 1) * width)
            acc_ref[:, cols] = product if part == 0 else acc_ref[:, cols] + product
    columns = 2 * width
    out_ref[...] = (
        acc_ref[:, :columns]
        + acc_ref[:, columns : 2 * columns] * jax.nn.sigmoid(acc_ref[:, 2 * columns :])
    ).astype(BF)


def grant(mib):
    return pltpu.CompilerParams(vmem_limit_bytes=mib << 20)


def whole(shape):
    return pl.BlockSpec(shape, lambda *_: (0,) * len(shape))


def spread(blocks, size):
    total, b = blocks.shape
    wide = total // size * b
    pick = lax.broadcasted_iota(jnp.int32, (b, wide), 1) % b == lax.broadcasted_iota(jnp.int32, (b, wide), 0)
    tiled = jnp.dot(blocks.astype(BF), pick.astype(BF), preferred_element_type=F32)
    row = lax.broadcasted_iota(jnp.int32, tiled.shape, 0) // size
    col = lax.broadcasted_iota(jnp.int32, tiled.shape, 1) // b
    return jnp.where(row == col, tiled, 0.0).astype(BF)


def rows_of(real, imag):
    n, s = real.shape
    return jnp.concatenate([real.reshape(n, s // LANES, LANES), imag.reshape(n, s // LANES, LANES)], axis=1)


def local(
    tokens,
    norm_gain,
    conv_value,
    conv_gate,
    state_feed,
    conv_taps,
    chan_gain,
    chan_shift,
    conv_project,
    decay_rate,
    frequency,
    input_real,
    input_imag,
    output_real,
    output_imag,
    skip_gain,
    state_value,
    state_gate,
    initial_state,
):
    seq_devices = lax.axis_size("z") * lax.axis_size("yh") * lax.axis_size("c")
    tp_devices = lax.axis_size("x") * lax.axis_size("yl")
    core = lax.axis_index("c")
    same = lax.axis_index("yl") == core
    position = (lax.axis_index("z") * lax.axis_size("yh") + lax.axis_index("yh")) * 2 + core
    length, model = tokens.shape
    rows_in, width = conv_value.shape
    rows_out, columns = conv_project.shape
    inner = lax.axis_size("yh")

    def swapped(value):
        return lax.ppermute(value, ("yl", "c"), [(a * 2 + b, b * 2 + a) for a in range(2) for b in range(2)])

    def packed(rows, *arrays):
        return pl.pallas_call(
            pack_kernel,
            out_shape=jax.ShapeDtypeStruct((rows, width), BF),
            name="pack",
        )(*arrays)

    def copies_of(shard):
        return jnp.broadcast_to(shard[None], (inner, *shard.shape))

    smem = pl.BlockSpec(memory_space=pltpu.SMEM)
    shard_first = packed(3 * rows_in, conv_value, conv_gate, state_feed)
    tokens, decay_rate, skip_gain, conv_taps, input_real, input_imag, output_real, output_imag, shard_first = (
        lax.optimization_barrier(
            (tokens, decay_rate, skip_gain, conv_taps, input_real, input_imag, output_real, output_imag, shard_first)
        )
    )
    blocks = []
    for shift in range(inner):
        pairs = [
            (h * 4 + a * 2 + b, (h + shift) % inner * 4 + b * 2 + a)
            for h in range(inner)
            for a in range(2)
            for b in range(2)
        ]
        blocks.append(lax.ppermute(shard_first, ("yh", "yl", "c"), pairs))
    places = (lax.axis_index("yh") - lax.iota(jnp.int32, inner)) % inner
    rows_first = pl.pallas_call(
        arrange_kernel,
        in_specs=[smem] + [whole(shard_first.shape)] * inner,
        out_shape=jax.ShapeDtypeStruct((inner, *shard_first.shape), BF),
        compiler_params=grant(4),
        name="arrange",
    )(places, *blocks)
    weights_first = lax.all_gather(rows_first, "z", axis=0, tiled=False)
    shard_last = packed(6 * rows_out, conv_project, state_value, state_gate)
    core_scalar = core.astype(jnp.int32).reshape(1)
    own_half = pl.pallas_call(
        norm_kernel,
        in_specs=[smem, whole(tokens.shape), whole((1, model))],
        out_shape=jax.ShapeDtypeStruct((length, model // 2), BF),
        name="norm",
    )(core_scalar, tokens, norm_gain.reshape(1, model))
    across = [(0, 1), (1, 0)]
    half_sent, _ = lax.optimization_barrier((own_half, rows_first))
    other_half = lax.ppermute(half_sent, "yl", across)
    shard_last, _ = lax.optimization_barrier((shard_last, rows_first))
    rows_last = lax.all_to_all(copies_of(swapped(shard_last)), "yh", 0, 0, tiled=True)
    keep = jnp.where(same, own_half, other_half)
    send = jnp.where(same, other_half, own_half)

    groups, state_size, group_size = input_real.shape
    small = groups * group_size
    parameters = [
        jnp.concatenate([jnp.swapaxes(p, 1, 2).reshape(small, state_size) for p in (input_real, input_imag)], axis=1),
        jnp.concatenate([p.reshape(small, state_size) for p in (output_real, output_imag)], axis=1),
        jnp.concatenate([decay_rate, frequency], axis=1),
        jnp.concatenate([initial_state[0], initial_state[1]], axis=1),
        conv_taps[:, :LANES],
        conv_taps[:, LANES:],
        skip_gain.reshape(width // LANES, LANES),
    ]
    ends_at = []
    for p in parameters:
        ends_at.append((ends_at[-1] if ends_at else 0) + p.shape[0])
    flat_parameters = jnp.concatenate(parameters, axis=0)
    flat_parameters = jnp.where(same, flat_parameters, lax.ppermute(flat_parameters, "c", across))
    flat_parameters, _ = lax.optimization_barrier((flat_parameters, own_half))
    inputs, outputs, rates, initial, taps_left, taps_right, skip = jnp.split(flat_parameters, ends_at[:-1], axis=0)
    conv_taps = jnp.concatenate([taps_left, taps_right], axis=1)
    input_real, input_imag = (
        part.reshape(groups, group_size, state_size) for part in jnp.split(inputs, 2, axis=1)
    )
    output_real, output_imag = (
        part.reshape(groups, group_size, state_size) for part in jnp.split(outputs, 2, axis=1)
    )
    decay_rate, frequency = jnp.split(rates, 2, axis=1)
    initial_state = jnp.split(initial, 2, axis=1)

    flat = groups * state_size
    total_tokens = length * seq_devices
    rate_real = -decay_rate / total_tokens
    magnitude = jnp.exp(rate_real)
    step_real = magnitude * jnp.cos(frequency)
    step_imag = magnitude * jnp.sin(frequency)
    modulus = rate_real * rate_real + frequency * frequency
    lift_real = step_real - 1.0
    factor_real = (lift_real * rate_real + step_imag * frequency) / modulus
    factor_imag = (step_imag * rate_real - lift_real * frequency) / modulus
    drive_real = factor_real[:, None] * input_real - factor_imag[:, None] * input_imag
    drive_imag = factor_real[:, None] * input_imag + factor_imag[:, None] * input_real

    drive_real = spread(drive_real.reshape(small, state_size), group_size)
    drive_imag = spread(drive_imag.reshape(small, state_size), group_size)
    mix_real = spread(jnp.swapaxes(output_real, 1, 2).reshape(flat, group_size), state_size)
    mix_imag = spread(jnp.swapaxes(-output_imag, 1, 2).reshape(flat, group_size), state_size)

    base_real = step_real.reshape(flat)
    base_imag = step_imag.reshape(flat)
    square_size = base_real * base_real + base_imag * base_imag

    def powers(real, imag):
        low = power_table(real, imag, lax.iota(jnp.int32, 8) + 1, 8)
        high = power_table(real, imag, lax.iota(jnp.int32, length // 8) * 8, length)
        table = rotate(high[0][:, None], high[1][:, None], low[0][None], low[1][None])
        return tuple(part.reshape(length, flat) for part in table)

    power_real, power_imag = powers(base_real, base_imag)
    undo_real, undo_imag = powers(base_real / square_size, -base_imag / square_size)
    span_real, span_imag = (power_real[-1], power_imag[-1])
    row_devices = inner * 2
    outer = seq_devices // row_devices
    in_row = position % row_devices
    row = position // row_devices
    lag = in_row - lax.iota(jnp.int32, row_devices)
    lag_rows = row - lax.iota(jnp.int32, outer)

    def spans(exponent, chosen=None):
        real, imag = power_table(span_real, span_imag, jnp.maximum(exponent, 0), seq_devices)
        if chosen is not None:
            real, imag = (part * chosen.astype(F32)[:, None] for part in (real, imag))
        return rows_of(real, imag)

    lead = spans(lag, lag > 0)
    tail = spans(row_devices - lax.iota(jnp.int32, row_devices))
    lead_rows = spans((lag_rows - 1) * row_devices + in_row, lag_rows > 0)
    tail_rows = spans((outer - 1 - lax.iota(jnp.int32, outer)) * row_devices)
    ends = rows_of(
        *rotate(
            *power_table(span_real, span_imag, jnp.stack([position, jnp.int32(seq_devices)]), seq_devices),
            initial_state[0].reshape(1, flat),
            initial_state[1].reshape(1, flat),
        )
    )
    (
        rows_last, keep, drive_real, drive_imag, mix_real, mix_imag, power_real, power_imag, undo_real, undo_imag, lead, tail, lead_rows,
        tail_rows, ends
    ) = lax.optimization_barrier((
        rows_last, keep, drive_real, drive_imag, mix_real, mix_imag, power_real, power_imag, undo_real, undo_imag, lead, tail, lead_rows,
        tail_rows, ends
    ))
    weights_last = lax.all_gather(rows_last, "z", axis=0, tiled=False)
    chunks = flat // LANES

    parts = 4
    hbm = pl.BlockSpec(memory_space=pl.ANY)
    kept, sent = pl.pallas_call(
        project_kernel,
        in_specs=[hbm, hbm, hbm],
        out_shape=[jax.ShapeDtypeStruct((length, 3 * width), F32)] * 2,
        scratch_shapes=[
            pltpu.VMEM(weights_first.shape, BF),
            pltpu.VMEM((parts, 2 * length, model // 2 // parts), BF),
            pltpu.SemaphoreType.DMA((parts,)),
            pltpu.SemaphoreType.DMA((parts, 2)),
        ],
        name="project",
    )(keep, send, weights_first)
    received = lax.ppermute(sent, "c", across)
    gated, feed, sums_real, sums_imag, total = pl.pallas_call(
        first_kernel,
        out_shape=[
            jax.ShapeDtypeStruct((length, width), BF),
            jax.ShapeDtypeStruct((length, width), BF),
            jax.ShapeDtypeStruct((length, flat), F32),
            jax.ShapeDtypeStruct((length, flat), F32),
            jax.ShapeDtypeStruct((row_devices, 2 * chunks, LANES), F32),
        ],
        scratch_shapes=[pltpu.VMEM((2 * chunks, LANES), F32)],
        name="first",
    )(kept, received, drive_real, drive_imag, undo_real, undo_imag)

    taps = conv_taps.shape[0]
    halo = (taps - 1 + 15) // 16 * 16
    before = lax.ppermute(
        gated[length - halo :], SEQUENCE, [(source, source + 1) for source in range(seq_devices - 1)]
    )
    totals = lax.all_to_all(total, SEQUENCE[1:], 0, 0, tiled=True)
    end_of_row = pl.pallas_call(
        row_kernel,
        out_shape=jax.ShapeDtypeStruct((outer, 2 * chunks, LANES), F32),
        name="row",
    )(totals, tail)
    ends_of_rows = lax.all_to_all(end_of_row, SEQUENCE[0], 0, 0, tiled=True)
    conv_out = pl.pallas_call(
        conv_kernel,
        out_shape=jax.ShapeDtypeStruct((length, width), BF),
        scratch_shapes=[pltpu.VMEM((halo + length, width), F32)],
        compiler_params=grant(4),
        name="conv",
    )(before, gated, conv_taps)

    copies, final = pl.pallas_call(
        second_kernel,
        out_shape=[
            jax.ShapeDtypeStruct((tp_devices, 2 * length, width), BF),
            jax.ShapeDtypeStruct((2 * chunks, LANES), F32),
        ],
        scratch_shapes=[pltpu.VMEM((2 * chunks, LANES), F32)],
        name="second",
    )(
        totals, lead, ends_of_rows, lead_rows, tail_rows, ends, power_real, power_imag, sums_real, sums_imag,
        mix_real, mix_imag, feed,
        skip.reshape(1, width), conv_out,
    )
    final = swapped(final)
    exchanged = lax.all_to_all(copies, ("x", "yl"), 0, 0, tiled=True)

    exchanged, final = lax.optimization_barrier((exchanged, final))
    weights_sent, _ = lax.optimization_barrier((weights_last, copies))
    weights_other = lax.ppermute(weights_sent, "c", across)
    mixed = pl.pallas_call(
        last_kernel,
        in_specs=[
            smem,
            whole(exchanged.shape),
            hbm,
            hbm,
            whole((1, chan_gain.shape[0])),
            whole((1, chan_gain.shape[0])),
        ],
        out_shape=jax.ShapeDtypeStruct((length, columns), BF),
        scratch_shapes=[
            pltpu.VMEM((*weights_last.shape[:2], 2, *weights_last.shape[2:]), BF),
            pltpu.VMEM((length, tp_devices * width), BF),
            pltpu.VMEM((length, 6 * width), F32),
            pltpu.SemaphoreType.DMA((parts, 2)),
        ],
        name="last",
    )(core_scalar, exchanged, weights_last, weights_other, chan_gain.reshape(1, -1), chan_shift.reshape(1, -1))
    mixer_out = swapped(mixed)
    return (mixer_out, final.reshape(2, groups, state_size))


def solution(mesh):
    mesh = Mesh(mesh.devices.reshape(8, 4, 2, 4, 2), ("z", "yh", "yl", "x", "c"))
    in_specs = (
        P(SP, None),
        P(),
        P(SP, TP),
        P(SP, TP),
        P(SP, TP),
        P(None, TP),
        P(),
        P(),
        P(SP, TP),
        P(TP, None),
        P(TP, None),
        P(TP, None, None),
        P(TP, None, None),
        P(TP, None, None),
        P(TP, None, None),
        P(TP),
        P(SP, TP),
        P(SP, TP),
        P(None, TP, None),
    )
    out_specs = (P(SP, TP), P(None, TP, None))
    return jax.shard_map(local, mesh=mesh, in_specs=in_specs, out_specs=out_specs, check_vma=False)
```

```python
import jax
import jax.numpy as jnp
from jax import lax
from jax.experimental import pallas as pl
from jax.experimental.pallas import tpu as pltpu
from jax.sharding import Mesh, PartitionSpec as P

BF = jnp.bfloat16
F32 = jnp.float32
LANES = 128
CHUNK = 256
SP = ("z", "yh", "yl")
TP = ("x", "c")
SEQUENCE = ("z", "yh", "c")


def rotate(first_real, first_imag, second_real, second_imag):
    return (
        first_real * second_real - first_imag * second_imag,
        first_real * second_imag + first_imag * second_real,
    )


def power_table(base_real, base_imag, exponent, largest):
    result_real = jnp.ones((exponent.shape[0], base_real.shape[0]), F32)
    result_imag = jnp.zeros((exponent.shape[0], base_real.shape[0]), F32)
    square_real, square_imag = (base_real, base_imag)
    for place in range(max(largest, 1).bit_length()):
        chosen = (exponent >> place & 1 == 1)[:, None]
        next_real, next_imag = rotate(result_real, result_imag, square_real, square_imag)
        result_real = jnp.where(chosen, next_real, result_real)
        result_imag = jnp.where(chosen, next_imag, result_imag)
        square_real, square_imag = rotate(square_real, square_imag, square_real, square_imag)
    return (result_real, result_imag)


def pack_kernel(*refs):
    out_ref = refs[-1]
    width = out_ref.shape[1]
    at = 0
    for ref in refs[:-1]:
        for col in range(0, ref.shape[1], width):
            out_ref[at : at + ref.shape[0]] = ref[:, col : col + width]
            at += ref.shape[0]


def arrange_kernel(places_ref, *refs):
    out_ref = refs[-1]
    for at, ref in enumerate(refs[:-1]):
        out_ref[places_ref[at]] = ref[...]


def norm_kernel(core_ref, tokens_ref, gain_ref, out_ref):
    floats = tokens_ref[...].astype(F32)
    model = floats.shape[1]
    scale = lax.rsqrt(jnp.sum(floats * floats, axis=1, keepdims=True) / model + 1e-06)
    first_core = core_ref[0] == 0
    low = lax.broadcasted_iota(jnp.int32, (floats.shape[0], LANES), 1) < LANES // 2
    for at in range(0, model, 2 * LANES):
        left = tokens_ref[:, at : at + LANES].astype(F32) * scale * gain_ref[:, at : at + LANES]
        right = (
            tokens_ref[:, at + LANES : at + 2 * LANES].astype(F32)
            * scale
            * gain_ref[:, at + LANES : at + 2 * LANES]
        )
        taken = jnp.where(
            low,
            jnp.where(first_core, left, pltpu.roll(left, LANES // 2, 1)),
            jnp.where(first_core, pltpu.roll(right, LANES // 2, 1), right),
        )
        out_ref[:, at // 2 : at // 2 + LANES] = taken.astype(BF)


def project_kernel(
    keep_ref, send_ref, weights_ref, keep_out_ref, send_out_ref, buffer_ref, tokens_ref, sems, token_sems
):
    outer, inner, rows, width = buffer_ref.shape
    rows //= 3
    parts = sems.shape[0]
    per_part = outer // parts
    length = keep_out_ref.shape[0]
    span = per_part * inner * rows

    def fetch(part):
        at = pl.ds(part * per_part, per_part)
        return pltpu.make_async_copy(weights_ref.at[at], buffer_ref.at[at], sems.at[part])

    def fetch_tokens(part, half):
        ref = (send_ref, keep_ref)[half]
        return pltpu.make_async_copy(
            ref.at[:, pl.ds(part * span, span)],
            tokens_ref.at[part, pl.ds(half * length, length)],
            token_sems.at[part, half],
        )

    for part in range(parts):
        fetch_tokens(part, 0).start()
        fetch_tokens(part, 1).start()
        fetch(part).start()
    for part in range(parts):
        fetch_tokens(part, 0).wait()
        fetch_tokens(part, 1).wait()
        fetch(part).wait()
        for kind in range(3):
            block = buffer_ref[
                part * per_part : (part + 1) * per_part, :, kind * rows : (kind + 1) * rows, :
            ].reshape(span, width)
            cols = slice(kind * width, (kind + 1) * width)
            product = jnp.dot(tokens_ref[part], block, preferred_element_type=F32)
            for at, out_ref in ((0, send_out_ref), (length, keep_out_ref)):
                its_rows = product[at : at + length]
                out_ref[:, cols] = its_rows if part == 0 else out_ref[:, cols] + its_rows


def first_kernel(
    kept_ref,
    received_ref,
    drive_real_ref,
    drive_imag_ref,
    undo_real_ref,
    undo_imag_ref,
    gated_ref,
    feed_ref,
    sums_real_ref,
    sums_imag_ref,
    total_ref,
    last_ref,
):
    length, width = gated_ref.shape
    feed = (kept_ref[:, 2 * width :] + received_ref[:, 2 * width :]).astype(BF)
    feed_ref[...] = feed
    lower = (
        lax.broadcasted_iota(jnp.int32, (length, length), 0)
        >= lax.broadcasted_iota(jnp.int32, (length, length), 1)
    ).astype(BF)
    flat = sums_real_ref.shape[1]
    half = last_ref.shape[0] // 2
    for at in range(0, flat, CHUNK):
        cols = slice(at, at + CHUNK)
        pushed_real = jnp.dot(feed, drive_real_ref[:, cols], preferred_element_type=F32)
        pushed_imag = jnp.dot(feed, drive_imag_ref[:, cols], preferred_element_type=F32)
        scaled = rotate(undo_real_ref[:, cols], undo_imag_ref[:, cols], pushed_real, pushed_imag)
        for part, ref in enumerate((sums_real_ref, sums_imag_ref)):
            sums = jnp.dot(lower, scaled[part].astype(BF), preferred_element_type=F32)
            ref[:, cols] = sums
            for lane in range(0, CHUNK, LANES):
                row = part * half + (at + lane) // LANES
                last_ref[row : row + 1, :] = sums[length - 1 :, lane : lane + LANES]
    total_ref[...] = jnp.broadcast_to(last_ref[...][None], total_ref.shape)
    value = kept_ref[:, :width] + received_ref[:, :width]
    gate = kept_ref[:, width : 2 * width] + received_ref[:, width : 2 * width]
    gated_ref[...] = (value * jax.nn.sigmoid(gate)).astype(BF)


def conv_kernel(before_ref, gated_ref, taps_ref, out_ref, pad_ref):
    length, width = gated_ref.shape
    lead = before_ref.shape[0]
    taps = taps_ref.shape[0]
    pad_ref[:lead] = before_ref[...].astype(F32)
    pad_ref[lead:] = gated_ref[...].astype(F32)
    for col in range(width // LANES):
        cols = slice(col * LANES, (col + 1) * LANES)
        acc = jnp.zeros((length, LANES), F32)
        for tap in range(taps):
            start = lead - (taps - 1) + tap
            acc = acc + taps_ref[tap : tap + 1, cols] * pad_ref[start : start + length, cols]
        out_ref[:, cols] = acc.astype(BF)


def weighted(weights_ref, values_ref):
    half = values_ref.shape[1] // 2
    real, imag = rotate(
        weights_ref[:, :half, :], weights_ref[:, half:, :], values_ref[:, :half, :], values_ref[:, half:, :]
    )
    return jnp.sum(real, axis=0), jnp.sum(imag, axis=0)


def row_kernel(totals_ref, tail_ref, out_ref):
    half = totals_ref.shape[1] // 2
    real, imag = weighted(tail_ref, totals_ref)
    for copy in range(out_ref.shape[0]):
        out_ref[copy, :half] = real
        out_ref[copy, half:] = imag


def second_kernel(
    totals_ref,
    lead_ref,
    ends_of_rows_ref,
    lead_rows_ref,
    tail_rows_ref,
    ends_ref,
    power_real_ref,
    power_imag_ref,
    sums_real_ref,
    sums_imag_ref,
    mix_real_ref,
    mix_imag_ref,
    feed_ref,
    skip_ref,
    conv_ref,
    out_ref,
    final_ref,
    entry_ref,
):
    half = final_ref.shape[0] // 2
    lead = weighted(lead_ref, totals_ref)
    lead_rows = weighted(lead_rows_ref, ends_of_rows_ref)
    tail_rows = weighted(tail_rows_ref, ends_of_rows_ref)
    for part in range(2):
        rows = slice(part * half, (part + 1) * half)
        entry_ref[rows] = ends_ref[0, rows] + lead[part] + lead_rows[part]
        final_ref[rows] = ends_ref[1, rows] + tail_rows[part]
    response = skip_ref[...] * feed_ref[...].astype(F32)
    for at in range(0, sums_real_ref.shape[1], CHUNK):
        cols = slice(at, at + CHUNK)
        rows = range(at // LANES, (at + CHUNK) // LANES)
        entry_real = jnp.concatenate([entry_ref[row : row + 1] for row in rows], axis=1)
        entry_imag = jnp.concatenate([entry_ref[half + row : half + row + 1] for row in rows], axis=1)
        state_real, state_imag = rotate(
            power_real_ref[:, cols],
            power_imag_ref[:, cols],
            sums_real_ref[:, cols] + entry_real,
            sums_imag_ref[:, cols] + entry_imag,
        )
        response = response + jnp.dot(state_real.astype(BF), mix_real_ref[cols, :], preferred_element_type=F32)
        response = response + jnp.dot(state_imag.astype(BF), mix_imag_ref[cols, :], preferred_element_type=F32)
    activated = jax.nn.gelu(response).astype(BF)
    length = activated.shape[0]
    conv = conv_ref[...]
    for copy in range(out_ref.shape[0]):
        out_ref[copy, :length] = conv
        out_ref[copy, length:] = activated


def last_kernel(
    core_ref, rows_ref, own_ref, other_ref, gain_ref, shift_ref, out_ref, buffer_ref, act_ref, acc_ref, sems
):
    blocks, length, width = rows_ref.shape
    length //= 2
    outer, inner, cores, rows, _ = buffer_ref.shape
    rows //= 6
    parts = sems.shape[0]
    per_part = outer // parts
    per_block = blocks // parts
    core = core_ref[0]

    def fetch(part, half):
        at = pl.ds(part * per_part, per_part)
        slot, ref = ((core, own_ref), (1 - core, other_ref))[half]
        return pltpu.make_async_copy(ref.at[at], buffer_ref.at[at, :, slot], sems.at[part, half])

    for part in range(parts):
        fetch(part, 0).start()
        fetch(part, 1).start()
    channels = blocks * width
    total = jnp.zeros((length, width), F32)
    squares = jnp.zeros((length, width), F32)
    for at in range(blocks):
        total = total + rows_ref[at, :length, :].astype(F32)
    mean = jnp.sum(total, axis=1, keepdims=True) / channels
    for at in range(blocks):
        centred = rows_ref[at, :length, :].astype(F32) - mean
        squares = squares + centred * centred
    scale = lax.rsqrt(jnp.sum(squares, axis=1, keepdims=True) / channels + 1e-05)
    for at in range(blocks):
        centred = rows_ref[at, :length, :].astype(F32) - mean
        cols = slice(at * width, (at + 1) * width)
        act_ref[:, cols] = jax.nn.silu(centred * scale * gain_ref[:, cols] + shift_ref[:, cols]).astype(BF)
    span = per_part * inner * cores * rows
    for part in range(parts):
        fetch(part, 0).wait()
        fetch(part, 1).wait()
        conv_act = act_ref[:, part * span : (part + 1) * span]
        activated = jnp.concatenate(
            [rows_ref[part * per_block + at, length:, :] for at in range(per_block)], axis=1
        )
        for kind in range(6):
            block = buffer_ref[
                part * per_part : (part + 1) * per_part, :, :, kind * rows : (kind + 1) * rows, :
            ].reshape(span, width)
            product = jnp.dot(conv_act if kind < 2 else activated, block, preferred_element_type=F32)
            cols = slice(kind * width, (kind + 1) * width)
            acc_ref[:, cols] = product if part == 0 else acc_ref[:, cols] + product
    columns = 2 * width
    out_ref[...] = (
        acc_ref[:, :columns]
        + acc_ref[:, columns : 2 * columns] * jax.nn.sigmoid(acc_ref[:, 2 * columns :])
    ).astype(BF)


def grant(mib):
    return pltpu.CompilerParams(vmem_limit_bytes=mib << 20)


def whole(shape):
    return pl.BlockSpec(shape, lambda *_: (0,) * len(shape))


def spread(blocks, size):
    total, b = blocks.shape
    wide = total // size * b
    pick = lax.broadcasted_iota(jnp.int32, (b, wide), 1) % b == lax.broadcasted_iota(jnp.int32, (b, wide), 0)
    tiled = jnp.dot(blocks.astype(BF), pick.astype(BF), preferred_element_type=F32)
    row = lax.broadcasted_iota(jnp.int32, tiled.shape, 0) // size
    col = lax.broadcasted_iota(jnp.int32, tiled.shape, 1) // b
    return jnp.where(row == col, tiled, 0.0).astype(BF)


def rows_of(real, imag):
    n, s = real.shape
    return jnp.concatenate([real.reshape(n, s // LANES, LANES), imag.reshape(n, s // LANES, LANES)], axis=1)


def local(
    tokens,
    norm_gain,
    conv_value,
    conv_gate,
    state_feed,
    conv_taps,
    chan_gain,
    chan_shift,
    conv_project,
    decay_rate,
    frequency,
    input_real,
    input_imag,
    output_real,
    output_imag,
    skip_gain,
    state_value,
    state_gate,
    initial_state,
):
    seq_devices = lax.axis_size("z") * lax.axis_size("yh") * lax.axis_size("c")
    tp_devices = lax.axis_size("x") * lax.axis_size("yl")
    core = lax.axis_index("c")
    same = lax.axis_index("yl") == core
    position = (lax.axis_index("z") * lax.axis_size("yh") + lax.axis_index("yh")) * 2 + core
    length, model = tokens.shape
    rows_in, width = conv_value.shape
    rows_out, columns = conv_project.shape
    inner = lax.axis_size("yh")

    def swapped(value):
        return lax.ppermute(value, ("yl", "c"), [(a * 2 + b, b * 2 + a) for a in range(2) for b in range(2)])

    def packed(rows, *arrays):
        return pl.pallas_call(
            pack_kernel,
            out_shape=jax.ShapeDtypeStruct((rows, width), BF),
            name="pack",
        )(*arrays)

    def copies_of(shard):
        return jnp.broadcast_to(shard[None], (inner, *shard.shape))

    smem = pl.BlockSpec(memory_space=pltpu.SMEM)
    shard_first = packed(3 * rows_in, conv_value, conv_gate, state_feed)
    decay_rate, skip_gain, conv_taps, input_real, input_imag, output_real, output_imag, shard_first = (
        lax.optimization_barrier(
            (decay_rate, skip_gain, conv_taps, input_real, input_imag, output_real, output_imag, shard_first)
        )
    )
    blocks = []
    for shift in range(inner):
        pairs = [
            (h * 4 + a * 2 + b, (h + shift) % inner * 4 + b * 2 + a)
            for h in range(inner)
            for a in range(2)
            for b in range(2)
        ]
        blocks.append(lax.ppermute(shard_first, ("yh", "yl", "c"), pairs))
    places = (lax.axis_index("yh") - lax.iota(jnp.int32, inner)) % inner
    rows_first = pl.pallas_call(
        arrange_kernel,
        in_specs=[smem] + [whole(shard_first.shape)] * inner,
        out_shape=jax.ShapeDtypeStruct((inner, *shard_first.shape), BF),
        compiler_params=grant(4),
        name="arrange",
    )(places, *blocks)
    weights_first = lax.all_gather(rows_first, "z", axis=0, tiled=False)
    tokens, conv_project, state_value, state_gate, _ = lax.optimization_barrier(
        (tokens, conv_project, state_value, state_gate, rows_first)
    )
    shard_last = packed(6 * rows_out, conv_project, state_value, state_gate)
    core_scalar = core.astype(jnp.int32).reshape(1)
    own_half = pl.pallas_call(
        norm_kernel,
        in_specs=[smem, whole(tokens.shape), whole((1, model))],
        out_shape=jax.ShapeDtypeStruct((length, model // 2), BF),
        name="norm",
    )(core_scalar, tokens, norm_gain.reshape(1, model))
    across = [(0, 1), (1, 0)]
    half_sent, _ = lax.optimization_barrier((own_half, rows_first))
    other_half = lax.ppermute(half_sent, "yl", across)
    shard_last, _ = lax.optimization_barrier((shard_last, rows_first))
    rows_last = lax.all_to_all(copies_of(swapped(shard_last)), "yh", 0, 0, tiled=True)
    keep = jnp.where(same, own_half, other_half)
    send = jnp.where(same, other_half, own_half)

    groups, state_size, group_size = input_real.shape
    small = groups * group_size
    parameters = [
        jnp.concatenate([jnp.swapaxes(p, 1, 2).reshape(small, state_size) for p in (input_real, input_imag)], axis=1),
        jnp.concatenate([p.reshape(small, state_size) for p in (output_real, output_imag)], axis=1),
        jnp.concatenate([decay_rate, frequency], axis=1),
        jnp.concatenate([initial_state[0], initial_state[1]], axis=1),
        conv_taps[:, :LANES],
        conv_taps[:, LANES:],
        skip_gain.reshape(width // LANES, LANES),
    ]
    ends_at = []
    for p in parameters:
        ends_at.append((ends_at[-1] if ends_at else 0) + p.shape[0])
    flat_parameters = jnp.concatenate(parameters, axis=0)
    flat_parameters = jnp.where(same, flat_parameters, lax.ppermute(flat_parameters, "c", across))
    flat_parameters, _ = lax.optimization_barrier((flat_parameters, own_half))
    inputs, outputs, rates, initial, taps_left, taps_right, skip = jnp.split(flat_parameters, ends_at[:-1], axis=0)
    conv_taps = jnp.concatenate([taps_left, taps_right], axis=1)
    input_real, input_imag = (
        part.reshape(groups, group_size, state_size) for part in jnp.split(inputs, 2, axis=1)
    )
    output_real, output_imag = (
        part.reshape(groups, group_size, state_size) for part in jnp.split(outputs, 2, axis=1)
    )
    decay_rate, frequency = jnp.split(rates, 2, axis=1)
    initial_state = jnp.split(initial, 2, axis=1)

    flat = groups * state_size
    total_tokens = length * seq_devices
    rate_real = -decay_rate / total_tokens
    magnitude = jnp.exp(rate_real)
    step_real = magnitude * jnp.cos(frequency)
    step_imag = magnitude * jnp.sin(frequency)
    modulus = rate_real * rate_real + frequency * frequency
    lift_real = step_real - 1.0
    factor_real = (lift_real * rate_real + step_imag * frequency) / modulus
    factor_imag = (step_imag * rate_real - lift_real * frequency) / modulus
    drive_real = factor_real[:, None] * input_real - factor_imag[:, None] * input_imag
    drive_imag = factor_real[:, None] * input_imag + factor_imag[:, None] * input_real

    drive_real = spread(drive_real.reshape(small, state_size), group_size)
    drive_imag = spread(drive_imag.reshape(small, state_size), group_size)
    mix_real = spread(jnp.swapaxes(output_real, 1, 2).reshape(flat, group_size), state_size)
    mix_imag = spread(jnp.swapaxes(-output_imag, 1, 2).reshape(flat, group_size), state_size)

    base_real = step_real.reshape(flat)
    base_imag = step_imag.reshape(flat)
    square_size = base_real * base_real + base_imag * base_imag

    counted = jnp.concatenate([lax.iota(jnp.int32, 8) + 1, lax.iota(jnp.int32, length // 8) * 8])
    counted_real, counted_imag = power_table(
        jnp.concatenate([base_real, base_real / square_size]),
        jnp.concatenate([base_imag, -base_imag / square_size]),
        counted,
        length,
    )

    def powers(cols):
        real, imag = (counted_real[:, cols], counted_imag[:, cols])
        table = rotate(real[8:, None], imag[8:, None], real[None, :8], imag[None, :8])
        return tuple(part.reshape(length, flat) for part in table)

    power_real, power_imag = powers(slice(0, flat))
    undo_real, undo_imag = powers(slice(flat, 2 * flat))
    span_real, span_imag = (power_real[-1], power_imag[-1])
    row_devices = inner * 2
    outer = seq_devices // row_devices
    in_row = position % row_devices
    row = position // row_devices
    lag = in_row - lax.iota(jnp.int32, row_devices)
    lag_rows = row - lax.iota(jnp.int32, outer)

    exponents = (
        lag,
        row_devices - lax.iota(jnp.int32, row_devices),
        (lag_rows - 1) * row_devices + in_row,
        (outer - 1 - lax.iota(jnp.int32, outer)) * row_devices,
        jnp.stack([position, jnp.int32(seq_devices)] + [jnp.int32(0)] * 6),
    )
    chosen = jnp.concatenate(
        [lag > 0, jnp.ones(row_devices, bool), lag_rows > 0, jnp.ones(outer + 8, bool)]
    ).astype(F32)[:, None]
    spans_real, spans_imag = power_table(
        span_real, span_imag, jnp.maximum(jnp.concatenate(exponents), 0), seq_devices
    )
    spans = rows_of(spans_real * chosen, spans_imag * chosen)
    cuts = (0, row_devices, 2 * row_devices, 2 * row_devices + outer, 2 * row_devices + 2 * outer)
    lead, tail, lead_rows, tail_rows = (spans[first:last] for first, last in zip(cuts[:-1], cuts[1:]))
    ends = rows_of(
        *rotate(
            spans_real[cuts[-1] : cuts[-1] + 2],
            spans_imag[cuts[-1] : cuts[-1] + 2],
            initial_state[0].reshape(1, flat),
            initial_state[1].reshape(1, flat),
        )
    )
    (
        rows_last, keep, drive_real, drive_imag, mix_real, mix_imag, power_real, power_imag, undo_real, undo_imag, lead, tail, lead_rows,
        tail_rows, ends
    ) = lax.optimization_barrier((
        rows_last, keep, drive_real, drive_imag, mix_real, mix_imag, power_real, power_imag, undo_real, undo_imag, lead, tail, lead_rows,
        tail_rows, ends
    ))
    weights_last = lax.all_gather(rows_last, "z", axis=0, tiled=False)
    chunks = flat // LANES

    parts = 4
    hbm = pl.BlockSpec(memory_space=pl.ANY)
    kept, sent = pl.pallas_call(
        project_kernel,
        in_specs=[hbm, hbm, hbm],
        out_shape=[jax.ShapeDtypeStruct((length, 3 * width), F32)] * 2,
        scratch_shapes=[
            pltpu.VMEM(weights_first.shape, BF),
            pltpu.VMEM((parts, 2 * length, model // 2 // parts), BF),
            pltpu.SemaphoreType.DMA((parts,)),
            pltpu.SemaphoreType.DMA((parts, 2)),
        ],
        name="project",
    )(keep, send, weights_first)
    received = lax.ppermute(sent, "c", across)
    gated, feed, sums_real, sums_imag, total = pl.pallas_call(
        first_kernel,
        out_shape=[
            jax.ShapeDtypeStruct((length, width), BF),
            jax.ShapeDtypeStruct((length, width), BF),
            jax.ShapeDtypeStruct((length, flat), F32),
            jax.ShapeDtypeStruct((length, flat), F32),
            jax.ShapeDtypeStruct((row_devices, 2 * chunks, LANES), F32),
        ],
        scratch_shapes=[pltpu.VMEM((2 * chunks, LANES), F32)],
        name="first",
    )(kept, received, drive_real, drive_imag, undo_real, undo_imag)

    taps = conv_taps.shape[0]
    halo = (taps - 1 + 15) // 16 * 16
    before = lax.ppermute(
        gated[length - halo :], SEQUENCE, [(source, source + 1) for source in range(seq_devices - 1)]
    )
    totals = lax.all_to_all(total, SEQUENCE[1:], 0, 0, tiled=True)
    end_of_row = pl.pallas_call(
        row_kernel,
        out_shape=jax.ShapeDtypeStruct((outer, 2 * chunks, LANES), F32),
        name="row",
    )(totals, tail)
    ends_of_rows = lax.all_to_all(end_of_row, SEQUENCE[0], 0, 0, tiled=True)
    conv_out = pl.pallas_call(
        conv_kernel,
        out_shape=jax.ShapeDtypeStruct((length, width), BF),
        scratch_shapes=[pltpu.VMEM((halo + length, width), F32)],
        compiler_params=grant(4),
        name="conv",
    )(before, gated, conv_taps)

    copies, final = pl.pallas_call(
        second_kernel,
        out_shape=[
            jax.ShapeDtypeStruct((tp_devices, 2 * length, width), BF),
            jax.ShapeDtypeStruct((2 * chunks, LANES), F32),
        ],
        scratch_shapes=[pltpu.VMEM((2 * chunks, LANES), F32)],
        name="second",
    )(
        totals, lead, ends_of_rows, lead_rows, tail_rows, ends, power_real, power_imag, sums_real, sums_imag,
        mix_real, mix_imag, feed,
        skip.reshape(1, width), conv_out,
    )
    final = swapped(final)
    exchanged = lax.all_to_all(copies, ("x", "yl"), 0, 0, tiled=True)

    exchanged, final = lax.optimization_barrier((exchanged, final))
    weights_sent, _ = lax.optimization_barrier((weights_last, copies))
    weights_other = lax.ppermute(weights_sent, "c", across)
    mixed = pl.pallas_call(
        last_kernel,
        in_specs=[
            smem,
            whole(exchanged.shape),
            hbm,
            hbm,
            whole((1, chan_gain.shape[0])),
            whole((1, chan_gain.shape[0])),
        ],
        out_shape=jax.ShapeDtypeStruct((length, columns), BF),
        scratch_shapes=[
            pltpu.VMEM((*weights_last.shape[:2], 2, *weights_last.shape[2:]), BF),
            pltpu.VMEM((length, tp_devices * width), BF),
            pltpu.VMEM((length, 6 * width), F32),
            pltpu.SemaphoreType.DMA((parts, 2)),
        ],
        name="last",
    )(core_scalar, exchanged, weights_last, weights_other, chan_gain.reshape(1, -1), chan_shift.reshape(1, -1))
    mixer_out = swapped(mixed)
    return (mixer_out, final.reshape(2, groups, state_size))


def solution(mesh):
    mesh = Mesh(mesh.devices.reshape(8, 4, 2, 4, 2), ("z", "yh", "yl", "x", "c"))
    in_specs = (
        P(SP, None),
        P(),
        P(SP, TP),
        P(SP, TP),
        P(SP, TP),
        P(None, TP),
        P(),
        P(),
        P(SP, TP),
        P(TP, None),
        P(TP, None),
        P(TP, None, None),
        P(TP, None, None),
        P(TP, None, None),
        P(TP, None, None),
        P(TP),
        P(SP, TP),
        P(SP, TP),
        P(None, TP, None),
    )
    out_specs = (P(SP, TP), P(None, TP, None))
    return jax.shard_map(local, mesh=mesh, in_specs=in_specs, out_specs=out_specs, check_vma=False)
```

```python
import jax
import jax.numpy as jnp
from jax import lax
from jax.experimental import pallas as pl
from jax.experimental.pallas import tpu as pltpu
from jax.sharding import Mesh, PartitionSpec as P

BF = jnp.bfloat16
F32 = jnp.float32
LANES = 128
CHUNK = 256
SP = ("z", "yh", "yl")
TP = ("x", "c")
SEQUENCE = ("z", "yh", "c")


def rotate(first_real, first_imag, second_real, second_imag):
    return (
        first_real * second_real - first_imag * second_imag,
        first_real * second_imag + first_imag * second_real,
    )


def power_table(base_real, base_imag, exponent, largest):
    result_real = jnp.ones((exponent.shape[0], base_real.shape[0]), F32)
    result_imag = jnp.zeros((exponent.shape[0], base_real.shape[0]), F32)
    square_real, square_imag = (base_real, base_imag)
    for place in range(max(largest, 1).bit_length()):
        chosen = (exponent >> place & 1 == 1)[:, None]
        next_real, next_imag = rotate(result_real, result_imag, square_real, square_imag)
        result_real = jnp.where(chosen, next_real, result_real)
        result_imag = jnp.where(chosen, next_imag, result_imag)
        square_real, square_imag = rotate(square_real, square_imag, square_real, square_imag)
    return (result_real, result_imag)


def pack_kernel(*refs):
    out_ref = refs[-1]
    width = out_ref.shape[1]
    at = 0
    for ref in refs[:-1]:
        for col in range(0, ref.shape[1], width):
            out_ref[at : at + ref.shape[0]] = ref[:, col : col + width]
            at += ref.shape[0]


def arrange_kernel(places_ref, *refs):
    out_ref = refs[-1]
    for at, ref in enumerate(refs[:-1]):
        out_ref[places_ref[at]] = ref[...]


def norm_kernel(core_ref, tokens_ref, gain_ref, out_ref):
    floats = tokens_ref[...].astype(F32)
    model = floats.shape[1]
    scale = lax.rsqrt(jnp.sum(floats * floats, axis=1, keepdims=True) / model + 1e-06)
    first_core = core_ref[0] == 0
    low = lax.broadcasted_iota(jnp.int32, (floats.shape[0], LANES), 1) < LANES // 2
    for at in range(0, model, 2 * LANES):
        left = tokens_ref[:, at : at + LANES].astype(F32) * scale * gain_ref[:, at : at + LANES]
        right = (
            tokens_ref[:, at + LANES : at + 2 * LANES].astype(F32)
            * scale
            * gain_ref[:, at + LANES : at + 2 * LANES]
        )
        taken = jnp.where(
            low,
            jnp.where(first_core, left, pltpu.roll(left, LANES // 2, 1)),
            jnp.where(first_core, pltpu.roll(right, LANES // 2, 1), right),
        )
        out_ref[:, at // 2 : at // 2 + LANES] = taken.astype(BF)


def project_kernel(
    keep_ref, send_ref, weights_ref, keep_out_ref, send_out_ref, buffer_ref, tokens_ref, sems, token_sems
):
    outer, inner, rows, width = buffer_ref.shape
    rows //= 3
    parts = sems.shape[0]
    per_part = outer // parts
    length = keep_out_ref.shape[0]
    span = per_part * inner * rows

    def fetch(part):
        at = pl.ds(part * per_part, per_part)
        return pltpu.make_async_copy(weights_ref.at[at], buffer_ref.at[at], sems.at[part])

    def fetch_tokens(part, half):
        ref = (send_ref, keep_ref)[half]
        return pltpu.make_async_copy(
            ref.at[:, pl.ds(part * span, span)],
            tokens_ref.at[part, pl.ds(half * length, length)],
            token_sems.at[part, half],
        )

    for part in range(parts):
        fetch_tokens(part, 0).start()
        fetch_tokens(part, 1).start()
        fetch(part).start()
    for part in range(parts):
        fetch_tokens(part, 0).wait()
        fetch_tokens(part, 1).wait()
        fetch(part).wait()
        for kind in range(3):
            block = buffer_ref[
                part * per_part : (part + 1) * per_part, :, kind * rows : (kind + 1) * rows, :
            ].reshape(span, width)
            cols = slice(kind * width, (kind + 1) * width)
            product = jnp.dot(tokens_ref[part], block, preferred_element_type=F32)
            for at, out_ref in ((0, send_out_ref), (length, keep_out_ref)):
                its_rows = product[at : at + length]
                out_ref[:, cols] = its_rows if part == 0 else out_ref[:, cols] + its_rows


def first_kernel(
    kept_ref,
    received_ref,
    drive_real_ref,
    drive_imag_ref,
    undo_real_ref,
    undo_imag_ref,
    gated_ref,
    feed_ref,
    sums_real_ref,
    sums_imag_ref,
    total_ref,
    last_ref,
):
    length, width = gated_ref.shape
    feed = (kept_ref[:, 2 * width :] + received_ref[:, 2 * width :]).astype(BF)
    feed_ref[...] = feed
    lower = (
        lax.broadcasted_iota(jnp.int32, (length, length), 0)
        >= lax.broadcasted_iota(jnp.int32, (length, length), 1)
    ).astype(BF)
    flat = sums_real_ref.shape[1]
    half = last_ref.shape[0] // 2
    for at in range(0, flat, CHUNK):
        cols = slice(at, at + CHUNK)
        pushed_real = jnp.dot(feed, drive_real_ref[:, cols], preferred_element_type=F32)
        pushed_imag = jnp.dot(feed, drive_imag_ref[:, cols], preferred_element_type=F32)
        scaled = rotate(undo_real_ref[:, cols], undo_imag_ref[:, cols], pushed_real, pushed_imag)
        for part, ref in enumerate((sums_real_ref, sums_imag_ref)):
            sums = jnp.dot(lower, scaled[part].astype(BF), preferred_element_type=F32)
            ref[:, cols] = sums
            for lane in range(0, CHUNK, LANES):
                row = part * half + (at + lane) // LANES
                last_ref[row : row + 1, :] = sums[length - 1 :, lane : lane + LANES]
    total_ref[...] = jnp.broadcast_to(last_ref[...][None], total_ref.shape)
    value = kept_ref[:, :width] + received_ref[:, :width]
    gate = kept_ref[:, width : 2 * width] + received_ref[:, width : 2 * width]
    gated_ref[...] = (value * jax.nn.sigmoid(gate)).astype(BF)


def conv_kernel(before_ref, gated_ref, taps_ref, out_ref, pad_ref):
    length, width = gated_ref.shape
    lead = before_ref.shape[0]
    taps = taps_ref.shape[0]
    pad_ref[:lead] = before_ref[...].astype(F32)
    pad_ref[lead:] = gated_ref[...].astype(F32)
    for col in range(width // LANES):
        cols = slice(col * LANES, (col + 1) * LANES)
        acc = jnp.zeros((length, LANES), F32)
        for tap in range(taps):
            start = lead - (taps - 1) + tap
            acc = acc + taps_ref[tap : tap + 1, cols] * pad_ref[start : start + length, cols]
        out_ref[:, cols] = acc.astype(BF)


def weighted(weights_ref, values_ref):
    half = values_ref.shape[1] // 2
    real, imag = rotate(
        weights_ref[:, :half, :], weights_ref[:, half:, :], values_ref[:, :half, :], values_ref[:, half:, :]
    )
    return jnp.sum(real, axis=0), jnp.sum(imag, axis=0)


def row_kernel(totals_ref, tail_ref, out_ref):
    half = totals_ref.shape[1] // 2
    real, imag = weighted(tail_ref, totals_ref)
    for copy in range(out_ref.shape[0]):
        out_ref[copy, :half] = real
        out_ref[copy, half:] = imag


def second_kernel(
    totals_ref,
    lead_ref,
    ends_of_rows_ref,
    lead_rows_ref,
    tail_rows_ref,
    ends_ref,
    power_real_ref,
    power_imag_ref,
    sums_real_ref,
    sums_imag_ref,
    mix_real_ref,
    mix_imag_ref,
    feed_ref,
    skip_ref,
    out_ref,
    final_ref,
    entry_ref,
):
    half = final_ref.shape[0] // 2
    lead = weighted(lead_ref, totals_ref)
    lead_rows = weighted(lead_rows_ref, ends_of_rows_ref)
    tail_rows = weighted(tail_rows_ref, ends_of_rows_ref)
    for part in range(2):
        rows = slice(part * half, (part + 1) * half)
        entry_ref[rows] = ends_ref[0, rows] + lead[part] + lead_rows[part]
        final_ref[rows] = ends_ref[1, rows] + tail_rows[part]
    response = skip_ref[...] * feed_ref[...].astype(F32)
    for at in range(0, sums_real_ref.shape[1], CHUNK):
        cols = slice(at, at + CHUNK)
        rows = range(at // LANES, (at + CHUNK) // LANES)
        entry_real = jnp.concatenate([entry_ref[row : row + 1] for row in rows], axis=1)
        entry_imag = jnp.concatenate([entry_ref[half + row : half + row + 1] for row in rows], axis=1)
        state_real, state_imag = rotate(
            power_real_ref[:, cols],
            power_imag_ref[:, cols],
            sums_real_ref[:, cols] + entry_real,
            sums_imag_ref[:, cols] + entry_imag,
        )
        response = response + jnp.dot(state_real.astype(BF), mix_real_ref[cols, :], preferred_element_type=F32)
        response = response + jnp.dot(state_imag.astype(BF), mix_imag_ref[cols, :], preferred_element_type=F32)
    activated = jax.nn.gelu(response).astype(BF)
    for copy in range(out_ref.shape[0]):
        out_ref[copy] = activated


def last_kernel(
    place_ref, conv_own_ref, conv_other_ref, rows_ref, own_ref, other_ref, gain_ref, shift_ref, out_ref, buffer_ref, act_ref, acc_ref, sems
):
    blocks, length, width = rows_ref.shape
    outer, inner, cores, rows, _ = buffer_ref.shape
    rows //= 6
    parts = sems.shape[0]
    per_part = outer // parts
    per_block = blocks // parts
    core = place_ref[0]

    def fetch(part, half):
        at = pl.ds(part * per_part, per_part)
        slot, ref = ((core, own_ref), (1 - core, other_ref))[half]
        return pltpu.make_async_copy(ref.at[at], buffer_ref.at[at, :, slot], sems.at[part, half])

    for part in range(parts):
        fetch(part, 0).start()
        fetch(part, 1).start()
    def conv_block(at):
        return jnp.where(place_ref[1] == at % 2, conv_own_ref[at // 2], conv_other_ref[at // 2]).astype(F32)

    channels = blocks * width
    total = jnp.zeros((length, width), F32)
    squares = jnp.zeros((length, width), F32)
    for at in range(blocks):
        total = total + conv_block(at)
    mean = jnp.sum(total, axis=1, keepdims=True) / channels
    for at in range(blocks):
        centred = conv_block(at) - mean
        squares = squares + centred * centred
    scale = lax.rsqrt(jnp.sum(squares, axis=1, keepdims=True) / channels + 1e-05)
    for at in range(blocks):
        centred = conv_block(at) - mean
        cols = slice(at * width, (at + 1) * width)
        act_ref[:, cols] = jax.nn.silu(centred * scale * gain_ref[:, cols] + shift_ref[:, cols]).astype(BF)
    span = per_part * inner * cores * rows
    for part in range(parts):
        fetch(part, 0).wait()
        fetch(part, 1).wait()
        conv_act = act_ref[:, part * span : (part + 1) * span]
        activated = jnp.concatenate(
            [rows_ref[part * per_block + at] for at in range(per_block)], axis=1
        )
        for kind in range(6):
            block = buffer_ref[
                part * per_part : (part + 1) * per_part, :, :, kind * rows : (kind + 1) * rows, :
            ].reshape(span, width)
            product = jnp.dot(conv_act if kind < 2 else activated, block, preferred_element_type=F32)
            cols = slice(kind * width, (kind + 1) * width)
            acc_ref[:, cols] = product if part == 0 else acc_ref[:, cols] + product
    columns = 2 * width
    out_ref[...] = (
        acc_ref[:, :columns]
        + acc_ref[:, columns : 2 * columns] * jax.nn.sigmoid(acc_ref[:, 2 * columns :])
    ).astype(BF)


def grant(mib):
    return pltpu.CompilerParams(vmem_limit_bytes=mib << 20)


def whole(shape):
    return pl.BlockSpec(shape, lambda *_: (0,) * len(shape))


def spread(blocks, size):
    total, b = blocks.shape
    wide = total // size * b
    pick = lax.broadcasted_iota(jnp.int32, (b, wide), 1) % b == lax.broadcasted_iota(jnp.int32, (b, wide), 0)
    tiled = jnp.dot(blocks.astype(BF), pick.astype(BF), preferred_element_type=F32)
    row = lax.broadcasted_iota(jnp.int32, tiled.shape, 0) // size
    col = lax.broadcasted_iota(jnp.int32, tiled.shape, 1) // b
    return jnp.where(row == col, tiled, 0.0).astype(BF)


def rows_of(real, imag):
    n, s = real.shape
    return jnp.concatenate([real.reshape(n, s // LANES, LANES), imag.reshape(n, s // LANES, LANES)], axis=1)


def local(
    tokens,
    norm_gain,
    conv_value,
    conv_gate,
    state_feed,
    conv_taps,
    chan_gain,
    chan_shift,
    conv_project,
    decay_rate,
    frequency,
    input_real,
    input_imag,
    output_real,
    output_imag,
    skip_gain,
    state_value,
    state_gate,
    initial_state,
):
    seq_devices = lax.axis_size("z") * lax.axis_size("yh") * lax.axis_size("c")
    tp_devices = lax.axis_size("x") * lax.axis_size("yl")
    core = lax.axis_index("c")
    same = lax.axis_index("yl") == core
    position = (lax.axis_index("z") * lax.axis_size("yh") + lax.axis_index("yh")) * 2 + core
    length, model = tokens.shape
    rows_in, width = conv_value.shape
    rows_out, columns = conv_project.shape
    inner = lax.axis_size("yh")

    def swapped(value):
        return lax.ppermute(value, ("yl", "c"), [(a * 2 + b, b * 2 + a) for a in range(2) for b in range(2)])

    def packed(rows, *arrays):
        return pl.pallas_call(
            pack_kernel,
            out_shape=jax.ShapeDtypeStruct((rows, width), BF),
            name="pack",
        )(*arrays)

    def copies_of(shard):
        return jnp.broadcast_to(shard[None], (inner, *shard.shape))

    smem = pl.BlockSpec(memory_space=pltpu.SMEM)
    shard_first = packed(3 * rows_in, conv_value, conv_gate, state_feed)
    decay_rate, skip_gain, conv_taps, input_real, input_imag, output_real, output_imag, shard_first = (
        lax.optimization_barrier(
            (decay_rate, skip_gain, conv_taps, input_real, input_imag, output_real, output_imag, shard_first)
        )
    )
    blocks = []
    for shift in range(inner):
        pairs = [
            (h * 4 + a * 2 + b, (h + shift) % inner * 4 + b * 2 + a)
            for h in range(inner)
            for a in range(2)
            for b in range(2)
        ]
        blocks.append(lax.ppermute(shard_first, ("yh", "yl", "c"), pairs))
    places = (lax.axis_index("yh") - lax.iota(jnp.int32, inner)) % inner

    def arranged(places, blocks):
        shape = blocks[0].shape
        return pl.pallas_call(
            arrange_kernel,
            in_specs=[smem] + [whole(shape)] * len(blocks),
            out_shape=jax.ShapeDtypeStruct((len(blocks), *shape), BF),
            compiler_params=grant(4),
            name="arrange",
        )(places, *blocks)

    rows_first = arranged(places, blocks)
    weights_first = lax.all_gather(rows_first, "z", axis=0, tiled=False)
    tokens, conv_project, state_value, state_gate, _ = lax.optimization_barrier(
        (tokens, conv_project, state_value, state_gate, rows_first)
    )
    shard_last = packed(6 * rows_out, conv_project, state_value, state_gate)
    core_scalar = core.astype(jnp.int32).reshape(1)
    own_half = pl.pallas_call(
        norm_kernel,
        in_specs=[smem, whole(tokens.shape), whole((1, model))],
        out_shape=jax.ShapeDtypeStruct((length, model // 2), BF),
        name="norm",
    )(core_scalar, tokens, norm_gain.reshape(1, model))
    across = [(0, 1), (1, 0)]
    half_sent, _ = lax.optimization_barrier((own_half, rows_first))
    other_half = lax.ppermute(half_sent, "yl", across)
    shard_last, _ = lax.optimization_barrier((shard_last, rows_first))
    rows_last = lax.all_to_all(copies_of(swapped(shard_last)), "yh", 0, 0, tiled=True)
    keep = jnp.where(same, own_half, other_half)
    send = jnp.where(same, other_half, own_half)

    groups, state_size, group_size = input_real.shape
    small = groups * group_size
    parameters = [
        jnp.concatenate([jnp.swapaxes(p, 1, 2).reshape(small, state_size) for p in (input_real, input_imag)], axis=1),
        jnp.concatenate([p.reshape(small, state_size) for p in (output_real, output_imag)], axis=1),
        jnp.concatenate([decay_rate, frequency], axis=1),
        jnp.concatenate([initial_state[0], initial_state[1]], axis=1),
        conv_taps[:, :LANES],
        conv_taps[:, LANES:],
        skip_gain.reshape(width // LANES, LANES),
    ]
    ends_at = []
    for p in parameters:
        ends_at.append((ends_at[-1] if ends_at else 0) + p.shape[0])
    flat_parameters = jnp.concatenate(parameters, axis=0)
    flat_parameters = jnp.where(same, flat_parameters, lax.ppermute(flat_parameters, "c", across))
    flat_parameters, _ = lax.optimization_barrier((flat_parameters, own_half))
    inputs, outputs, rates, initial, taps_left, taps_right, skip = jnp.split(flat_parameters, ends_at[:-1], axis=0)
    conv_taps = jnp.concatenate([taps_left, taps_right], axis=1)
    input_real, input_imag = (
        part.reshape(groups, group_size, state_size) for part in jnp.split(inputs, 2, axis=1)
    )
    output_real, output_imag = (
        part.reshape(groups, group_size, state_size) for part in jnp.split(outputs, 2, axis=1)
    )
    decay_rate, frequency = jnp.split(rates, 2, axis=1)
    initial_state = jnp.split(initial, 2, axis=1)

    flat = groups * state_size
    total_tokens = length * seq_devices
    rate_real = -decay_rate / total_tokens
    magnitude = jnp.exp(rate_real)
    step_real = magnitude * jnp.cos(frequency)
    step_imag = magnitude * jnp.sin(frequency)
    modulus = rate_real * rate_real + frequency * frequency
    lift_real = step_real - 1.0
    factor_real = (lift_real * rate_real + step_imag * frequency) / modulus
    factor_imag = (step_imag * rate_real - lift_real * frequency) / modulus
    drive_real = factor_real[:, None] * input_real - factor_imag[:, None] * input_imag
    drive_imag = factor_real[:, None] * input_imag + factor_imag[:, None] * input_real

    drive_real = spread(drive_real.reshape(small, state_size), group_size)
    drive_imag = spread(drive_imag.reshape(small, state_size), group_size)
    mix_real = spread(jnp.swapaxes(output_real, 1, 2).reshape(flat, group_size), state_size)
    mix_imag = spread(jnp.swapaxes(-output_imag, 1, 2).reshape(flat, group_size), state_size)

    base_real = step_real.reshape(flat)
    base_imag = step_imag.reshape(flat)
    square_size = base_real * base_real + base_imag * base_imag

    counted = jnp.concatenate([lax.iota(jnp.int32, 8) + 1, lax.iota(jnp.int32, length // 8) * 8])
    counted_real, counted_imag = power_table(
        jnp.concatenate([base_real, base_real / square_size]),
        jnp.concatenate([base_imag, -base_imag / square_size]),
        counted,
        length,
    )

    def powers(cols):
        real, imag = (counted_real[:, cols], counted_imag[:, cols])
        table = rotate(real[8:, None], imag[8:, None], real[None, :8], imag[None, :8])
        return tuple(part.reshape(length, flat) for part in table)

    power_real, power_imag = powers(slice(0, flat))
    undo_real, undo_imag = powers(slice(flat, 2 * flat))
    span_real, span_imag = (power_real[-1], power_imag[-1])
    row_devices = inner * 2
    outer = seq_devices // row_devices
    in_row = position % row_devices
    row = position // row_devices
    lag = in_row - lax.iota(jnp.int32, row_devices)
    lag_rows = row - lax.iota(jnp.int32, outer)

    exponents = (
        lag,
        row_devices - lax.iota(jnp.int32, row_devices),
        (lag_rows - 1) * row_devices + in_row,
        (outer - 1 - lax.iota(jnp.int32, outer)) * row_devices,
        jnp.stack([position, jnp.int32(seq_devices)] + [jnp.int32(0)] * 6),
    )
    chosen = jnp.concatenate(
        [lag > 0, jnp.ones(row_devices, bool), lag_rows > 0, jnp.ones(outer + 8, bool)]
    ).astype(F32)[:, None]
    spans_real, spans_imag = power_table(
        span_real, span_imag, jnp.maximum(jnp.concatenate(exponents), 0), seq_devices
    )
    spans = rows_of(spans_real * chosen, spans_imag * chosen)
    cuts = (0, row_devices, 2 * row_devices, 2 * row_devices + outer, 2 * row_devices + 2 * outer)
    lead, tail, lead_rows, tail_rows = (spans[first:last] for first, last in zip(cuts[:-1], cuts[1:]))
    ends = rows_of(
        *rotate(
            spans_real[cuts[-1] : cuts[-1] + 2],
            spans_imag[cuts[-1] : cuts[-1] + 2],
            initial_state[0].reshape(1, flat),
            initial_state[1].reshape(1, flat),
        )
    )
    (
        rows_last, keep, drive_real, drive_imag, mix_real, mix_imag, power_real, power_imag, undo_real, undo_imag, lead, tail, lead_rows,
        tail_rows, ends
    ) = lax.optimization_barrier((
        rows_last, keep, drive_real, drive_imag, mix_real, mix_imag, power_real, power_imag, undo_real, undo_imag, lead, tail, lead_rows,
        tail_rows, ends
    ))
    weights_last = lax.all_gather(rows_last, "z", axis=0, tiled=False)
    chunks = flat // LANES

    parts = 4
    hbm = pl.BlockSpec(memory_space=pl.ANY)
    kept, sent = pl.pallas_call(
        project_kernel,
        in_specs=[hbm, hbm, hbm],
        out_shape=[jax.ShapeDtypeStruct((length, 3 * width), F32)] * 2,
        scratch_shapes=[
            pltpu.VMEM(weights_first.shape, BF),
            pltpu.VMEM((parts, 2 * length, model // 2 // parts), BF),
            pltpu.SemaphoreType.DMA((parts,)),
            pltpu.SemaphoreType.DMA((parts, 2)),
        ],
        name="project",
    )(keep, send, weights_first)
    received = lax.ppermute(sent, "c", across)
    gated, feed, sums_real, sums_imag, total = pl.pallas_call(
        first_kernel,
        out_shape=[
            jax.ShapeDtypeStruct((length, width), BF),
            jax.ShapeDtypeStruct((length, width), BF),
            jax.ShapeDtypeStruct((length, flat), F32),
            jax.ShapeDtypeStruct((length, flat), F32),
            jax.ShapeDtypeStruct((row_devices, 2 * chunks, LANES), F32),
        ],
        scratch_shapes=[pltpu.VMEM((2 * chunks, LANES), F32)],
        name="first",
    )(kept, received, drive_real, drive_imag, undo_real, undo_imag)

    taps = conv_taps.shape[0]
    halo = (taps - 1 + 15) // 16 * 16
    before = lax.ppermute(
        gated[length - halo :], SEQUENCE, [(source, source + 1) for source in range(seq_devices - 1)]
    )
    totals = lax.all_to_all(total, SEQUENCE[1:], 0, 0, tiled=True)
    end_of_row = pl.pallas_call(
        row_kernel,
        out_shape=jax.ShapeDtypeStruct((outer, 2 * chunks, LANES), F32),
        name="row",
    )(totals, tail)
    conv_out = pl.pallas_call(
        conv_kernel,
        out_shape=jax.ShapeDtypeStruct((length, width), BF),
        scratch_shapes=[pltpu.VMEM((halo + length, width), F32)],
        compiler_params=grant(4),
        name="conv",
    )(before, gated, conv_taps)

    spread_x = lax.axis_size("x")
    conv_blocks = [conv_out] + [
        lax.ppermute(conv_out, "x", [(i, (i + shift) % spread_x) for i in range(spread_x)])
        for shift in range(1, spread_x)
    ]
    conv_own = arranged((lax.axis_index("x") - lax.iota(jnp.int32, spread_x)) % spread_x, conv_blocks)
    end_of_row, conv_own = lax.optimization_barrier((end_of_row, conv_own))
    ends_of_rows = lax.all_to_all(end_of_row, SEQUENCE[0], 0, 0, tiled=True)
    conv_other = lax.ppermute(conv_own, "yl", across)
    place = jnp.stack([core, lax.axis_index("yl")]).astype(jnp.int32)

    copies, final = pl.pallas_call(
        second_kernel,
        out_shape=[
            jax.ShapeDtypeStruct((tp_devices, length, width), BF),
            jax.ShapeDtypeStruct((2 * chunks, LANES), F32),
        ],
        scratch_shapes=[pltpu.VMEM((2 * chunks, LANES), F32)],
        name="second",
    )(
        totals, lead, ends_of_rows, lead_rows, tail_rows, ends, power_real, power_imag, sums_real, sums_imag,
        mix_real, mix_imag, feed,
        skip.reshape(1, width),
    )
    final = swapped(final)
    exchanged = lax.all_to_all(copies, ("x", "yl"), 0, 0, tiled=True)

    exchanged, final = lax.optimization_barrier((exchanged, final))
    weights_sent, _ = lax.optimization_barrier((weights_last, copies))
    weights_other = lax.ppermute(weights_sent, "c", across)
    mixed = pl.pallas_call(
        last_kernel,
        in_specs=[
            smem,
            whole(conv_own.shape),
            whole(conv_other.shape),
            whole(exchanged.shape),
            hbm,
            hbm,
            whole((1, chan_gain.shape[0])),
            whole((1, chan_gain.shape[0])),
        ],
        out_shape=jax.ShapeDtypeStruct((length, columns), BF),
        scratch_shapes=[
            pltpu.VMEM((*weights_last.shape[:2], 2, *weights_last.shape[2:]), BF),
            pltpu.VMEM((length, tp_devices * width), BF),
            pltpu.VMEM((length, 6 * width), F32),
            pltpu.SemaphoreType.DMA((parts, 2)),
        ],
        name="last",
    )(place, conv_own, conv_other, exchanged, weights_last, weights_other, chan_gain.reshape(1, -1), chan_shift.reshape(1, -1))
    mixer_out = swapped(mixed)
    return (mixer_out, final.reshape(2, groups, state_size))


def solution(mesh):
    mesh = Mesh(mesh.devices.reshape(8, 4, 2, 4, 2), ("z", "yh", "yl", "x", "c"))
    in_specs = (
        P(SP, None),
        P(),
        P(SP, TP),
        P(SP, TP),
        P(SP, TP),
        P(None, TP),
        P(),
        P(),
        P(SP, TP),
        P(TP, None),
        P(TP, None),
        P(TP, None, None),
        P(TP, None, None),
        P(TP, None, None),
        P(TP, None, None),
        P(TP),
        P(SP, TP),
        P(SP, TP),
        P(None, TP, None),
    )
    out_specs = (P(SP, TP), P(None, TP, None))
    return jax.shard_map(local, mesh=mesh, in_specs=in_specs, out_specs=out_specs, check_vma=False)
```

```python
import jax
import jax.numpy as jnp
from jax import lax
from jax.experimental import pallas as pl
from jax.experimental.pallas import tpu as pltpu
from jax.sharding import Mesh, PartitionSpec as P

BF = jnp.bfloat16
F32 = jnp.float32
LANES = 128
CHUNK = 256
SP = ("z", "yh", "yl")
TP = ("x", "c")
SEQUENCE = ("z", "yh", "c")


def rotate(first_real, first_imag, second_real, second_imag):
    return (
        first_real * second_real - first_imag * second_imag,
        first_real * second_imag + first_imag * second_real,
    )


def power_table(base_real, base_imag, exponent, largest):
    result_real = jnp.ones((exponent.shape[0], base_real.shape[0]), F32)
    result_imag = jnp.zeros((exponent.shape[0], base_real.shape[0]), F32)
    square_real, square_imag = (base_real, base_imag)
    for place in range(max(largest, 1).bit_length()):
        chosen = (exponent >> place & 1 == 1)[:, None]
        next_real, next_imag = rotate(result_real, result_imag, square_real, square_imag)
        result_real = jnp.where(chosen, next_real, result_real)
        result_imag = jnp.where(chosen, next_imag, result_imag)
        square_real, square_imag = rotate(square_real, square_imag, square_real, square_imag)
    return (result_real, result_imag)


def pack_kernel(*refs):
    out_ref = refs[-1]
    width = out_ref.shape[1]
    at = 0
    for ref in refs[:-1]:
        for col in range(0, ref.shape[1], width):
            out_ref[at : at + ref.shape[0]] = ref[:, col : col + width]
            at += ref.shape[0]


def arrange_kernel(places_ref, *refs):
    out_ref = refs[-1]
    for at, ref in enumerate(refs[:-1]):
        out_ref[places_ref[at]] = ref[...]


def norm_kernel(core_ref, tokens_ref, gain_ref, out_ref):
    floats = tokens_ref[...].astype(F32)
    model = floats.shape[1]
    scale = lax.rsqrt(jnp.sum(floats * floats, axis=1, keepdims=True) / model + 1e-06)
    first_core = core_ref[0] == 0
    low = lax.broadcasted_iota(jnp.int32, (floats.shape[0], LANES), 1) < LANES // 2
    for at in range(0, model, 2 * LANES):
        left = tokens_ref[:, at : at + LANES].astype(F32) * scale * gain_ref[:, at : at + LANES]
        right = (
            tokens_ref[:, at + LANES : at + 2 * LANES].astype(F32)
            * scale
            * gain_ref[:, at + LANES : at + 2 * LANES]
        )
        taken = jnp.where(
            low,
            jnp.where(first_core, left, pltpu.roll(left, LANES // 2, 1)),
            jnp.where(first_core, pltpu.roll(right, LANES // 2, 1), right),
        )
        out_ref[:, at // 2 : at // 2 + LANES] = taken.astype(BF)


def project_kernel(
    keep_ref, send_ref, weights_ref, keep_out_ref, send_out_ref, buffer_ref, tokens_ref, sems, token_sems
):
    outer, inner, rows, width = buffer_ref.shape
    rows //= 3
    parts = sems.shape[0]
    per_part = outer // parts
    length = keep_out_ref.shape[0]
    span = per_part * inner * rows

    def fetch(part):
        at = pl.ds(part * per_part, per_part)
        return pltpu.make_async_copy(weights_ref.at[at], buffer_ref.at[at], sems.at[part])

    def fetch_tokens(part, half):
        ref = (send_ref, keep_ref)[half]
        return pltpu.make_async_copy(
            ref.at[:, pl.ds(part * span, span)],
            tokens_ref.at[part, pl.ds(half * length, length)],
            token_sems.at[part, half],
        )

    for part in range(parts):
        fetch_tokens(part, 0).start()
        fetch_tokens(part, 1).start()
        fetch(part).start()
    for part in range(parts):
        fetch_tokens(part, 0).wait()
        fetch_tokens(part, 1).wait()
        fetch(part).wait()
        for kind in range(3):
            block = buffer_ref[
                part * per_part : (part + 1) * per_part, :, kind * rows : (kind + 1) * rows, :
            ].reshape(span, width)
            cols = slice(kind * width, (kind + 1) * width)
            product = jnp.dot(tokens_ref[part], block, preferred_element_type=F32)
            for at, out_ref in ((0, send_out_ref), (length, keep_out_ref)):
                its_rows = product[at : at + length]
                out_ref[:, cols] = its_rows if part == 0 else out_ref[:, cols] + its_rows


def first_kernel(
    kept_ref,
    received_ref,
    drive_real_ref,
    drive_imag_ref,
    undo_real_ref,
    undo_imag_ref,
    gated_ref,
    feed_ref,
    sums_real_ref,
    sums_imag_ref,
    total_ref,
    last_ref,
):
    length, width = gated_ref.shape
    feed = (kept_ref[:, 2 * width :] + received_ref[:, 2 * width :]).astype(BF)
    feed_ref[...] = feed
    lower = (
        lax.broadcasted_iota(jnp.int32, (length, length), 0)
        >= lax.broadcasted_iota(jnp.int32, (length, length), 1)
    ).astype(BF)
    flat = sums_real_ref.shape[1]
    half = last_ref.shape[0] // 2
    for at in range(0, flat, CHUNK):
        cols = slice(at, at + CHUNK)
        pushed_real = jnp.dot(feed, drive_real_ref[:, cols], preferred_element_type=F32)
        pushed_imag = jnp.dot(feed, drive_imag_ref[:, cols], preferred_element_type=F32)
        scaled = rotate(undo_real_ref[:, cols], undo_imag_ref[:, cols], pushed_real, pushed_imag)
        for part, ref in enumerate((sums_real_ref, sums_imag_ref)):
            sums = jnp.dot(lower, scaled[part].astype(BF), preferred_element_type=F32)
            ref[:, cols] = sums
            for lane in range(0, CHUNK, LANES):
                row = part * half + (at + lane) // LANES
                last_ref[row : row + 1, :] = sums[length - 1 :, lane : lane + LANES]
    total_ref[...] = jnp.broadcast_to(last_ref[...][None], total_ref.shape)
    value = kept_ref[:, :width] + received_ref[:, :width]
    gate = kept_ref[:, width : 2 * width] + received_ref[:, width : 2 * width]
    gated_ref[...] = (value * jax.nn.sigmoid(gate)).astype(BF)


def conv_kernel(before_ref, gated_ref, taps_ref, out_ref, pad_ref):
    length, width = gated_ref.shape
    lead = before_ref.shape[0]
    taps = taps_ref.shape[0]
    pad_ref[:lead] = before_ref[...].astype(F32)
    pad_ref[lead:] = gated_ref[...].astype(F32)
    for col in range(width // LANES):
        cols = slice(col * LANES, (col + 1) * LANES)
        acc = jnp.zeros((length, LANES), F32)
        for tap in range(taps):
            start = lead - (taps - 1) + tap
            acc = acc + taps_ref[tap : tap + 1, cols] * pad_ref[start : start + length, cols]
        out_ref[:, cols] = acc.astype(BF)


def weighted(weights_ref, values_ref):
    half = values_ref.shape[1] // 2
    real, imag = rotate(
        weights_ref[:, :half, :], weights_ref[:, half:, :], values_ref[:, :half, :], values_ref[:, half:, :]
    )
    return jnp.sum(real, axis=0), jnp.sum(imag, axis=0)


def row_kernel(totals_ref, tail_ref, out_ref):
    half = totals_ref.shape[1] // 2
    real, imag = weighted(tail_ref, totals_ref)
    for copy in range(out_ref.shape[0]):
        out_ref[copy, :half] = real
        out_ref[copy, half:] = imag


def second_kernel(
    totals_ref,
    lead_ref,
    ends_of_rows_ref,
    lead_rows_ref,
    tail_rows_ref,
    ends_ref,
    power_real_ref,
    power_imag_ref,
    sums_real_ref,
    sums_imag_ref,
    mix_real_ref,
    mix_imag_ref,
    feed_ref,
    skip_ref,
    conv_ref,
    out_ref,
    final_ref,
    entry_ref,
):
    half = final_ref.shape[0] // 2
    lead = weighted(lead_ref, totals_ref)
    lead_rows = weighted(lead_rows_ref, ends_of_rows_ref)
    tail_rows = weighted(tail_rows_ref, ends_of_rows_ref)
    for part in range(2):
        rows = slice(part * half, (part + 1) * half)
        entry_ref[rows] = ends_ref[0, rows] + lead[part] + lead_rows[part]
        final_ref[rows] = ends_ref[1, rows] + tail_rows[part]
    response = skip_ref[...] * feed_ref[...].astype(F32)
    for at in range(0, sums_real_ref.shape[1], CHUNK):
        cols = slice(at, at + CHUNK)
        rows = range(at // LANES, (at + CHUNK) // LANES)
        entry_real = jnp.concatenate([entry_ref[row : row + 1] for row in rows], axis=1)
        entry_imag = jnp.concatenate([entry_ref[half + row : half + row + 1] for row in rows], axis=1)
        state_real, state_imag = rotate(
            power_real_ref[:, cols],
            power_imag_ref[:, cols],
            sums_real_ref[:, cols] + entry_real,
            sums_imag_ref[:, cols] + entry_imag,
        )
        response = response + jnp.dot(state_real.astype(BF), mix_real_ref[cols, :], preferred_element_type=F32)
        response = response + jnp.dot(state_imag.astype(BF), mix_imag_ref[cols, :], preferred_element_type=F32)
    activated = jax.nn.gelu(response).astype(BF)
    length = activated.shape[0]
    conv = conv_ref[...]
    for copy in range(out_ref.shape[0]):
        out_ref[copy, :length] = conv
        out_ref[copy, length:] = activated


def last_kernel(
    core_ref, rows_ref, own_ref, other_ref, gain_ref, shift_ref, out_ref, buffer_ref, act_ref, acc_ref, sems
):
    blocks, length, width = rows_ref.shape
    length //= 2
    outer, inner, cores, rows, _ = buffer_ref.shape
    rows //= 6
    parts = sems.shape[0]
    per_part = outer // parts
    per_block = blocks // parts
    core = core_ref[0]

    def fetch(part, half):
        at = pl.ds(part * per_part, per_part)
        slot, ref = ((core, own_ref), (1 - core, other_ref))[half]
        return pltpu.make_async_copy(ref.at[at], buffer_ref.at[at, :, slot], sems.at[part, half])

    for part in range(parts):
        fetch(part, 0).start()
        fetch(part, 1).start()
    channels = blocks * width
    total = jnp.zeros((length, width), F32)
    squares = jnp.zeros((length, width), F32)
    for at in range(blocks):
        total = total + rows_ref[at, :length, :].astype(F32)
    mean = jnp.sum(total, axis=1, keepdims=True) / channels
    for at in range(blocks):
        centred = rows_ref[at, :length, :].astype(F32) - mean
        squares = squares + centred * centred
    scale = lax.rsqrt(jnp.sum(squares, axis=1, keepdims=True) / channels + 1e-05)
    for at in range(blocks):
        centred = rows_ref[at, :length, :].astype(F32) - mean
        cols = slice(at * width, (at + 1) * width)
        act_ref[:, cols] = jax.nn.silu(centred * scale * gain_ref[:, cols] + shift_ref[:, cols]).astype(BF)
    span = per_part * inner * cores * rows
    for part in range(parts):
        fetch(part, 0).wait()
        fetch(part, 1).wait()
        conv_act = act_ref[:, part * span : (part + 1) * span]
        activated = jnp.concatenate(
            [rows_ref[part * per_block + at, length:, :] for at in range(per_block)], axis=1
        )
        for kind in range(6):
            block = buffer_ref[
                part * per_part : (part + 1) * per_part, :, :, kind * rows : (kind + 1) * rows, :
            ].reshape(span, width)
            product = jnp.dot(conv_act if kind < 2 else activated, block, preferred_element_type=F32)
            cols = slice(kind * width, (kind + 1) * width)
            acc_ref[:, cols] = product if part == 0 else acc_ref[:, cols] + product
    columns = 2 * width
    out_ref[...] = (
        acc_ref[:, :columns]
        + acc_ref[:, columns : 2 * columns] * jax.nn.sigmoid(acc_ref[:, 2 * columns :])
    ).astype(BF)


def grant(mib):
    return pltpu.CompilerParams(vmem_limit_bytes=mib << 20)


def whole(shape):
    return pl.BlockSpec(shape, lambda *_: (0,) * len(shape))


def spread(blocks, size):
    total, b = blocks.shape
    wide = total // size * b
    pick = lax.broadcasted_iota(jnp.int32, (b, wide), 1) % b == lax.broadcasted_iota(jnp.int32, (b, wide), 0)
    tiled = jnp.dot(blocks.astype(BF), pick.astype(BF), preferred_element_type=F32)
    row = lax.broadcasted_iota(jnp.int32, tiled.shape, 0) // size
    col = lax.broadcasted_iota(jnp.int32, tiled.shape, 1) // b
    return jnp.where(row == col, tiled, 0.0).astype(BF)


def rows_of(real, imag):
    n, s = real.shape
    return jnp.concatenate([real.reshape(n, s // LANES, LANES), imag.reshape(n, s // LANES, LANES)], axis=1)


def local(
    tokens,
    norm_gain,
    conv_value,
    conv_gate,
    state_feed,
    conv_taps,
    chan_gain,
    chan_shift,
    conv_project,
    decay_rate,
    frequency,
    input_real,
    input_imag,
    output_real,
    output_imag,
    skip_gain,
    state_value,
    state_gate,
    initial_state,
):
    seq_devices = lax.axis_size("z") * lax.axis_size("yh") * lax.axis_size("c")
    tp_devices = lax.axis_size("x") * lax.axis_size("yl")
    core = lax.axis_index("c")
    same = lax.axis_index("yl") == core
    position = (lax.axis_index("z") * lax.axis_size("yh") + lax.axis_index("yh")) * 2 + core
    length, model = tokens.shape
    rows_in, width = conv_value.shape
    rows_out, columns = conv_project.shape
    inner = lax.axis_size("yh")

    def swapped(value):
        return lax.ppermute(value, ("yl", "c"), [(a * 2 + b, b * 2 + a) for a in range(2) for b in range(2)])

    def packed(rows, *arrays):
        return pl.pallas_call(
            pack_kernel,
            out_shape=jax.ShapeDtypeStruct((rows, width), BF),
            name="pack",
        )(*arrays)

    def copies_of(shard):
        return jnp.broadcast_to(shard[None], (inner, *shard.shape))

    smem = pl.BlockSpec(memory_space=pltpu.SMEM)
    shard_first = packed(3 * rows_in, conv_value, conv_gate, state_feed)
    decay_rate, skip_gain, conv_taps, input_real, input_imag, output_real, output_imag, shard_first = (
        lax.optimization_barrier(
            (decay_rate, skip_gain, conv_taps, input_real, input_imag, output_real, output_imag, shard_first)
        )
    )
    blocks = []
    for shift in range(inner):
        pairs = [
            (h * 4 + a * 2 + b, (h + shift) % inner * 4 + b * 2 + a)
            for h in range(inner)
            for a in range(2)
            for b in range(2)
        ]
        blocks.append(lax.ppermute(shard_first, ("yh", "yl", "c"), pairs))
    places = (lax.axis_index("yh") - lax.iota(jnp.int32, inner)) % inner
    rows_first = pl.pallas_call(
        arrange_kernel,
        in_specs=[smem] + [whole(shard_first.shape)] * inner,
        out_shape=jax.ShapeDtypeStruct((inner, *shard_first.shape), BF),
        compiler_params=grant(4),
        name="arrange",
    )(places, *blocks)
    weights_first = lax.all_gather(rows_first, "z", axis=0, tiled=False)
    tokens, conv_project, state_value, state_gate, _ = lax.optimization_barrier(
        (tokens, conv_project, state_value, state_gate, rows_first)
    )
    shard_last = packed(6 * rows_out, conv_project, state_value, state_gate)
    core_scalar = core.astype(jnp.int32).reshape(1)
    own_half = pl.pallas_call(
        norm_kernel,
        in_specs=[smem, whole(tokens.shape), whole((1, model))],
        out_shape=jax.ShapeDtypeStruct((length, model // 2), BF),
        name="norm",
    )(core_scalar, tokens, norm_gain.reshape(1, model))
    across = [(0, 1), (1, 0)]
    half_sent, _ = lax.optimization_barrier((own_half, rows_first))
    other_half = lax.ppermute(half_sent, "yl", across)
    shard_last, _ = lax.optimization_barrier((shard_last, rows_first))
    rows_last = lax.all_to_all(copies_of(swapped(shard_last)), "yh", 0, 0, tiled=True)
    keep = jnp.where(same, own_half, other_half)
    send = jnp.where(same, other_half, own_half)

    groups, state_size, group_size = input_real.shape
    small = groups * group_size
    parameters = [
        jnp.concatenate([jnp.swapaxes(p, 1, 2).reshape(small, state_size) for p in (input_real, input_imag)], axis=1),
        jnp.concatenate([p.reshape(small, state_size) for p in (output_real, output_imag)], axis=1),
        jnp.concatenate([decay_rate, frequency], axis=1),
        jnp.concatenate([initial_state[0], initial_state[1]], axis=1),
        conv_taps[:, :LANES],
        conv_taps[:, LANES:],
        skip_gain.reshape(width // LANES, LANES),
    ]
    ends_at = []
    for p in parameters:
        ends_at.append((ends_at[-1] if ends_at else 0) + p.shape[0])
    flat_parameters = jnp.concatenate(parameters, axis=0)
    flat_parameters = jnp.where(same, flat_parameters, lax.ppermute(flat_parameters, "c", across))
    flat_parameters, _ = lax.optimization_barrier((flat_parameters, own_half))
    inputs, outputs, rates, initial, taps_left, taps_right, skip = jnp.split(flat_parameters, ends_at[:-1], axis=0)
    conv_taps = jnp.concatenate([taps_left, taps_right], axis=1)
    input_real, input_imag = (
        part.reshape(groups, group_size, state_size) for part in jnp.split(inputs, 2, axis=1)
    )
    output_real, output_imag = (
        part.reshape(groups, group_size, state_size) for part in jnp.split(outputs, 2, axis=1)
    )
    decay_rate, frequency = jnp.split(rates, 2, axis=1)
    initial_state = jnp.split(initial, 2, axis=1)

    flat = groups * state_size
    total_tokens = length * seq_devices
    rate_real = -decay_rate / total_tokens
    magnitude = jnp.exp(rate_real)
    step_real = magnitude * jnp.cos(frequency)
    step_imag = magnitude * jnp.sin(frequency)
    modulus = rate_real * rate_real + frequency * frequency
    lift_real = step_real - 1.0
    factor_real = (lift_real * rate_real + step_imag * frequency) / modulus
    factor_imag = (step_imag * rate_real - lift_real * frequency) / modulus
    drive_real = factor_real[:, None] * input_real - factor_imag[:, None] * input_imag
    drive_imag = factor_real[:, None] * input_imag + factor_imag[:, None] * input_real

    drive_real = spread(drive_real.reshape(small, state_size), group_size)
    drive_imag = spread(drive_imag.reshape(small, state_size), group_size)
    mix_real = spread(jnp.swapaxes(output_real, 1, 2).reshape(flat, group_size), state_size)
    mix_imag = spread(jnp.swapaxes(-output_imag, 1, 2).reshape(flat, group_size), state_size)

    base_real = step_real.reshape(flat)
    base_imag = step_imag.reshape(flat)
    square_size = base_real * base_real + base_imag * base_imag

    counted = jnp.concatenate([lax.iota(jnp.int32, 8) + 1, lax.iota(jnp.int32, length // 8) * 8])
    counted_real, counted_imag = power_table(
        jnp.concatenate([base_real, base_real / square_size]),
        jnp.concatenate([base_imag, -base_imag / square_size]),
        counted,
        length,
    )

    def powers(cols):
        real, imag = (counted_real[:, cols], counted_imag[:, cols])
        table = rotate(real[8:, None], imag[8:, None], real[None, :8], imag[None, :8])
        return tuple(part.reshape(length, flat) for part in table)

    power_real, power_imag = powers(slice(0, flat))
    undo_real, undo_imag = powers(slice(flat, 2 * flat))
    span_real, span_imag = (power_real[-1], power_imag[-1])
    row_devices = inner * 2
    outer = seq_devices // row_devices
    in_row = position % row_devices
    row = position // row_devices
    lag = in_row - lax.iota(jnp.int32, row_devices)
    lag_rows = row - lax.iota(jnp.int32, outer)

    exponents = (
        lag,
        row_devices - lax.iota(jnp.int32, row_devices),
        (lag_rows - 1) * row_devices + in_row,
        (outer - 1 - lax.iota(jnp.int32, outer)) * row_devices,
        jnp.stack([position, jnp.int32(seq_devices)] + [jnp.int32(0)] * 6),
    )
    chosen = jnp.concatenate(
        [lag > 0, jnp.ones(row_devices, bool), lag_rows > 0, jnp.ones(outer + 8, bool)]
    ).astype(F32)[:, None]
    spans_real, spans_imag = power_table(
        span_real, span_imag, jnp.maximum(jnp.concatenate(exponents), 0), seq_devices
    )
    spans = rows_of(spans_real * chosen, spans_imag * chosen)
    cuts = (0, row_devices, 2 * row_devices, 2 * row_devices + outer, 2 * row_devices + 2 * outer)
    lead, tail, lead_rows, tail_rows = (spans[first:last] for first, last in zip(cuts[:-1], cuts[1:]))
    ends = rows_of(
        *rotate(
            spans_real[cuts[-1] : cuts[-1] + 2],
            spans_imag[cuts[-1] : cuts[-1] + 2],
            initial_state[0].reshape(1, flat),
            initial_state[1].reshape(1, flat),
        )
    )
    (
        rows_last, keep, drive_real, drive_imag, mix_real, mix_imag, power_real, power_imag, undo_real, undo_imag, lead, tail, lead_rows,
        tail_rows, ends
    ) = lax.optimization_barrier((
        rows_last, keep, drive_real, drive_imag, mix_real, mix_imag, power_real, power_imag, undo_real, undo_imag, lead, tail, lead_rows,
        tail_rows, ends
    ))
    weights_last = lax.all_gather(rows_last, "z", axis=0, tiled=False)
    chunks = flat // LANES

    parts = 4
    hbm = pl.BlockSpec(memory_space=pl.ANY)
    kept, sent = pl.pallas_call(
        project_kernel,
        in_specs=[hbm, hbm, hbm],
        out_shape=[jax.ShapeDtypeStruct((length, 3 * width), F32)] * 2,
        scratch_shapes=[
            pltpu.VMEM(weights_first.shape, BF),
            pltpu.VMEM((parts, 2 * length, model // 2 // parts), BF),
            pltpu.SemaphoreType.DMA((parts,)),
            pltpu.SemaphoreType.DMA((parts, 2)),
        ],
        name="project",
    )(keep, send, weights_first)
    received = lax.ppermute(sent, "c", across)
    gated, feed, sums_real, sums_imag, total = pl.pallas_call(
        first_kernel,
        out_shape=[
            jax.ShapeDtypeStruct((length, width), BF),
            jax.ShapeDtypeStruct((length, width), BF),
            jax.ShapeDtypeStruct((length, flat), F32),
            jax.ShapeDtypeStruct((length, flat), F32),
            jax.ShapeDtypeStruct((row_devices, 2 * chunks, LANES), F32),
        ],
        scratch_shapes=[pltpu.VMEM((2 * chunks, LANES), F32)],
        name="first",
    )(kept, received, drive_real, drive_imag, undo_real, undo_imag)

    taps = conv_taps.shape[0]
    halo = (taps - 1 + 15) // 16 * 16
    before = lax.ppermute(
        gated[length - halo :], SEQUENCE, [(source, source + 1) for source in range(seq_devices - 1)]
    )
    totals = lax.all_to_all(total, SEQUENCE[1:], 0, 0, tiled=True)
    end_of_row = pl.pallas_call(
        row_kernel,
        out_shape=jax.ShapeDtypeStruct((outer, 2 * chunks, LANES), F32),
        name="row",
    )(totals, tail)
    ends_of_rows = lax.all_to_all(end_of_row, SEQUENCE[0], 0, 0, tiled=True)
    conv_out = pl.pallas_call(
        conv_kernel,
        out_shape=jax.ShapeDtypeStruct((length, width), BF),
        scratch_shapes=[pltpu.VMEM((halo + length, width), F32)],
        compiler_params=grant(4),
        name="conv",
    )(before, gated, conv_taps)

    copies, final = pl.pallas_call(
        second_kernel,
        out_shape=[
            jax.ShapeDtypeStruct((tp_devices, 2 * length, width), BF),
            jax.ShapeDtypeStruct((2 * chunks, LANES), F32),
        ],
        scratch_shapes=[pltpu.VMEM((2 * chunks, LANES), F32)],
        name="second",
    )(
        totals, lead, ends_of_rows, lead_rows, tail_rows, ends, power_real, power_imag, sums_real, sums_imag,
        mix_real, mix_imag, feed,
        skip.reshape(1, width), conv_out,
    )
    final = swapped(final)
    exchanged = lax.all_to_all(copies, ("x", "yl"), 0, 0, tiled=True)

    exchanged, final = lax.optimization_barrier((exchanged, final))
    weights_sent, _ = lax.optimization_barrier((weights_last, copies))
    weights_other = lax.ppermute(weights_sent, "c", across)
    mixed = pl.pallas_call(
        last_kernel,
        in_specs=[
            smem,
            whole(exchanged.shape),
            hbm,
            hbm,
            whole((1, chan_gain.shape[0])),
            whole((1, chan_gain.shape[0])),
        ],
        out_shape=jax.ShapeDtypeStruct((length, columns), BF),
        scratch_shapes=[
            pltpu.VMEM((*weights_last.shape[:2], 2, *weights_last.shape[2:]), BF),
            pltpu.VMEM((length, tp_devices * width), BF),
            pltpu.VMEM((length, 6 * width), F32),
            pltpu.SemaphoreType.DMA((parts, 2)),
        ],
        compiler_params=grant(20),
        name="last",
    )(core_scalar, exchanged, weights_last, weights_other, chan_gain.reshape(1, -1), chan_shift.reshape(1, -1))
    mixer_out = swapped(mixed)
    return (mixer_out, final.reshape(2, groups, state_size))


def solution(mesh):
    mesh = Mesh(mesh.devices.reshape(8, 4, 2, 4, 2), ("z", "yh", "yl", "x", "c"))
    in_specs = (
        P(SP, None),
        P(),
        P(SP, TP),
        P(SP, TP),
        P(SP, TP),
        P(None, TP),
        P(),
        P(),
        P(SP, TP),
        P(TP, None),
        P(TP, None),
        P(TP, None, None),
        P(TP, None, None),
        P(TP, None, None),
        P(TP, None, None),
        P(TP),
        P(SP, TP),
        P(SP, TP),
        P(None, TP, None),
    )
    out_specs = (P(SP, TP), P(None, TP, None))
    return jax.shard_map(local, mesh=mesh, in_specs=in_specs, out_specs=out_specs, check_vma=False)
```

```python
import jax
import jax.numpy as jnp
from jax import lax
from jax.experimental import pallas as pl
from jax.experimental.pallas import tpu as pltpu
from jax.sharding import Mesh, PartitionSpec as P

BF = jnp.bfloat16
F32 = jnp.float32
LANES = 128
CHUNK = 256
SP = ("z", "yh", "yl")
TP = ("x", "c")
SEQUENCE = ("z", "yh", "c")


def rotate(first_real, first_imag, second_real, second_imag):
    return (
        first_real * second_real - first_imag * second_imag,
        first_real * second_imag + first_imag * second_real,
    )


def power_table(base_real, base_imag, exponent, largest):
    result_real = jnp.ones((exponent.shape[0], base_real.shape[0]), F32)
    result_imag = jnp.zeros((exponent.shape[0], base_real.shape[0]), F32)
    square_real, square_imag = (base_real, base_imag)
    for place in range(max(largest, 1).bit_length()):
        chosen = (exponent >> place & 1 == 1)[:, None]
        next_real, next_imag = rotate(result_real, result_imag, square_real, square_imag)
        result_real = jnp.where(chosen, next_real, result_real)
        result_imag = jnp.where(chosen, next_imag, result_imag)
        square_real, square_imag = rotate(square_real, square_imag, square_real, square_imag)
    return (result_real, result_imag)


def pack_kernel(*refs):
    out_ref = refs[-1]
    width = out_ref.shape[1]
    at = 0
    for ref in refs[:-1]:
        for col in range(0, ref.shape[1], width):
            out_ref[at : at + ref.shape[0]] = ref[:, col : col + width]
            at += ref.shape[0]


def arrange_kernel(places_ref, *refs):
    out_ref = refs[-1]
    for at, ref in enumerate(refs[:-1]):
        out_ref[places_ref[at]] = ref[...]


def norm_kernel(core_ref, tokens_ref, gain_ref, out_ref):
    floats = tokens_ref[...].astype(F32)
    model = floats.shape[1]
    scale = lax.rsqrt(jnp.sum(floats * floats, axis=1, keepdims=True) / model + 1e-06)
    first_core = core_ref[0] == 0
    low = lax.broadcasted_iota(jnp.int32, (floats.shape[0], LANES), 1) < LANES // 2
    for at in range(0, model, 2 * LANES):
        left = tokens_ref[:, at : at + LANES].astype(F32) * scale * gain_ref[:, at : at + LANES]
        right = (
            tokens_ref[:, at + LANES : at + 2 * LANES].astype(F32)
            * scale
            * gain_ref[:, at + LANES : at + 2 * LANES]
        )
        taken = jnp.where(
            low,
            jnp.where(first_core, left, pltpu.roll(left, LANES // 2, 1)),
            jnp.where(first_core, pltpu.roll(right, LANES // 2, 1), right),
        )
        out_ref[:, at // 2 : at // 2 + LANES] = taken.astype(BF)


def project_kernel(
    keep_ref, send_ref, weights_ref, keep_out_ref, send_out_ref, buffer_ref, tokens_ref, sems, token_sems
):
    outer, inner, rows, width = buffer_ref.shape
    rows //= 3
    parts = sems.shape[0]
    per_part = outer // parts
    length = keep_out_ref.shape[0]
    span = per_part * inner * rows

    def fetch(part):
        at = pl.ds(part * per_part, per_part)
        return pltpu.make_async_copy(weights_ref.at[at], buffer_ref.at[at], sems.at[part])

    def fetch_tokens(part, half):
        ref = (send_ref, keep_ref)[half]
        return pltpu.make_async_copy(
            ref.at[:, pl.ds(part * span, span)],
            tokens_ref.at[part, pl.ds(half * length, length)],
            token_sems.at[part, half],
        )

    for part in range(parts):
        fetch_tokens(part, 0).start()
        fetch_tokens(part, 1).start()
        fetch(part).start()
    for part in range(parts):
        fetch_tokens(part, 0).wait()
        fetch_tokens(part, 1).wait()
        fetch(part).wait()
        for kind in range(3):
            block = buffer_ref[
                part * per_part : (part + 1) * per_part, :, kind * rows : (kind + 1) * rows, :
            ].reshape(span, width)
            cols = slice(kind * width, (kind + 1) * width)
            product = jnp.dot(tokens_ref[part], block, preferred_element_type=F32)
            for at, out_ref in ((0, send_out_ref), (length, keep_out_ref)):
                its_rows = product[at : at + length]
                out_ref[:, cols] = its_rows if part == 0 else out_ref[:, cols] + its_rows


def first_kernel(
    kept_ref,
    received_ref,
    drive_real_ref,
    drive_imag_ref,
    undo_real_ref,
    undo_imag_ref,
    gated_ref,
    feed_ref,
    sums_real_ref,
    sums_imag_ref,
    total_ref,
    last_ref,
):
    length, width = gated_ref.shape
    feed = (kept_ref[:, 2 * width :] + received_ref[:, 2 * width :]).astype(BF)
    feed_ref[...] = feed
    lower = (
        lax.broadcasted_iota(jnp.int32, (length, length), 0)
        >= lax.broadcasted_iota(jnp.int32, (length, length), 1)
    ).astype(BF)
    flat = sums_real_ref.shape[1]
    half = last_ref.shape[0] // 2
    for at in range(0, flat, CHUNK):
        cols = slice(at, at + CHUNK)
        pushed_real = jnp.dot(feed, drive_real_ref[:, cols], preferred_element_type=F32)
        pushed_imag = jnp.dot(feed, drive_imag_ref[:, cols], preferred_element_type=F32)
        scaled = rotate(undo_real_ref[:, cols], undo_imag_ref[:, cols], pushed_real, pushed_imag)
        for part, ref in enumerate((sums_real_ref, sums_imag_ref)):
            sums = jnp.dot(lower, scaled[part].astype(BF), preferred_element_type=F32)
            ref[:, cols] = sums
            for lane in range(0, CHUNK, LANES):
                row = part * half + (at + lane) // LANES
                last_ref[row : row + 1, :] = sums[length - 1 :, lane : lane + LANES]
    total_ref[...] = jnp.broadcast_to(last_ref[...][None], total_ref.shape)
    value = kept_ref[:, :width] + received_ref[:, :width]
    gate = kept_ref[:, width : 2 * width] + received_ref[:, width : 2 * width]
    gated_ref[...] = (value * jax.nn.sigmoid(gate)).astype(BF)


def conv_kernel(before_ref, gated_ref, taps_ref, out_ref, pad_ref):
    length, width = gated_ref.shape
    lead = before_ref.shape[0]
    taps = taps_ref.shape[0]
    pad_ref[:lead] = before_ref[...].astype(F32)
    pad_ref[lead:] = gated_ref[...].astype(F32)
    for col in range(width // LANES):
        cols = slice(col * LANES, (col + 1) * LANES)
        acc = jnp.zeros((length, LANES), F32)
        for tap in range(taps):
            start = lead - (taps - 1) + tap
            acc = acc + taps_ref[tap : tap + 1, cols] * pad_ref[start : start + length, cols]
        out_ref[:, cols] = acc.astype(BF)


def weighted(weights_ref, values_ref):
    half = values_ref.shape[1] // 2
    real, imag = rotate(
        weights_ref[:, :half, :], weights_ref[:, half:, :], values_ref[:, :half, :], values_ref[:, half:, :]
    )
    return jnp.sum(real, axis=0), jnp.sum(imag, axis=0)


def row_kernel(totals_ref, tail_ref, out_ref):
    half = totals_ref.shape[1] // 2
    real, imag = weighted(tail_ref, totals_ref)
    for copy in range(out_ref.shape[0]):
        out_ref[copy, :half] = real
        out_ref[copy, half:] = imag


def second_kernel(
    totals_ref,
    lead_ref,
    ends_of_rows_ref,
    lead_rows_ref,
    tail_rows_ref,
    ends_ref,
    power_real_ref,
    power_imag_ref,
    sums_real_ref,
    sums_imag_ref,
    mix_real_ref,
    mix_imag_ref,
    feed_ref,
    skip_ref,
    conv_ref,
    out_ref,
    final_ref,
    entry_ref,
):
    half = final_ref.shape[0] // 2
    lead = weighted(lead_ref, totals_ref)
    lead_rows = weighted(lead_rows_ref, ends_of_rows_ref)
    tail_rows = weighted(tail_rows_ref, ends_of_rows_ref)
    for part in range(2):
        rows = slice(part * half, (part + 1) * half)
        entry_ref[rows] = ends_ref[0, rows] + lead[part] + lead_rows[part]
        final_ref[rows] = ends_ref[1, rows] + tail_rows[part]
    response = skip_ref[...] * feed_ref[...].astype(F32)
    for at in range(0, sums_real_ref.shape[1], CHUNK):
        cols = slice(at, at + CHUNK)
        rows = range(at // LANES, (at + CHUNK) // LANES)
        entry_real = jnp.concatenate([entry_ref[row : row + 1] for row in rows], axis=1)
        entry_imag = jnp.concatenate([entry_ref[half + row : half + row + 1] for row in rows], axis=1)
        state_real, state_imag = rotate(
            power_real_ref[:, cols],
            power_imag_ref[:, cols],
            sums_real_ref[:, cols] + entry_real,
            sums_imag_ref[:, cols] + entry_imag,
        )
        response = response + jnp.dot(state_real.astype(BF), mix_real_ref[cols, :], preferred_element_type=F32)
        response = response + jnp.dot(state_imag.astype(BF), mix_imag_ref[cols, :], preferred_element_type=F32)
    activated = jax.nn.gelu(response).astype(BF)
    length = activated.shape[0]
    conv = conv_ref[...]
    for copy in range(out_ref.shape[0]):
        out_ref[copy, :length] = conv
        out_ref[copy, length:] = activated


def last_kernel(
    core_ref, rows_ref, own_ref, other_ref, gain_ref, shift_ref, out_ref, buffer_ref, act_ref, acc_ref, sems
):
    blocks, length, width = rows_ref.shape
    length //= 2
    outer, inner, cores, rows, _ = buffer_ref.shape
    rows //= 6
    parts = sems.shape[0]
    per_part = outer // parts
    per_block = blocks // parts
    core = core_ref[0]

    def fetch(part, half):
        at = pl.ds(part * per_part, per_part)
        slot, ref = ((core, own_ref), (1 - core, other_ref))[half]
        return pltpu.make_async_copy(ref.at[at], buffer_ref.at[at, :, slot], sems.at[part, half])

    for part in range(parts):
        fetch(part, 0).start()
        fetch(part, 1).start()
    channels = blocks * width
    total = jnp.zeros((length, width), F32)
    squares = jnp.zeros((length, width), F32)
    for at in range(blocks):
        total = total + rows_ref[at, :length, :].astype(F32)
    mean = jnp.sum(total, axis=1, keepdims=True) / channels
    for at in range(blocks):
        centred = rows_ref[at, :length, :].astype(F32) - mean
        squares = squares + centred * centred
    scale = lax.rsqrt(jnp.sum(squares, axis=1, keepdims=True) / channels + 1e-05)
    for at in range(blocks):
        centred = rows_ref[at, :length, :].astype(F32) - mean
        cols = slice(at * width, (at + 1) * width)
        act_ref[:, cols] = jax.nn.silu(centred * scale * gain_ref[:, cols] + shift_ref[:, cols]).astype(BF)
    span = per_part * inner * cores * rows
    for part in range(parts):
        fetch(part, 0).wait()
        fetch(part, 1).wait()
        conv_act = act_ref[:, part * span : (part + 1) * span]
        activated = jnp.concatenate(
            [rows_ref[part * per_block + at, length:, :] for at in range(per_block)], axis=1
        )
        for kind in range(6):
            block = buffer_ref[
                part * per_part : (part + 1) * per_part, :, :, kind * rows : (kind + 1) * rows, :
            ].reshape(span, width)
            product = jnp.dot(conv_act if kind < 2 else activated, block, preferred_element_type=F32)
            cols = slice(kind * width, (kind + 1) * width)
            acc_ref[:, cols] = product if part == 0 else acc_ref[:, cols] + product
    columns = 2 * width
    out_ref[...] = (
        acc_ref[:, :columns]
        + acc_ref[:, columns : 2 * columns] * jax.nn.sigmoid(acc_ref[:, 2 * columns :])
    ).astype(BF)


def grant(mib):
    return pltpu.CompilerParams(vmem_limit_bytes=mib << 20)


def whole(shape):
    return pl.BlockSpec(shape, lambda *_: (0,) * len(shape))


def spread(blocks, size):
    total, b = blocks.shape
    wide = total // size * b
    pick = lax.broadcasted_iota(jnp.int32, (b, wide), 1) % b == lax.broadcasted_iota(jnp.int32, (b, wide), 0)
    tiled = jnp.dot(blocks.astype(BF), pick.astype(BF), preferred_element_type=F32)
    row = lax.broadcasted_iota(jnp.int32, tiled.shape, 0) // size
    col = lax.broadcasted_iota(jnp.int32, tiled.shape, 1) // b
    return jnp.where(row == col, tiled, 0.0).astype(BF)


def rows_of(real, imag):
    n, s = real.shape
    return jnp.concatenate([real.reshape(n, s // LANES, LANES), imag.reshape(n, s // LANES, LANES)], axis=1)


def local(
    tokens,
    norm_gain,
    conv_value,
    conv_gate,
    state_feed,
    conv_taps,
    chan_gain,
    chan_shift,
    conv_project,
    decay_rate,
    frequency,
    input_real,
    input_imag,
    output_real,
    output_imag,
    skip_gain,
    state_value,
    state_gate,
    initial_state,
):
    seq_devices = lax.axis_size("z") * lax.axis_size("yh") * lax.axis_size("c")
    tp_devices = lax.axis_size("x") * lax.axis_size("yl")
    core = lax.axis_index("c")
    same = lax.axis_index("yl") == core
    position = (lax.axis_index("z") * lax.axis_size("yh") + lax.axis_index("yh")) * 2 + core
    length, model = tokens.shape
    rows_in, width = conv_value.shape
    rows_out, columns = conv_project.shape
    inner = lax.axis_size("yh")

    def swapped(value):
        return lax.ppermute(value, ("yl", "c"), [(a * 2 + b, b * 2 + a) for a in range(2) for b in range(2)])

    def packed(rows, *arrays):
        return pl.pallas_call(
            pack_kernel,
            out_shape=jax.ShapeDtypeStruct((rows, width), BF),
            name="pack",
        )(*arrays)

    def copies_of(shard):
        return jnp.broadcast_to(shard[None], (inner, *shard.shape))

    smem = pl.BlockSpec(memory_space=pltpu.SMEM)
    shard_first = packed(3 * rows_in, conv_value, conv_gate, state_feed)
    decay_rate, skip_gain, conv_taps, input_real, input_imag, output_real, output_imag, shard_first = (
        lax.optimization_barrier(
            (decay_rate, skip_gain, conv_taps, input_real, input_imag, output_real, output_imag, shard_first)
        )
    )
    blocks = []
    for shift in range(inner):
        pairs = [
            (h * 4 + a * 2 + b, (h + shift) % inner * 4 + b * 2 + a)
            for h in range(inner)
            for a in range(2)
            for b in range(2)
        ]
        blocks.append(lax.ppermute(shard_first, ("yh", "yl", "c"), pairs))
    places = (lax.axis_index("yh") - lax.iota(jnp.int32, inner)) % inner
    rows_first = pl.pallas_call(
        arrange_kernel,
        in_specs=[smem] + [whole(shard_first.shape)] * inner,
        out_shape=jax.ShapeDtypeStruct((inner, *shard_first.shape), BF),
        compiler_params=grant(4),
        name="arrange",
    )(places, *blocks)
    weights_first = lax.all_gather(rows_first, "z", axis=0, tiled=False)
    tokens, conv_project, state_value, state_gate, _ = lax.optimization_barrier(
        (tokens, conv_project, state_value, state_gate, rows_first)
    )
    shard_last = packed(6 * rows_out, conv_project, state_value, state_gate)
    core_scalar = core.astype(jnp.int32).reshape(1)
    own_half = pl.pallas_call(
        norm_kernel,
        in_specs=[smem, whole(tokens.shape), whole((1, model))],
        out_shape=jax.ShapeDtypeStruct((length, model // 2), BF),
        name="norm",
    )(core_scalar, tokens, norm_gain.reshape(1, model))
    across = [(0, 1), (1, 0)]
    half_sent, _ = lax.optimization_barrier((own_half, rows_first))
    other_half = lax.ppermute(half_sent, "yl", across)
    shard_last, _ = lax.optimization_barrier((shard_last, rows_first))
    rows_last = lax.all_to_all(copies_of(swapped(shard_last)), "yh", 0, 0, tiled=True)
    keep = jnp.where(same, own_half, other_half)
    send = jnp.where(same, other_half, own_half)

    groups, state_size, group_size = input_real.shape
    small = groups * group_size
    parameters = [
        jnp.concatenate([jnp.swapaxes(p, 1, 2).reshape(small, state_size) for p in (input_real, input_imag)], axis=1),
        jnp.concatenate([p.reshape(small, state_size) for p in (output_real, output_imag)], axis=1),
        jnp.concatenate([decay_rate, frequency], axis=1),
        jnp.concatenate([initial_state[0], initial_state[1]], axis=1),
        conv_taps[:, :LANES],
        conv_taps[:, LANES:],
        skip_gain.reshape(width // LANES, LANES),
    ]
    ends_at = []
    for p in parameters:
        ends_at.append((ends_at[-1] if ends_at else 0) + p.shape[0])
    flat_parameters = jnp.concatenate(parameters, axis=0)
    flat_parameters = jnp.where(same, flat_parameters, lax.ppermute(flat_parameters, "c", across))
    flat_parameters, _ = lax.optimization_barrier((flat_parameters, own_half))
    inputs, outputs, rates, initial, taps_left, taps_right, skip = jnp.split(flat_parameters, ends_at[:-1], axis=0)
    conv_taps = jnp.concatenate([taps_left, taps_right], axis=1)
    input_real, input_imag = (
        part.reshape(groups, group_size, state_size) for part in jnp.split(inputs, 2, axis=1)
    )
    output_real, output_imag = (
        part.reshape(groups, group_size, state_size) for part in jnp.split(outputs, 2, axis=1)
    )
    decay_rate, frequency = jnp.split(rates, 2, axis=1)
    initial_state = jnp.split(initial, 2, axis=1)

    flat = groups * state_size
    total_tokens = length * seq_devices
    rate_real = -decay_rate / total_tokens
    magnitude = jnp.exp(rate_real)
    step_real = magnitude * jnp.cos(frequency)
    step_imag = magnitude * jnp.sin(frequency)
    modulus = rate_real * rate_real + frequency * frequency
    lift_real = step_real - 1.0
    factor_real = (lift_real * rate_real + step_imag * frequency) / modulus
    factor_imag = (step_imag * rate_real - lift_real * frequency) / modulus
    drive_real = factor_real[:, None] * input_real - factor_imag[:, None] * input_imag
    drive_imag = factor_real[:, None] * input_imag + factor_imag[:, None] * input_real

    drive_real = spread(drive_real.reshape(small, state_size), group_size)
    drive_imag = spread(drive_imag.reshape(small, state_size), group_size)
    mix_real = spread(jnp.swapaxes(output_real, 1, 2).reshape(flat, group_size), state_size)
    mix_imag = spread(jnp.swapaxes(-output_imag, 1, 2).reshape(flat, group_size), state_size)

    base_real = step_real.reshape(flat)
    base_imag = step_imag.reshape(flat)
    square_size = base_real * base_real + base_imag * base_imag

    counted = jnp.concatenate([lax.iota(jnp.int32, 8) + 1, lax.iota(jnp.int32, length // 8) * 8])
    counted_real, counted_imag = power_table(
        jnp.concatenate([base_real, base_real / square_size]),
        jnp.concatenate([base_imag, -base_imag / square_size]),
        counted,
        length,
    )

    def powers(cols):
        real, imag = (counted_real[:, cols], counted_imag[:, cols])
        table = rotate(real[8:, None], imag[8:, None], real[None, :8], imag[None, :8])
        return tuple(part.reshape(length, flat) for part in table)

    power_real, power_imag = powers(slice(0, flat))
    undo_real, undo_imag = powers(slice(flat, 2 * flat))
    span_real, span_imag = (power_real[-1], power_imag[-1])
    row_devices = inner * 2
    outer = seq_devices // row_devices
    in_row = position % row_devices
    row = position // row_devices
    lag = in_row - lax.iota(jnp.int32, row_devices)
    lag_rows = row - lax.iota(jnp.int32, outer)

    exponents = (
        lag,
        row_devices - lax.iota(jnp.int32, row_devices),
        (lag_rows - 1) * row_devices + in_row,
        (outer - 1 - lax.iota(jnp.int32, outer)) * row_devices,
        jnp.stack([position, jnp.int32(seq_devices)] + [jnp.int32(0)] * 6),
    )
    chosen = jnp.concatenate(
        [lag > 0, jnp.ones(row_devices, bool), lag_rows > 0, jnp.ones(outer + 8, bool)]
    ).astype(F32)[:, None]
    spans_real, spans_imag = power_table(
        span_real, span_imag, jnp.maximum(jnp.concatenate(exponents), 0), seq_devices
    )
    spans = rows_of(spans_real * chosen, spans_imag * chosen)
    cuts = (0, row_devices, 2 * row_devices, 2 * row_devices + outer, 2 * row_devices + 2 * outer)
    lead, tail, lead_rows, tail_rows = (spans[first:last] for first, last in zip(cuts[:-1], cuts[1:]))
    ends = rows_of(
        *rotate(
            spans_real[cuts[-1] : cuts[-1] + 2],
            spans_imag[cuts[-1] : cuts[-1] + 2],
            initial_state[0].reshape(1, flat),
            initial_state[1].reshape(1, flat),
        )
    )
    (
        rows_last, keep, drive_real, drive_imag, mix_real, mix_imag, power_real, power_imag, undo_real, undo_imag, lead, tail, lead_rows,
        tail_rows, ends
    ) = lax.optimization_barrier((
        rows_last, keep, drive_real, drive_imag, mix_real, mix_imag, power_real, power_imag, undo_real, undo_imag, lead, tail, lead_rows,
        tail_rows, ends
    ))
    weights_last = lax.all_gather(rows_last, "z", axis=0, tiled=False)
    chunks = flat // LANES

    parts = 4
    hbm = pl.BlockSpec(memory_space=pl.ANY)
    kept, sent = pl.pallas_call(
        project_kernel,
        in_specs=[hbm, hbm, hbm],
        out_shape=[jax.ShapeDtypeStruct((length, 3 * width), F32)] * 2,
        scratch_shapes=[
            pltpu.VMEM(weights_first.shape, BF),
            pltpu.VMEM((parts, 2 * length, model // 2 // parts), BF),
            pltpu.SemaphoreType.DMA((parts,)),
            pltpu.SemaphoreType.DMA((parts, 2)),
        ],
        compiler_params=grant(24),
        name="project",
    )(keep, send, weights_first)
    received = lax.ppermute(sent, "c", across)
    gated, feed, sums_real, sums_imag, total = pl.pallas_call(
        first_kernel,
        out_shape=[
            jax.ShapeDtypeStruct((length, width), BF),
            jax.ShapeDtypeStruct((length, width), BF),
            jax.ShapeDtypeStruct((length, flat), F32),
            jax.ShapeDtypeStruct((length, flat), F32),
            jax.ShapeDtypeStruct((row_devices, 2 * chunks, LANES), F32),
        ],
        scratch_shapes=[pltpu.VMEM((2 * chunks, LANES), F32)],
        compiler_params=grant(24),
        name="first",
    )(kept, received, drive_real, drive_imag, undo_real, undo_imag)

    taps = conv_taps.shape[0]
    halo = (taps - 1 + 15) // 16 * 16
    before = lax.ppermute(
        gated[length - halo :], SEQUENCE, [(source, source + 1) for source in range(seq_devices - 1)]
    )
    totals = lax.all_to_all(total, SEQUENCE[1:], 0, 0, tiled=True)
    end_of_row = pl.pallas_call(
        row_kernel,
        out_shape=jax.ShapeDtypeStruct((outer, 2 * chunks, LANES), F32),
        name="row",
    )(totals, tail)
    ends_of_rows = lax.all_to_all(end_of_row, SEQUENCE[0], 0, 0, tiled=True)
    conv_out = pl.pallas_call(
        conv_kernel,
        out_shape=jax.ShapeDtypeStruct((length, width), BF),
        scratch_shapes=[pltpu.VMEM((halo + length, width), F32)],
        compiler_params=grant(4),
        name="conv",
    )(before, gated, conv_taps)

    copies, final = pl.pallas_call(
        second_kernel,
        out_shape=[
            jax.ShapeDtypeStruct((tp_devices, 2 * length, width), BF),
            jax.ShapeDtypeStruct((2 * chunks, LANES), F32),
        ],
        scratch_shapes=[pltpu.VMEM((2 * chunks, LANES), F32)],
        name="second",
    )(
        totals, lead, ends_of_rows, lead_rows, tail_rows, ends, power_real, power_imag, sums_real, sums_imag,
        mix_real, mix_imag, feed,
        skip.reshape(1, width), conv_out,
    )
    final = swapped(final)
    exchanged = lax.all_to_all(copies, ("x", "yl"), 0, 0, tiled=True)

    exchanged, final = lax.optimization_barrier((exchanged, final))
    weights_sent, _ = lax.optimization_barrier((weights_last, copies))
    weights_other = lax.ppermute(weights_sent, "c", across)
    mixed = pl.pallas_call(
        last_kernel,
        in_specs=[
            smem,
            whole(exchanged.shape),
            hbm,
            hbm,
            whole((1, chan_gain.shape[0])),
            whole((1, chan_gain.shape[0])),
        ],
        out_shape=jax.ShapeDtypeStruct((length, columns), BF),
        scratch_shapes=[
            pltpu.VMEM((*weights_last.shape[:2], 2, *weights_last.shape[2:]), BF),
            pltpu.VMEM((length, tp_devices * width), BF),
            pltpu.VMEM((length, 6 * width), F32),
            pltpu.SemaphoreType.DMA((parts, 2)),
        ],
        compiler_params=grant(20),
        name="last",
    )(core_scalar, exchanged, weights_last, weights_other, chan_gain.reshape(1, -1), chan_shift.reshape(1, -1))
    mixer_out = swapped(mixed)
    return (mixer_out, final.reshape(2, groups, state_size))


def solution(mesh):
    mesh = Mesh(mesh.devices.reshape(8, 4, 2, 4, 2), ("z", "yh", "yl", "x", "c"))
    in_specs = (
        P(SP, None),
        P(),
        P(SP, TP),
        P(SP, TP),
        P(SP, TP),
        P(None, TP),
        P(),
        P(),
        P(SP, TP),
        P(TP, None),
        P(TP, None),
        P(TP, None, None),
        P(TP, None, None),
        P(TP, None, None),
        P(TP, None, None),
        P(TP),
        P(SP, TP),
        P(SP, TP),
        P(None, TP, None),
    )
    out_specs = (P(SP, TP), P(None, TP, None))
    return jax.shard_map(local, mesh=mesh, in_specs=in_specs, out_specs=out_specs, check_vma=False)
```
